32 devices in a mesh: sp: 8 (over z, x), tp: 4 (over y, core).
Axes of the slice: x: 2, y: 2, z: 4, core: 2. Of those that a mesh axis runs over, the one named last changes fastest.
Arguments:
- residual: bfloat16 [4096, 2048], P('sp'), may hold values from -80 to 80
- queries: bfloat16 [4096, 1024], P('sp', 'tp'), may hold values from -260 to 260
- keys: bfloat16 [4096, 512], P('sp', 'tp'), may hold values from -7 to 7
- values: bfloat16 [4096, 512], P('sp', 'tp'), may hold values from -12 to 12
- documents: int32 [4096], P('sp'), may hold values from 0 to 3, never falling along the last dimension, each value on 1 to 3072 neighbouring positions
- sinks: float32 [16], P('tp'), may hold values from 1 to 6
- out_weight: bfloat16 [1024, 2048], P('tp'), may hold values from -0.5 to 0.5
- norm_gain: float32 [2048], replicated, may hold values from 0.1 to 1.9
- gate_weight: bfloat16 [2048, 5632], P('sp', 'tp'), may hold values from -0.125 to 0.125
- up_weight: bfloat16 [2048, 5632], P('sp', 'tp'), may hold values from -0.125 to 0.125
- down_weight: bfloat16 [2048, 5632], P('sp', 'tp'), may hold values from -0.078125 to 0.078125
Outputs:
- mixed: bfloat16 [4096, 2048], P('sp', 'tp')
The draws below stay inside these ranges and needn't reach their ends.
Inputs may be any that keep to these rules, and one draw needn't show every extreme that they name: `documents`: document numbers never fall along the positions; a document holds at most 3072 positions.
All inputs are finite; a program needn't handle non-finite values.
Results may differ from the reference program's by a relative error of at most 0.01.
Values may be sent and summed in bfloat16 or wider, within the bound.
A program may use at most 64 MiB of HBM per device.

```python
import math
import jax
import jax.numpy as jnp
import numpy as np
from jax import lax

D = 2048
HEADS = 16
KV_HEADS = 8
HEAD_DIM = 64
FF = 5632
WINDOW = 128
GROUP = 2
D_ATT = 1024
TOKENS = 4096
DOC_MOST = 3072
N_SP = 8
N_TP = 4


def drawn_keys(key):
    return jnp.clip(jax.random.normal(jax.random.fold_in(key, 11), (TOKENS, KV_HEADS * HEAD_DIM), jnp.float32), -6.0, 6.0)


def draw_keys(key, part):
    base_keys = drawn_keys(key)
    return base_keys.astype(jnp.bfloat16)


def draw_queries(key, part):
    entries = jnp.clip(jax.random.normal(jax.random.fold_in(key, 21), (TOKENS, HEADS * HEAD_DIM), jnp.float32), -6.0, 6.0)
    return entries.astype(jnp.bfloat16)


def draw_residual(key, part):
    col_scale = jnp.exp(jnp.linspace(jnp.log(0.5), jnp.log(3.0), D, dtype=jnp.float32))[None, :]
    row_scale = jnp.exp(jax.random.uniform(jax.random.fold_in(key, 31), (TOKENS, 1), jnp.float32, jnp.log(0.5), jnp.log(3.0)))
    entries = jnp.clip(jax.random.normal(jax.random.fold_in(key, 32), (TOKENS, D), jnp.float32), -6.0, 6.0)
    return (entries * row_scale * col_scale).astype(jnp.bfloat16)


def steps_of(key, extent, shards, least, top_value):
    def one(axis_at, parts):
        draws = jax.random.uniform(jax.random.fold_in(jax.random.fold_in(key, 6), axis_at), (parts,), jnp.float32, least / len(shards), top_value / len(shards))
        return jnp.repeat(jnp.exp(draws), extent[axis_at] // parts).reshape((-1,) + (1,) * (len(extent) - axis_at - 1))

    factor_of = one(*shards[0])
    for cut in shards[1:]:
        factor_of = factor_of * one(*cut)
    return factor_of


def length_profile(count, total, most, skew):
    loads = [(1 << 20) // math.isqrt(standing ** skew) + 1 for standing in range(2, count + 1)]
    rest, counts = total - most - (count - 1), [1] * (count - 1)
    while rest > 0:
        movable = [i for i in range(count - 1) if counts[i] < most]
        pool, remaining = sum([loads[i] for i in movable]), rest
        for i in movable:
            more = min(most - counts[i], max(1, remaining * loads[i] // pool), rest)
            counts[i] = counts[i] + more
            rest = rest - more
    return np.array([most] + counts)


def uneven_parts(key, count, total, reach, slope):
    if count == 2:
        one = jax.random.randint(key, (), max(1, total - reach), min(reach, total - 1) + 1)
        return jnp.stack([one, total - one])
    tallies = jnp.asarray(length_profile(count, total, reach, slope), jnp.int32)
    twos = (count - 1) // 2
    donor, sink = tallies[1:1 + 2 * twos:2], tallies[2:2 + 2 * twos:2]
    room = jnp.minimum(donor - 1, reach - sink)
    moved = jax.random.randint(jax.random.fold_in(key, 1), (twos,), 0, 1 << 20) % (room + 1)
    tallies = tallies.at[1:1 + 2 * twos:2].set(donor - moved).at[2:2 + 2 * twos:2].set(sink + moved)
    return tallies[jax.random.permutation(jax.random.fold_in(key, 2), count)]


def centred(key, shape, width, reach, split=(), kind=jnp.bfloat16):
    drawn = jax.random.normal(key, shape, jnp.float32) * width
    if len(split) > 0:
        drawn = steps_of(key, shape, split, -0.22, 0.18) * drawn
    return jnp.clip(drawn, min=-reach, max=reach).astype(kind)


def setup_inputs(seed: int = 0) -> dict:
    seeds = jax.random.split(jax.random.key(seed), 12)
    return {
        "residual": draw_residual(jax.random.fold_in(seeds[11], 71), 0),
        "queries": draw_queries(jax.random.fold_in(seeds[11], 71), 0),
        "keys": draw_keys(jax.random.fold_in(seeds[11], 71), 0),
        "values": centred(seeds[3], (TOKENS, KV_HEADS * HEAD_DIM), 2.0, 12.0, ((0, 8), (1, 4))),
        "documents": jnp.searchsorted(jnp.cumsum(uneven_parts(seeds[4], N_SP // 2, TOKENS, DOC_MOST, 1)), jnp.arange(TOKENS), side="right").astype(jnp.int32),
        "sinks": jnp.clip(1.0 + 5.0 * jax.random.uniform(seeds[5], (HEADS,), jnp.float32) ** steps_of(seeds[5], (HEADS,), ((0, 4),), -0.2, 0.2), 1.0, 6.0),
        "out_weight": centred(seeds[6], (D_ATT, D), (2 * HEAD_DIM) ** -0.5, 0.5, ((0, 4),)),
        "norm_gain": jnp.clip(1.0 + 0.18 * jax.random.normal(seeds[7], (D,), jnp.float32), 0.1, 1.9),
        "gate_weight": centred(seeds[8], (D, FF), D ** -0.5, 0.125, ((0, 8), (1, 4))),
        "up_weight": centred(seeds[9], (D, FF), D ** -0.5, 0.125, ((0, 8), (1, 4))),
        "down_weight": centred(seeds[10], (D, FF), FF ** -0.5, 0.078125, ((0, 8), (1, 4))),
    }


neg_big = -1e+30
norm_eps = 1e-05

def attend(queries, keys, values, documents, sinks):
    total_rows = queries.shape[0]
    block_count = total_rows // WINDOW
    q_blocks = queries.astype(jnp.float32).reshape(block_count, WINDOW, KV_HEADS, GROUP, HEAD_DIM)
    k_blocks = keys.astype(jnp.float32).reshape(block_count, WINDOW, KV_HEADS, HEAD_DIM)
    v_blocks = values.astype(jnp.float32).reshape(block_count, WINDOW, KV_HEADS, HEAD_DIM)
    zero_block = jnp.zeros_like(k_blocks[:1])
    k_band = jnp.concatenate([jnp.concatenate([zero_block, k_blocks[:-1]], axis=0), k_blocks], axis=1)
    v_band = jnp.concatenate([jnp.concatenate([zero_block, v_blocks[:-1]], axis=0), v_blocks], axis=1)
    doc_own = documents.astype(jnp.int32).reshape(block_count, WINDOW)
    doc_prev = jnp.concatenate([jnp.zeros((1, WINDOW), jnp.int32), doc_own[:-1]], axis=0)
    doc_band = jnp.concatenate([doc_prev, doc_own], axis=1)
    row_idx = jnp.arange(WINDOW, dtype=jnp.int32)
    col_idx = jnp.arange(2 * WINDOW, dtype=jnp.int32)
    first = jnp.arange(block_count, dtype=jnp.int32) * WINDOW
    q_pos = first[:, None] + row_idx[None, :]
    k_pos = first[:, None] - WINDOW + col_idx[None, :]
    distance = q_pos[:, :, None] - k_pos[:, None, :]
    visible = (distance >= 0) & (distance < WINDOW) & (k_pos[:, None, :] >= 0) & (doc_own[:, :, None] == doc_band[:, None, :])
    scores = jnp.einsum('nikgd,njkd->nkgij', q_blocks, k_band) * HEAD_DIM ** (-0.5)
    scores = jnp.where(visible[:, None, None], scores, neg_big)
    sink_logit = sinks.astype(jnp.float32).reshape(1, KV_HEADS, GROUP, 1, 1)
    row_max = jnp.maximum(scores.max(-1, keepdims=True), sink_logit)
    expo = jnp.where(visible[:, None, None], jnp.exp(scores - row_max), 0.0)
    denom_sum = expo.sum(-1, keepdims=True) + jnp.exp(sink_logit - row_max)
    weights = (expo / denom_sum).astype(jnp.bfloat16)
    mixed = jnp.einsum('nkgij,njkd->nikgd', weights.astype(jnp.float32), v_band)
    return mixed.reshape(total_rows, D_ATT).astype(jnp.bfloat16)

def reference(residual, queries, keys, values, documents, sinks, out_weight, norm_gain, gate_weight, up_weight, down_weight):
    attended = attend(queries, keys, values, documents, sinks)
    head_cols = D_ATT // N_TP
    projected = jnp.zeros((TOKENS, D), jnp.float32)
    for index_tp in range(N_TP):
        partial_sum = jnp.dot(attended[:, index_tp * head_cols:(index_tp + 1) * head_cols], out_weight[index_tp * head_cols:(index_tp + 1) * head_cols], preferred_element_type=jnp.float32)
        projected = projected + lax.optimization_barrier(partial_sum.astype(jnp.bfloat16)).astype(jnp.float32)
    after = (residual.astype(jnp.float32) + projected).astype(jnp.bfloat16)
    after_f = after.astype(jnp.float32)
    inv_rms = lax.rsqrt(lax.optimization_barrier(jnp.mean(after_f * after_f, axis=1, keepdims=True)) + norm_eps)
    normed = (after_f * inv_rms * norm_gain[None, :]).astype(jnp.bfloat16)
    gate_act = jnp.dot(normed, gate_weight, preferred_element_type=jnp.float32)
    up_act = jnp.dot(normed, up_weight, preferred_element_type=jnp.float32)
    hidden = (jax.nn.silu(gate_act) * up_act).astype(jnp.bfloat16)
    unit_cols = FF // N_TP
    down_sum = jnp.zeros((TOKENS, D), jnp.float32)
    for index_tp in range(N_TP):
        partial_sum = lax.dot_general(hidden[:, index_tp * unit_cols:(index_tp + 1) * unit_cols], down_weight[:, index_tp * unit_cols:(index_tp + 1) * unit_cols], (((1,), (1,)), ((), ())), preferred_element_type=jnp.float32)
        down_sum = down_sum + lax.optimization_barrier(partial_sum.astype(jnp.bfloat16)).astype(jnp.float32)
    return (after.astype(jnp.float32) + down_sum).astype(jnp.bfloat16)
```

```python
import functools

import jax
import jax.numpy as jnp
from jax import lax
from jax.experimental import pallas as pl
from jax.experimental.pallas import tpu as pltpu
from jax.sharding import PartitionSpec as P

HEAD_DIM = 64
WINDOW = 128
GROUP = 2


neg_big = -1e30
norm_eps = 1e-05


def from_behind(shard, axis, by):
    length = lax.axis_size(axis)
    pairs = [(i, i + by) for i in range(length) if 0 <= i + by < length]
    return lax.ppermute(shard, axis, pairs)


def attend(queries, keys, values, documents, sinks, tail_keys, tail_values, tail_docs, offset):
    rows_here = queries.shape[0]
    block_count = rows_here // WINDOW
    kv_here = keys.shape[1] // HEAD_DIM
    q_blocks = queries.reshape(block_count, WINDOW, kv_here, GROUP, HEAD_DIM)
    k_blocks = keys.reshape(block_count, WINDOW, kv_here, HEAD_DIM)
    v_blocks = values.reshape(block_count, WINDOW, kv_here, HEAD_DIM)
    k_prev = jnp.concatenate(
        [tail_keys.reshape(1, WINDOW, kv_here, HEAD_DIM), k_blocks[:-1]], axis=0
    )
    v_prev = jnp.concatenate(
        [tail_values.reshape(1, WINDOW, kv_here, HEAD_DIM), v_blocks[:-1]], axis=0
    )
    k_band = jnp.concatenate([k_prev, k_blocks], axis=1)
    v_band = jnp.concatenate([v_prev, v_blocks], axis=1)
    doc_own = documents.astype(jnp.float32).reshape(block_count, WINDOW)
    doc_prev = jnp.concatenate(
        [tail_docs.astype(jnp.float32).reshape(1, WINDOW), doc_own[:-1]], axis=0
    )
    doc_band = jnp.concatenate([doc_prev, doc_own], axis=1)
    row_idx = jnp.arange(WINDOW, dtype=jnp.int32)
    col_idx = jnp.arange(2 * WINDOW, dtype=jnp.int32)
    first = offset + jnp.arange(block_count, dtype=jnp.int32) * WINDOW
    q_pos = first[:, None] + row_idx[None, :]
    k_pos = first[:, None] - WINDOW + col_idx[None, :]
    distance = q_pos[:, :, None] - k_pos[:, None, :]
    visible = (
        (distance >= 0)
        & (distance < WINDOW)
        & (k_pos[:, None, :] >= 0)
        & (doc_own[:, :, None] == doc_band[:, None, :])
    )
    scores = jnp.einsum(
        "nikgd,njkd->nkgij", q_blocks, k_band, preferred_element_type=jnp.float32
    ) * HEAD_DIM ** (-0.5)
    scores = jnp.where(visible[:, None, None], scores, neg_big)
    sink_logit = sinks.reshape(1, kv_here, GROUP, 1, 1)
    row_max = jnp.maximum(scores.max(-1, keepdims=True), sink_logit)
    expo = jnp.where(visible[:, None, None], jnp.exp(scores - row_max), 0.0)
    denom_sum = expo.sum(-1, keepdims=True) + jnp.exp(sink_logit - row_max)
    weights = (expo / denom_sum).astype(jnp.bfloat16)
    mixed = jnp.einsum("nkgij,njkd->nikgd", weights, v_band, preferred_element_type=jnp.float32)
    return mixed.reshape(rows_here, kv_here * GROUP * HEAD_DIM).astype(jnp.bfloat16)


def on_device(
    residual,
    queries,
    keys,
    values,
    documents,
    sinks,
    out_weight,
    norm_gain,
    gate_weight,
    up_weight,
    down_weight,
):
    rows_here = queries.shape[0]
    offset = lax.axis_index("sp") * rows_here
    doc_tail = documents[rows_here - WINDOW :].astype(jnp.bfloat16)
    tail_keys, tail_values, tail_docs = from_behind(
        (keys[rows_here - WINDOW :], values[rows_here - WINDOW :], doc_tail), "sp", 1
    )
    attended = attend(
        queries, keys, values, documents, sinks, tail_keys, tail_values, tail_docs, offset
    )
    model_width = residual.shape[1]
    col_count = model_width // lax.axis_size("tp")
    col_first = lax.axis_index("tp") * col_count
    full_term = jnp.dot(attended, out_weight, preferred_element_type=jnp.float32)
    projected = lax.psum(full_term.astype(jnp.bfloat16), "tp").astype(jnp.float32)
    after_full = (residual.astype(jnp.float32) + projected).astype(jnp.bfloat16)
    after_f = after_full.astype(jnp.float32)
    inv_rms = lax.rsqrt(jnp.mean(after_f * after_f, axis=1, keepdims=True) + norm_eps)
    normed = (after_f * inv_rms * norm_gain[None, :]).astype(jnp.bfloat16)
    after = lax.dynamic_slice_in_dim(after_full, col_first, col_count, 1)
    gate_act = jnp.dot(
        normed,
        lax.all_gather(gate_weight, "sp", axis=0, tiled=True),
        preferred_element_type=jnp.float32,
    )
    up_act = jnp.dot(
        normed,
        lax.all_gather(up_weight, "sp", axis=0, tiled=True),
        preferred_element_type=jnp.float32,
    )
    down_full = lax.all_gather(down_weight, "sp", axis=0, tiled=True)
    hidden = (jax.nn.silu(gate_act) * up_act).astype(jnp.bfloat16)
    summed = lax.psum_scatter(
        lax.dot_general(
            down_full, hidden, (((1,), (1,)), ((), ())), preferred_element_type=jnp.float32
        ).astype(jnp.bfloat16),
        "tp",
        scatter_dimension=0,
        tiled=True,
    ).astype(jnp.float32)
    return (after.astype(jnp.float32) + summed.T).astype(jnp.bfloat16)


MESH = pl.DeviceIdType.MESH
NT = (((1,), (1,)), ((), ()))


def dot(a, b, dims=(((1,), (0,)), ((), ()))):
    return lax.dot_general(a, b, dims, preferred_element_type=jnp.float32)


def when(cond, f):
    if cond is None:
        f()
    else:
        pl.when(cond)(f)


def kernel(
    S, T, W, N,
    res_hbm, q_ref, k_ref, v_ref, doc_ref, sink_ref, ow_hbm, gain_ref, g_hbm, u_hbm, d_hbm,
    out_ref,
    G, kx, vx, dx, att, res_v, ow_v, after, normed, ga, ua, hidden, dsend, drecv, ysend, yrecv, zsend, zrecv, own_sum,
    w_send, w_recv, tail_send, tail_recv, loc, ow_send, ow_recv, att_send, att_recv, n_send, n_recv,
    d_send, d_recv, y_send, y_recv, z_send, z_recv,
):
    s = lax.axis_index("sp")
    t = lax.axis_index("tp")
    R = q_ref.shape[0]
    C = gain_ref.shape[2]
    D = T * C
    K = D // S
    F = g_hbm.shape[1]
    HK = K // 2
    PER = C // K
    z, x = s // 2, s % 2
    p, c = z % 2, t % 2
    wide = p == c
    n1_z, fr_z, ot_z = z + 1 - 2 * p, (z + 2) % 4, 3 - z
    xp = z * 2 + 1 - x
    n1, fr, ot = n1_z * 2 + x, fr_z * 2 + x, ot_z * 2 + x
    n1_x, fr_x, ot_x = n1_z * 2 + 1 - x, fr_z * 2 + 1 - x, ot_z * 2 + 1 - x
    mid = (z == 1) | (z == 2)
    outer = (z == 0) | (z == 3)
    tc = t + 1 - 2 * c
    ty = (t + 2) % T

    weights = (g_hbm, u_hbm, d_hbm)
    ow_parts = [
        pltpu.make_async_copy(ow_hbm.at[:, i * C:(i + 1) * C], ow_v.at[t, i], loc.at[3 + i]) for i in range(T)
    ]
    res_parts = [
        pltpu.make_async_copy(res_hbm.at[:, i * C:(i + 1) * C], res_v.at[i], loc.at[3 + T + i]) for i in range(T)
    ]
    for cp in ow_parts + res_parts:
        cp.start()

    def split(is_wide, cond, f):
        for flag, width in ((is_wide, W), (jnp.logical_not(is_wide), N)):
            both = flag if cond is None else flag & cond
            pl.when(both)(functools.partial(f, width))

    def columns(q, width):
        return pl.ds(pl.multiple_of(q * (F - width), 128), width)

    def local(m, width):
        return pltpu.make_async_copy(
            weights[m].at[:, columns(p, width)], G.at[m, s, :, pl.ds(0, width)], loc.at[m])

    for m in range(3):
        split(wide, None, lambda width: local(m, width).start())

    barrier = pltpu.get_barrier_semaphore()
    peers = [(xp, t, None), (fr, t, None), (n1, t, None), (ot, t, mid)]
    peers += [(s, (t + d) % T, None) for d in range(1, T)]
    peers += [((s + 1) % S, t, (x == 1) & (z < 3)), ((s + S - 1) % S, t, (x == 0) & (z > 0))]
    for a, b, cond in peers:
        when(cond, lambda: pl.semaphore_signal(barrier, inc=1, device_id=(a, b), device_id_type=MESH))
    present = sum(1 if cond is None else cond.astype(jnp.int32) for _, _, cond in peers)
    pl.semaphore_wait(barrier, present)

    finish = []

    def go(cond, cp):
        when(cond, cp.start)
        finish.append(lambda: when(cond, cp.wait_send))

    def remote(src, dst, send_sem, recv_sem, to):
        return pltpu.make_async_remote_copy(
            src_ref=src, dst_ref=dst, send_sem=send_sem, recv_sem=recv_sem, device_id=to, device_id_type=MESH)

    tails = []
    for i, (a, b) in enumerate((
        (k_ref.at[pl.ds(R - WINDOW, WINDOW)], kx.at[pl.ds(0, WINDOW)]),
        (v_ref.at[pl.ds(R - WINDOW, WINDOW)], vx.at[pl.ds(0, WINDOW)]),
        (doc_ref.at[pl.ds(doc_ref.shape[0] - 8, 8)], dx.at[pl.ds(0, 8)]),
    )):
        cp = remote(a, b, tail_send.at[i], tail_recv.at[i], ((s + 1) % S, t))
        go(s < S - 1, cp)
        tails.append(cp)

    count = [0]

    def weight(kind, m, h, src=None, cond=None):
        q, to = {
            "A": (1 - p, n1), "B": (p, fr), "C": (1 - p, ot), "D": (p, fr), "X": (p, xp),
        }[kind]
        rows = pl.ds(h * HK, HK)
        sem = w_send.at[count[0]]
        count[0] += 1

        def copy(width):
            part = pl.ds(0, width)
            if src is None:
                return remote(weights[m].at[rows, columns(q, width)], G.at[m, s, rows, part],
                              sem, w_recv.at[m, s, h], (to, t))
            place = G.at[m, src, rows, part]
            return remote(place, place, sem, w_recv.at[m, src, h], (to, t))

        split(q == c, cond, lambda width: copy(width).start())
        finish.append(lambda: split(q == c, cond, lambda width: copy(width).wait_send()))

    def recv(m, src, h):
        def wait(width):
            place = G.at[m, src, pl.ds(h * HK, HK), pl.ds(0, width)]
            remote(place, place, w_send.at[0], w_recv.at[m, src, h], (xp, t)).wait_recv()
        split(wide, None, wait)

    def landed(ref, sem):
        remote(ref, ref, w_send.at[0], sem, (s, tc)).wait_recv()

    GU = ((0, 0), (1, 0), (0, 1), (1, 1))
    DN = ((2, 0), (2, 1))

    for m, h in GU:
        weight("A", m, h)
        weight("X", m, h)
    for i in range(T):
        part = ow_hbm.at[:, i * C:(i + 1) * C]
        go(None, remote(part, ow_v.at[t, i], ow_send.at[0, i], ow_recv.at[t, i], (s, ty)))
        go(None, remote(part, ow_v.at[t, i], ow_send.at[1, i], ow_recv.at[t, i], (s, tc)))
    for m, h in GU[:2]:
        weight("C", m, h, cond=mid)
        weight("B", m, h)
    weight("C", 0, 1, cond=mid)
    weight("B", 0, 1)
    weight("B", 1, 1, cond=outer)

    @pl.when(jnp.logical_not(wide))
    def _():
        def clear(i, carry):
            for m in range(3):
                G[m, i, :, N:W] = jnp.zeros((K, W - N), jnp.bfloat16)
            return carry
        if W > N:
            lax.fori_loop(0, S, clear, 0)

    @pl.when(s == 0)
    def _():
        kx[pl.ds(0, WINDOW), :] = jnp.zeros((WINDOW, kx.shape[1]), jnp.bfloat16)
        vx[pl.ds(0, WINDOW), :] = jnp.zeros((WINDOW, vx.shape[1]), jnp.bfloat16)
        dx[pl.ds(0, 8), :] = jnp.zeros((8, dx.shape[1]), jnp.int32)

    kx[pl.ds(WINDOW, R), :] = k_ref[...]
    vx[pl.ds(WINDOW, R), :] = v_ref[...]
    dx[pl.ds(8, doc_ref.shape[0]), :] = doc_ref[...]
    for cp in tails:
        when(s > 0, cp.wait_recv)
    heads = q_ref.shape[1] // HEAD_DIM

    def block(b, carry):
        rows = pl.ds(pl.multiple_of(b * WINDOW, WINDOW), WINDOW)
        band = pl.ds(pl.multiple_of(b * WINDOW, WINDOW), 2 * WINDOW)
        prev = dx[pl.ds(pl.multiple_of(b * 8, 8), 8), :][0:1].astype(jnp.float32)
        own = dx[pl.ds(pl.multiple_of(b * 8 + 8, 8), 8), :][0:1].astype(jnp.float32)
        doc_q = jnp.broadcast_to(own, (WINDOW, WINDOW)).T
        i = lax.broadcasted_iota(jnp.int32, (WINDOW, WINDOW), 0)
        j = lax.broadcasted_iota(jnp.int32, (WINDOW, WINDOW), 1)
        first = s * R + b * WINDOW - WINDOW
        see_prev = (j > i) & (doc_q == prev) & (first + j >= 0)
        see_own = (j <= i) & (doc_q == own)
        visible = jnp.concatenate(
            [see_prev.astype(jnp.float32), see_own.astype(jnp.float32)], axis=1) > 0.5
        for h in range(heads):
            kv = h // GROUP
            cols = slice(kv * HEAD_DIM, (kv + 1) * HEAD_DIM)
            q = q_ref[rows, h * HEAD_DIM:(h + 1) * HEAD_DIM]
            scores = dot(q, kx[band, cols], NT) * HEAD_DIM ** (-0.5)
            scores = jnp.where(visible, scores, neg_big)
            sink = sink_ref[h]
            row_max = jnp.maximum(scores.max(-1, keepdims=True), sink)
            expo = jnp.where(visible, jnp.exp(scores - row_max), 0.0)
            total = expo.sum(-1, keepdims=True) + jnp.exp(sink - row_max)
            w = (expo / total).astype(jnp.bfloat16)
            att[t, rows, h * HEAD_DIM:(h + 1) * HEAD_DIM] = dot(w, vx[band, cols]).astype(jnp.bfloat16)
        return carry

    lax.fori_loop(0, R // WINDOW, block, 0)

    go(None, remote(att.at[t], att.at[t], att_send.at[0], att_recv.at[t], (s, ty)))
    go(None, remote(att.at[t], att.at[t], att_send.at[1], att_recv.at[t], (s, tc)))

    def ow_relay(i):
        landed(ow_v.at[ty, i], ow_recv.at[ty, i])
        go(None, remote(ow_v.at[ty, i], ow_v.at[ty, i], ow_send.at[2, i], ow_recv.at[ty, i], (s, tc)))

    ow_relay(0)
    for i, (m, h) in enumerate(GU):
        recv(m, n1, h)
        weight("X", m, h, src=n1)
        weight("D", m, h, src=n1, cond=mid)
        if i == 1:
            weight("C", 1, 1, cond=mid)
            weight("B", 1, 1, cond=mid)
        if i < 3:
            ow_relay(i + 1)
    for m, h in DN:
        weight("X", m, h)
        weight("C", m, h, cond=mid)
        weight("B", m, h, cond=mid)

    landed(att.at[ty], att_recv.at[ty])
    go(None, remote(att.at[ty], att.at[ty], att_send.at[2], att_recv.at[ty], (s, tc)))
    for cp in ow_parts + res_parts:
        cp.wait()
    td = (tc + 2) % T
    for g in (tc, td):
        for i in range(T):
            landed(ow_v.at[g, i], ow_recv.at[g, i])
        landed(att.at[g], att_recv.at[g])

    HR = R // 2
    for r in range(2):
        rows = slice(r * HR, (r + 1) * HR)

        def project(i, square):
            total = dot(att[0, rows, :], ow_v[0, i]).astype(jnp.bfloat16).astype(jnp.float32)
            for g in range(1, T):
                total += dot(att[g, rows, :], ow_v[g, i]).astype(jnp.bfloat16).astype(jnp.float32)
            value = (res_v[i, rows, :].astype(jnp.float32) + total).astype(jnp.bfloat16)
            after[i, rows, :] = value
            value = value.astype(jnp.float32)
            return square + (value * value).sum(-1, keepdims=True)

        square = lax.fori_loop(0, T, project, jnp.zeros((HR, 1), jnp.float32))
        inv = lax.rsqrt(square / D + norm_eps)

        def norm(i, carry):
            n = (after[i, rows, :].astype(jnp.float32) * inv * gain_ref[i]).astype(jnp.bfloat16)
            for j in range(PER):
                normed[i * PER + j, rows, :] = n[:, j * K:(j + 1) * K]
            return carry

        lax.fori_loop(0, T, norm, 0)
        go(None, remote(
            normed.at[pl.ds(t * PER, PER), pl.ds(r * HR, HR)],
            normed.at[pl.ds(t * PER, PER), pl.ds(R + r * HR, HR)],
            n_send.at[0, r], n_recv.at[t, r], (n1, t)))

    for m, h in DN:
        weight("A", m, h)
        weight("B", m, h, cond=outer)

    def passed(g, r):
        return normed.at[pl.ds(g * PER, PER), pl.ds(R + r * HR, HR)]

    TM = 256

    def gate_up(src, first, last, begin=False):
        def tile(r, carry):
            rows = pl.ds(pl.multiple_of(r * TM, TM), TM)
            a = normed[src, rows, :]
            for m, acc in ((0, ga), (1, ua)):
                value = dot(a, G[m, src])
                if begin:
                    acc[rows, :] = value
                else:
                    acc[rows, :] += value
            return carry
        lax.fori_loop(first // TM, last // TM, tile, 0)

    for m in range(3):
        split(wide, None, lambda width: local(m, width).wait())
    gate_up(s, 0, R, True)
    gate_up(n1, 0, R)
    for m, h in GU:
        recv(m, fr, h)
        weight("X", m, h, src=fr)
    for m, h in GU:
        recv(m, xp, h)
    gate_up(xp, 0, R)
    for r in range(2):
        landed(passed(t, r), n_recv.at[t, r])
        go(None, remote(passed(t, r), passed(t, r), n_send.at[1, r], n_recv.at[t, r], (s, ty)))
        go(None, remote(passed(t, r), passed(t, r), n_send.at[2, r], n_recv.at[t, r], (s, tc)))
    gate_up(fr, 0, R)
    for r in range(2):
        landed(passed(ty, r), n_recv.at[ty, r])
        go(None, remote(passed(ty, r), passed(ty, r), n_send.at[3, r], n_recv.at[ty, r], (s, tc)))
    for m, h in DN:
        recv(m, n1, h)
        weight("X", m, h, src=n1)
        weight("D", m, h, src=n1, cond=mid)
    for g in (tc, td):
        for r in range(2):
            landed(passed(g, r), n_recv.at[g, r])
    gate_up(s, R, 2 * R, True)
    for src in (n1, xp, fr):
        gate_up(src, R, 2 * R)
    for m, h in GU:
        recv(m, n1_x, h)
    gate_up(n1_x, 0, 2 * R)
    for m, h in GU:
        recv(m, ot, h)
        weight("X", m, h, src=ot)
    gate_up(ot, 0, 2 * R)
    for m, h in GU:
        recv(m, fr_x, h)
    gate_up(fr_x, 0, 2 * R)
    for m, h in DN:
        recv(m, fr, h)
        weight("X", m, h, src=fr)
    for m, h in GU:
        recv(m, ot_x, h)
    gate_up(ot_x, 0, 2 * R)

    def act(r, carry):
        rows = pl.ds(pl.multiple_of(r * 32, 32), 32)
        g = ga[rows, :]
        hidden[rows, :] = (g / (1.0 + jnp.exp(-g)) * ua[rows, :]).astype(jnp.bfloat16)
        return carry

    lax.fori_loop(0, 2 * R // 32, act, 0)

    def handed(k, r):
        return remote(dsend.at[k, r], drecv.at[k, r], d_send.at[k, r], d_recv.at[k, r], (s, tc))

    def across(k, r):
        j = k % PER
        return remote(ysend.at[j, r], yrecv.at[j, r], y_send.at[j, r], y_recv.at[j, r], (s, ty))

    def back(k):
        j = k % PER
        return remote(zsend.at[j], zrecv.at[j], z_send.at[j], z_recv.at[j], (n1, t))

    def down(k):
        keep = (k // PER) % 2 == c
        for r in (1, 0):
            value = dot(hidden[r * R:(r + 1) * R, :], G[2, k], NT).astype(jnp.bfloat16)
            dsend[k, r] = value
            pl.when(jnp.logical_not(keep))(lambda: handed(k, r).start())
        finish.append(lambda: pl.when(jnp.logical_not(keep))(
            lambda: [handed(k, r).wait_send() for r in (1, 0)] and None))

    def pair(k, r):
        landed(drecv.at[k, r], d_recv.at[k, r])
        return dsend[k, r].astype(jnp.float32) + drecv[k, r].astype(jnp.float32)

    def cross(k):
        @pl.when(k // PER == ty)
        def _():
            for r in (1, 0):
                ysend[k % PER, r] = pair(k, r).astype(jnp.bfloat16)
                across(k, r).start()

    def settle(k):
        @pl.when(k // PER == t)
        def _():
            j = k % PER
            for r in (1, 0):
                total = pair(k, r)
                landed(yrecv.at[j, r], y_recv.at[j, r])
                total += yrecv[j, r].astype(jnp.float32)
                if r == 1:
                    zsend[j] = total.astype(jnp.bfloat16)
                    back(k).start()
                else:
                    own_sum[j] = total

    order = (s, n1, xp, fr, n1_x, ot, fr_x, ot_x)
    for n, k in enumerate(order):
        if n == 3:
            pass
        elif k is ot:
            for m, h in DN:
                recv(m, k, h)
                weight("X", m, h, src=k)
        elif n in (2, 4, 6, 7):
            for m, h in DN:
                recv(m, k, h)
        down(k)
        if n >= 1:
            cross(order[n - 1])
        if n >= 2:
            settle(order[n - 2])
    cross(order[-1])
    settle(order[-2])
    settle(order[-1])

    for j in range(PER):
        landed(zrecv.at[j], z_recv.at[j])
        cols = slice(j * K, (j + 1) * K)
        out_ref[:, cols] = (
            after[t, :, cols].astype(jnp.float32) + (own_sum[j] + zrecv[j].astype(jnp.float32))
        ).astype(jnp.bfloat16)

    for f in finish:
        f()
    for j in range(PER):
        back(j).wait_send()
        for r in (0, 1):
            across(j, r).wait_send()


def fused(residual, queries, keys, values, documents, sinks, out_weight, norm_gain, gate_weight, up_weight, down_weight):
    S, T = lax.axis_size("sp"), lax.axis_size("tp")
    R, D = residual.shape
    F = gate_weight.shape[1]
    C, K = D // T, D // S
    W = (F // 128 + 1) // 2 * 128
    N = F - W
    PER = C // K
    blocks = R // WINDOW
    docs = jnp.broadcast_to(documents.reshape(blocks, 1, WINDOW), (blocks, 8, WINDOW)).reshape(blocks * 8, WINDOW)
    bf, f32 = jnp.bfloat16, jnp.float32
    vm, hbm = pl.BlockSpec(memory_space=pltpu.VMEM), pl.BlockSpec(memory_space=pl.ANY)
    dma = pltpu.SemaphoreType.DMA
    scratch = [
        pltpu.VMEM((3, S, K, W), bf),
        pltpu.VMEM((R + WINDOW, keys.shape[1]), bf),
        pltpu.VMEM((R + WINDOW, keys.shape[1]), bf),
        pltpu.VMEM((blocks * 8 + 8, WINDOW), jnp.int32),
        pltpu.VMEM((T, R, queries.shape[1]), bf),
        pltpu.VMEM((T, R, C), bf),
        pltpu.VMEM((T, T, out_weight.shape[0], C), bf),
        pltpu.VMEM((T, R, C), bf),
        pltpu.VMEM((S, 2 * R, K), bf),
        pltpu.VMEM((2 * R, W), f32),
        pltpu.VMEM((2 * R, W), f32),
        pltpu.VMEM((2 * R, W), bf),
        pltpu.VMEM((S, 2, R, K), bf),
        pltpu.VMEM((S, 2, R, K), bf),
        pltpu.VMEM((PER, 2, R, K), bf),
        pltpu.VMEM((PER, 2, R, K), bf),
        pltpu.VMEM((PER, R, K), bf),
        pltpu.VMEM((PER, R, K), bf),
        pltpu.VMEM((PER, R, K), f32),
        dma((64,)), dma((3, S, 2)), dma((3,)), dma((3,)), dma((3 + 2 * T,)),
        dma((3, T)), dma((T, T)), dma((3,)), dma((T,)), dma((4, 2)), dma((T, 2)),
        dma((S, 2)), dma((S, 2)), dma((PER, 2)), dma((PER, 2)), dma((PER,)), dma((PER,)),
    ]
    return pl.pallas_call(
        functools.partial(kernel, S, T, W, N),
        out_shape=jax.ShapeDtypeStruct((R, C), bf),
        in_specs=[hbm, vm, vm, vm, vm, pl.BlockSpec(memory_space=pltpu.SMEM), hbm, vm, hbm, hbm, hbm],
        out_specs=vm,
        scratch_shapes=scratch,
        compiler_params=pltpu.CompilerParams(
            collective_id=0, has_side_effects=True, vmem_limit_bytes=60 * 2**20),
    )(residual, queries, keys, values, docs, sinks, out_weight, norm_gain.reshape(T, 1, C),
      gate_weight, up_weight, down_weight)


def line_of_four_pairs(mesh):
    return mesh.shape["sp"] == 8 and mesh.shape["tp"] == 4


def solution(mesh):
    return jax.shard_map(
        fused if line_of_four_pairs(mesh) else on_device,
        mesh=mesh,
        in_specs=(
            P("sp", None),
            P("sp", "tp"),
            P("sp", "tp"),
            P("sp", "tp"),
            P("sp"),
            P("tp"),
            P("tp", None),
            P(),
            P("sp", "tp"),
            P("sp", "tp"),
            P("sp", "tp"),
        ),
        out_specs=P("sp", "tp"),
        check_vma=False,
    )
```

```python
import functools

import jax
import jax.numpy as jnp
from jax import lax
from jax.experimental import pallas as pl
from jax.experimental.pallas import tpu as pltpu
from jax.sharding import PartitionSpec as P

HEAD_DIM = 64
WINDOW = 128
GROUP = 2


neg_big = -1e30
norm_eps = 1e-05


def from_behind(shard, axis, by):
    length = lax.axis_size(axis)
    pairs = [(i, i + by) for i in range(length) if 0 <= i + by < length]
    return lax.ppermute(shard, axis, pairs)


def attend(queries, keys, values, documents, sinks, tail_keys, tail_values, tail_docs, offset):
    rows_here = queries.shape[0]
    block_count = rows_here // WINDOW
    kv_here = keys.shape[1] // HEAD_DIM
    q_blocks = queries.reshape(block_count, WINDOW, kv_here, GROUP, HEAD_DIM)
    k_blocks = keys.reshape(block_count, WINDOW, kv_here, HEAD_DIM)
    v_blocks = values.reshape(block_count, WINDOW, kv_here, HEAD_DIM)
    k_prev = jnp.concatenate(
        [tail_keys.reshape(1, WINDOW, kv_here, HEAD_DIM), k_blocks[:-1]], axis=0
    )
    v_prev = jnp.concatenate(
        [tail_values.reshape(1, WINDOW, kv_here, HEAD_DIM), v_blocks[:-1]], axis=0
    )
    k_band = jnp.concatenate([k_prev, k_blocks], axis=1)
    v_band = jnp.concatenate([v_prev, v_blocks], axis=1)
    doc_own = documents.astype(jnp.float32).reshape(block_count, WINDOW)
    doc_prev = jnp.concatenate(
        [tail_docs.astype(jnp.float32).reshape(1, WINDOW), doc_own[:-1]], axis=0
    )
    doc_band = jnp.concatenate([doc_prev, doc_own], axis=1)
    row_idx = jnp.arange(WINDOW, dtype=jnp.int32)
    col_idx = jnp.arange(2 * WINDOW, dtype=jnp.int32)
    first = offset + jnp.arange(block_count, dtype=jnp.int32) * WINDOW
    q_pos = first[:, None] + row_idx[None, :]
    k_pos = first[:, None] - WINDOW + col_idx[None, :]
    distance = q_pos[:, :, None] - k_pos[:, None, :]
    visible = (
        (distance >= 0)
        & (distance < WINDOW)
        & (k_pos[:, None, :] >= 0)
        & (doc_own[:, :, None] == doc_band[:, None, :])
    )
    scores = jnp.einsum(
        "nikgd,njkd->nkgij", q_blocks, k_band, preferred_element_type=jnp.float32
    ) * HEAD_DIM ** (-0.5)
    scores = jnp.where(visible[:, None, None], scores, neg_big)
    sink_logit = sinks.reshape(1, kv_here, GROUP, 1, 1)
    row_max = jnp.maximum(scores.max(-1, keepdims=True), sink_logit)
    expo = jnp.where(visible[:, None, None], jnp.exp(scores - row_max), 0.0)
    denom_sum = expo.sum(-1, keepdims=True) + jnp.exp(sink_logit - row_max)
    weights = (expo / denom_sum).astype(jnp.bfloat16)
    mixed = jnp.einsum("nkgij,njkd->nikgd", weights, v_band, preferred_element_type=jnp.float32)
    return mixed.reshape(rows_here, kv_here * GROUP * HEAD_DIM).astype(jnp.bfloat16)


def on_device(
    residual,
    queries,
    keys,
    values,
    documents,
    sinks,
    out_weight,
    norm_gain,
    gate_weight,
    up_weight,
    down_weight,
):
    rows_here = queries.shape[0]
    offset = lax.axis_index("sp") * rows_here
    doc_tail = documents[rows_here - WINDOW :].astype(jnp.bfloat16)
    tail_keys, tail_values, tail_docs = from_behind(
        (keys[rows_here - WINDOW :], values[rows_here - WINDOW :], doc_tail), "sp", 1
    )
    attended = attend(
        queries, keys, values, documents, sinks, tail_keys, tail_values, tail_docs, offset
    )
    model_width = residual.shape[1]
    col_count = model_width // lax.axis_size("tp")
    col_first = lax.axis_index("tp") * col_count
    full_term = jnp.dot(attended, out_weight, preferred_element_type=jnp.float32)
    projected = lax.psum(full_term.astype(jnp.bfloat16), "tp").astype(jnp.float32)
    after_full = (residual.astype(jnp.float32) + projected).astype(jnp.bfloat16)
    after_f = after_full.astype(jnp.float32)
    inv_rms = lax.rsqrt(jnp.mean(after_f * after_f, axis=1, keepdims=True) + norm_eps)
    normed = (after_f * inv_rms * norm_gain[None, :]).astype(jnp.bfloat16)
    after = lax.dynamic_slice_in_dim(after_full, col_first, col_count, 1)
    gate_act = jnp.dot(
        normed,
        lax.all_gather(gate_weight, "sp", axis=0, tiled=True),
        preferred_element_type=jnp.float32,
    )
    up_act = jnp.dot(
        normed,
        lax.all_gather(up_weight, "sp", axis=0, tiled=True),
        preferred_element_type=jnp.float32,
    )
    down_full = lax.all_gather(down_weight, "sp", axis=0, tiled=True)
    hidden = (jax.nn.silu(gate_act) * up_act).astype(jnp.bfloat16)
    summed = lax.psum_scatter(
        lax.dot_general(
            down_full, hidden, (((1,), (1,)), ((), ())), preferred_element_type=jnp.float32
        ).astype(jnp.bfloat16),
        "tp",
        scatter_dimension=0,
        tiled=True,
    ).astype(jnp.float32)
    return (after.astype(jnp.float32) + summed.T).astype(jnp.bfloat16)


MESH = pl.DeviceIdType.MESH
NT = (((1,), (1,)), ((), ()))


def dot(a, b, dims=(((1,), (0,)), ((), ()))):
    return lax.dot_general(a, b, dims, preferred_element_type=jnp.float32)


def when(cond, f):
    if cond is None:
        f()
    else:
        pl.when(cond)(f)


def kernel(
    S, T, W, N,
    res_hbm, q_ref, k_ref, v_ref, doc_ref, sink_ref, ow_hbm, gain_ref, g_hbm, u_hbm, d_hbm,
    out_ref,
    G, kx, vx, dx, att, res_v, ow_v, after, normed, ga, ua, hidden, dsend, drecv, ysend, yrecv, zsend, zrecv, own_sum,
    w_send, w_recv, tail_send, tail_recv, loc, ow_send, ow_recv, att_send, att_recv, n_send, n_recv,
    d_send, d_recv, y_send, y_recv, z_send, z_recv,
):
    s = lax.axis_index("sp")
    t = lax.axis_index("tp")
    R = q_ref.shape[0]
    C = gain_ref.shape[2]
    D = T * C
    K = D // S
    F = g_hbm.shape[1]
    HK = K // 2
    PER = C // K
    z, x = s // 2, s % 2
    p, c = z % 2, t % 2
    wide = p == c
    n1_z, fr_z, ot_z = z + 1 - 2 * p, (z + 2) % 4, 3 - z
    xp = z * 2 + 1 - x
    n1, fr, ot = n1_z * 2 + x, fr_z * 2 + x, ot_z * 2 + x
    n1_x, fr_x, ot_x = n1_z * 2 + 1 - x, fr_z * 2 + 1 - x, ot_z * 2 + 1 - x
    mid = (z == 1) | (z == 2)
    one, two = jnp.where(mid, fr, ot), jnp.where(mid, ot, fr)
    one_x, two_x = jnp.where(mid, fr_x, ot_x), jnp.where(mid, ot_x, fr_x)
    outer = (z == 0) | (z == 3)
    tc = t + 1 - 2 * c
    ty = (t + 2) % T

    weights = (g_hbm, u_hbm, d_hbm)
    ow_parts = [
        pltpu.make_async_copy(ow_hbm.at[:, i * C:(i + 1) * C], ow_v.at[t, i], loc.at[3 + i]) for i in range(T)
    ]
    res_parts = [
        pltpu.make_async_copy(res_hbm.at[:, i * C:(i + 1) * C], res_v.at[i], loc.at[3 + T + i]) for i in range(T)
    ]
    for cp in ow_parts + res_parts:
        cp.start()

    def split(is_wide, cond, f):
        for flag, width in ((is_wide, W), (jnp.logical_not(is_wide), N)):
            both = flag if cond is None else flag & cond
            pl.when(both)(functools.partial(f, width))

    def columns(q, width):
        return pl.ds(pl.multiple_of(q * (F - width), 128), width)

    def local(m, width):
        return pltpu.make_async_copy(
            weights[m].at[:, columns(p, width)], G.at[m, s, :, pl.ds(0, width)], loc.at[m])

    for m in range(3):
        split(wide, None, lambda width: local(m, width).start())

    barrier = pltpu.get_barrier_semaphore()
    peers = [(xp, t, None), (fr, t, None), (n1, t, None), (ot, t, mid)]
    peers += [(s, (t + d) % T, None) for d in range(1, T)]
    peers += [((s + 1) % S, t, (x == 1) & (z < 3)), ((s + S - 1) % S, t, (x == 0) & (z > 0))]
    for a, b, cond in peers:
        when(cond, lambda: pl.semaphore_signal(barrier, inc=1, device_id=(a, b), device_id_type=MESH))
    present = sum(1 if cond is None else cond.astype(jnp.int32) for _, _, cond in peers)
    pl.semaphore_wait(barrier, present)

    finish = []

    def go(cond, cp):
        when(cond, cp.start)
        finish.append(lambda: when(cond, cp.wait_send))

    def remote(src, dst, send_sem, recv_sem, to):
        return pltpu.make_async_remote_copy(
            src_ref=src, dst_ref=dst, send_sem=send_sem, recv_sem=recv_sem, device_id=to, device_id_type=MESH)

    tails = []
    for i, (a, b) in enumerate((
        (k_ref.at[pl.ds(R - WINDOW, WINDOW)], kx.at[pl.ds(0, WINDOW)]),
        (v_ref.at[pl.ds(R - WINDOW, WINDOW)], vx.at[pl.ds(0, WINDOW)]),
        (doc_ref.at[pl.ds(doc_ref.shape[0] - 8, 8)], dx.at[pl.ds(0, 8)]),
    )):
        cp = remote(a, b, tail_send.at[i], tail_recv.at[i], ((s + 1) % S, t))
        go(s < S - 1, cp)
        tails.append(cp)

    count = [0]

    def weight(kind, m, h, src=None, cond=None):
        q, to = {
            "A": (1 - p, n1), "B": (p, fr), "C": (1 - p, ot), "D": (p, fr), "X": (p, xp),
        }[kind]
        rows = pl.ds(h * HK, HK)
        sem = w_send.at[count[0]]
        count[0] += 1

        def copy(width):
            part = pl.ds(0, width)
            if src is None:
                return remote(weights[m].at[rows, columns(q, width)], G.at[m, s, rows, part],
                              sem, w_recv.at[m, s, h], (to, t))
            place = G.at[m, src, rows, part]
            return remote(place, place, sem, w_recv.at[m, src, h], (to, t))

        split(q == c, cond, lambda width: copy(width).start())
        finish.append(lambda: split(q == c, cond, lambda width: copy(width).wait_send()))

    def recv(m, src, h, cond=None):
        def wait(width):
            place = G.at[m, src, pl.ds(h * HK, HK), pl.ds(0, width)]
            remote(place, place, w_send.at[0], w_recv.at[m, src, h], (xp, t)).wait_recv()
        split(wide, cond, wait)

    def landed(ref, sem):
        remote(ref, ref, w_send.at[0], sem, (s, tc)).wait_recv()

    GU = ((0, 0), (1, 0), (0, 1), (1, 1))
    DN = ((2, 0), (2, 1))

    for m, h in GU:
        weight("A", m, h)
        weight("X", m, h)
    for i in range(T):
        part = ow_hbm.at[:, i * C:(i + 1) * C]
        go(None, remote(part, ow_v.at[t, i], ow_send.at[0, i], ow_recv.at[t, i], (s, ty)))
        go(None, remote(part, ow_v.at[t, i], ow_send.at[1, i], ow_recv.at[t, i], (s, tc)))
    for m, h in DN:
        weight("A", m, h, cond=mid)
    for m, h in GU[:2]:
        weight("C", m, h, cond=mid)
        weight("B", m, h)
    for m, h in GU[2:]:
        weight("B", m, h, cond=outer)

    @pl.when(jnp.logical_not(wide))
    def _():
        def clear(i, carry):
            for m in range(3):
                G[m, i, :, N:W] = jnp.zeros((K, W - N), jnp.bfloat16)
            return carry
        if W > N:
            lax.fori_loop(0, S, clear, 0)

    @pl.when(s == 0)
    def _():
        kx[pl.ds(0, WINDOW), :] = jnp.zeros((WINDOW, kx.shape[1]), jnp.bfloat16)
        vx[pl.ds(0, WINDOW), :] = jnp.zeros((WINDOW, vx.shape[1]), jnp.bfloat16)
        dx[pl.ds(0, 8), :] = jnp.zeros((8, dx.shape[1]), jnp.int32)

    kx[pl.ds(WINDOW, R), :] = k_ref[...]
    vx[pl.ds(WINDOW, R), :] = v_ref[...]
    dx[pl.ds(8, doc_ref.shape[0]), :] = doc_ref[...]
    for cp in tails:
        when(s > 0, cp.wait_recv)
    heads = q_ref.shape[1] // HEAD_DIM

    def block(b, carry):
        rows = pl.ds(pl.multiple_of(b * WINDOW, WINDOW), WINDOW)
        band = pl.ds(pl.multiple_of(b * WINDOW, WINDOW), 2 * WINDOW)
        prev = dx[pl.ds(pl.multiple_of(b * 8, 8), 8), :][0:1].astype(jnp.float32)
        own = dx[pl.ds(pl.multiple_of(b * 8 + 8, 8), 8), :][0:1].astype(jnp.float32)
        doc_q = jnp.broadcast_to(own, (WINDOW, WINDOW)).T
        i = lax.broadcasted_iota(jnp.int32, (WINDOW, WINDOW), 0)
        j = lax.broadcasted_iota(jnp.int32, (WINDOW, WINDOW), 1)
        first = s * R + b * WINDOW - WINDOW
        see_prev = (j > i) & (doc_q == prev) & (first + j >= 0)
        see_own = (j <= i) & (doc_q == own)
        visible = jnp.concatenate(
            [see_prev.astype(jnp.float32), see_own.astype(jnp.float32)], axis=1) > 0.5
        for h in range(heads):
            kv = h // GROUP
            cols = slice(kv * HEAD_DIM, (kv + 1) * HEAD_DIM)
            q = q_ref[rows, h * HEAD_DIM:(h + 1) * HEAD_DIM]
            scores = dot(q, kx[band, cols], NT) * HEAD_DIM ** (-0.5)
            scores = jnp.where(visible, scores, neg_big)
            sink = sink_ref[h]
            row_max = jnp.maximum(scores.max(-1, keepdims=True), sink)
            expo = jnp.where(visible, jnp.exp(scores - row_max), 0.0)
            total = expo.sum(-1, keepdims=True) + jnp.exp(sink - row_max)
            w = (expo / total).astype(jnp.bfloat16)
            att[t, rows, h * HEAD_DIM:(h + 1) * HEAD_DIM] = dot(w, vx[band, cols]).astype(jnp.bfloat16)
        return carry

    lax.fori_loop(0, R // WINDOW, block, 0)

    go(None, remote(att.at[t], att.at[t], att_send.at[0], att_recv.at[t], (s, ty)))
    go(None, remote(att.at[t], att.at[t], att_send.at[1], att_recv.at[t], (s, tc)))

    def ow_relay(i):
        landed(ow_v.at[ty, i], ow_recv.at[ty, i])
        go(None, remote(ow_v.at[ty, i], ow_v.at[ty, i], ow_send.at[2, i], ow_recv.at[ty, i], (s, tc)))

    def pass_on(m, h, src, cond=None):
        recv(m, src, h, cond)
        weight("X", m, h, src=src, cond=cond)

    pass_on(0, 0, n1)
    weight("D", 0, 0, src=n1, cond=mid)
    for m, h in (GU[2], GU[3], DN[0]):
        weight("C", m, h, cond=mid)
    pass_on(1, 0, n1)
    weight("D", 1, 0, src=n1, cond=mid)
    weight("B", 0, 1, cond=mid)
    ow_relay(0)
    pass_on(0, 0, ot, mid)
    pass_on(0, 0, fr, outer)
    ow_relay(1)
    pass_on(0, 1, n1)
    weight("D", 0, 1, src=n1, cond=mid)
    weight("B", 1, 1, cond=mid)
    pass_on(1, 1, n1)
    weight("D", 1, 1, src=n1, cond=mid)
    ow_relay(2)
    pass_on(1, 0, ot, mid)
    pass_on(1, 0, fr, outer)
    ow_relay(3)
    landed(att.at[ty], att_recv.at[ty])
    go(None, remote(att.at[ty], att.at[ty], att_send.at[2], att_recv.at[ty], (s, tc)))
    for cp in ow_parts + res_parts:
        cp.wait()
    td = (tc + 2) % T
    for g in (tc, td):
        for i in range(T):
            landed(ow_v.at[g, i], ow_recv.at[g, i])
        landed(att.at[g], att_recv.at[g])

    HR = R // 2
    for r in range(2):
        rows = slice(r * HR, (r + 1) * HR)

        def project(i, square):
            total = dot(att[0, rows, :], ow_v[0, i]).astype(jnp.bfloat16).astype(jnp.float32)
            for g in range(1, T):
                total += dot(att[g, rows, :], ow_v[g, i]).astype(jnp.bfloat16).astype(jnp.float32)
            value = (res_v[i, rows, :].astype(jnp.float32) + total).astype(jnp.bfloat16)
            after[i, rows, :] = value
            value = value.astype(jnp.float32)
            return square + (value * value).sum(-1, keepdims=True)

        square = lax.fori_loop(0, T, project, jnp.zeros((HR, 1), jnp.float32))
        inv = lax.rsqrt(square / D + norm_eps)

        def norm(i, carry):
            n = (after[i, rows, :].astype(jnp.float32) * inv * gain_ref[i]).astype(jnp.bfloat16)
            for j in range(PER):
                normed[i * PER + j, rows, :] = n[:, j * K:(j + 1) * K]
            return carry

        lax.fori_loop(0, T, norm, 0)
        go(None, remote(
            normed.at[pl.ds(t * PER, PER), pl.ds(r * HR, HR)],
            normed.at[pl.ds(t * PER, PER), pl.ds(R + r * HR, HR)],
            n_send.at[0, r], n_recv.at[t, r], (n1, t)))

    for m, h in DN:
        weight("A", m, h, cond=outer)

    def passed(g, r):
        return normed.at[pl.ds(g * PER, PER), pl.ds(R + r * HR, HR)]

    TM = 256

    def gate_up(src, first, last, begin=False):
        def tile(r, carry):
            rows = pl.ds(pl.multiple_of(r * TM, TM), TM)
            a = normed[src, rows, :]
            for m, acc in ((0, ga), (1, ua)):
                value = dot(a, G[m, src])
                if begin:
                    acc[rows, :] = value
                else:
                    acc[rows, :] += value
            return carry
        lax.fori_loop(first // TM, last // TM, tile, 0)

    for m in range(3):
        split(wide, None, lambda width: local(m, width).wait())
    for m, h in GU:
        pass_on(m, h, fr, mid)
    for m, h in DN:
        weight("X", m, h, cond=outer)
    gate_up(s, 0, R, True)
    gate_up(n1, 0, R)
    pass_on(0, 0, ot, outer)
    for src in (xp, n1_x):
        for m, h in GU:
            recv(m, src, h)
        gate_up(src, 0, R)
    pass_on(0, 1, ot, mid)
    for r in range(2):
        landed(passed(t, r), n_recv.at[t, r])
        go(None, remote(passed(t, r), passed(t, r), n_send.at[1, r], n_recv.at[t, r], (s, ty)))
        go(None, remote(passed(t, r), passed(t, r), n_send.at[2, r], n_recv.at[t, r], (s, tc)))
    pass_on(1, 1, ot, mid)
    for m, h in DN:
        weight("X", m, h, cond=mid)
    pass_on(1, 0, ot, outer)
    for r in range(2):
        landed(passed(ty, r), n_recv.at[ty, r])
        go(None, remote(passed(ty, r), passed(ty, r), n_send.at[3, r], n_recv.at[ty, r], (s, tc)))
    for m, h in DN:
        recv(m, n1, h, mid)
        weight("X", m, h, src=n1, cond=mid)
        weight("D", m, h, src=n1, cond=mid)
        weight("B", m, h, cond=mid)
        if h == 0:
            weight("C", 2, 1, cond=mid)
    pass_on(0, 1, fr, outer)
    for g in (tc, td):
        for r in range(2):
            landed(passed(g, r), n_recv.at[g, r])
    gate_up(s, R, 2 * R, True)
    gate_up(n1, R, 2 * R)
    pass_on(0, 1, ot, outer)
    gate_up(xp, R, 2 * R)
    gate_up(n1_x, R, 2 * R)
    pass_on(1, 1, fr, outer)
    gate_up(fr, 0, 2 * R)
    pass_on(1, 1, ot, outer)
    for m, h in DN:
        weight("B", m, h, cond=outer)
        pass_on(m, h, n1, outer)
    gate_up(ot, 0, 2 * R)
    for m, h in GU:
        recv(m, fr_x, h)
    gate_up(fr_x, 0, 2 * R)
    for m, h in GU:
        recv(m, ot_x, h)
    gate_up(ot_x, 0, 2 * R)

    def act(r, carry):
        rows = pl.ds(pl.multiple_of(r * 32, 32), 32)
        g = ga[rows, :]
        hidden[rows, :] = (g / (1.0 + jnp.exp(-g)) * ua[rows, :]).astype(jnp.bfloat16)
        return carry

    lax.fori_loop(0, 2 * R // 32, act, 0)

    def handed(k, r):
        return remote(dsend.at[k, r], drecv.at[k, r], d_send.at[k, r], d_recv.at[k, r], (s, tc))

    def across(j):
        return remote(ysend.at[j], yrecv.at[j], y_send.at[j], y_recv.at[j], (s, ty))

    def back(k):
        return remote(zsend.at[k], zrecv.at[k], z_send.at[k], z_recv.at[k], (n1, t))

    def kept(k):
        return (k // PER) % 2 == c

    def down(k):
        keep = kept(k)
        for r in (1, 0):
            value = dot(hidden[r * R:(r + 1) * R, :], G[2, k], NT).astype(jnp.bfloat16)
            dsend[k, r] = value
            pl.when(jnp.logical_not(keep))(lambda: handed(k, r).start())
        finish.append(lambda: pl.when(jnp.logical_not(keep))(
            lambda: [handed(k, r).wait_send() for r in (1, 0)] and None))

    def pair(k, r):
        landed(drecv.at[k, r], d_recv.at[k, r])
        return dsend[k, r].astype(jnp.float32) + drecv[k, r].astype(jnp.float32)

    def cross(k):
        @pl.when(kept(k))
        def _():
            zsend[k] = pair(k, 1).astype(jnp.bfloat16)
            back(k).start()
        finish.append(lambda: pl.when(kept(k))(lambda: back(k).wait_send()))

    def settle(k):
        @pl.when(kept(k))
        def _():
            j = k % PER
            total = pair(k, 0)
            landed(zrecv.at[k], z_recv.at[k])
            total += zrecv[k].astype(jnp.float32)

            @pl.when(k // PER == t)
            def _():
                own_sum[j] = total

            @pl.when(k // PER == ty)
            def _():
                ysend[j] = total.astype(jnp.bfloat16)
                across(j).start()

    order = (s, n1, xp, n1_x, one, two, one_x, two_x)
    down(order[0])
    down(order[1])
    cross(order[0])
    pass_on(2, 0, ot)
    for m, h in DN:
        recv(m, xp, h)
    down(order[2])
    cross(order[1])
    pass_on(2, 0, fr)
    for m, h in DN:
        recv(m, n1_x, h)
    down(order[3])
    cross(order[2])
    pass_on(2, 1, one)
    down(order[4])
    cross(order[3])
    pass_on(2, 1, two)
    down(order[5])
    cross(order[4])
    settle(order[0])
    settle(order[1])
    for m, h in DN:
        recv(m, one_x, h)
    down(order[6])
    cross(order[5])
    settle(order[2])
    settle(order[3])
    for m, h in DN:
        recv(m, two_x, h)
    down(order[7])
    cross(order[6])
    cross(order[7])
    settle(order[4])
    settle(order[5])
    settle(order[6])
    settle(order[7])

    for j in range(PER):
        landed(yrecv.at[j], y_recv.at[j])
        cols = slice(j * K, (j + 1) * K)
        out_ref[:, cols] = (
            after[t, :, cols].astype(jnp.float32) + (own_sum[j] + yrecv[j].astype(jnp.float32))
        ).astype(jnp.bfloat16)

    for f in finish:
        f()
    for j in range(PER):
        across(j).wait_send()


def fused(residual, queries, keys, values, documents, sinks, out_weight, norm_gain, gate_weight, up_weight, down_weight):
    S, T = lax.axis_size("sp"), lax.axis_size("tp")
    R, D = residual.shape
    F = gate_weight.shape[1]
    C, K = D // T, D // S
    W = (F // 128 + 1) // 2 * 128
    N = F - W
    PER = C // K
    blocks = R // WINDOW
    docs = jnp.broadcast_to(documents.reshape(blocks, 1, WINDOW), (blocks, 8, WINDOW)).reshape(blocks * 8, WINDOW)
    bf, f32 = jnp.bfloat16, jnp.float32
    vm, hbm = pl.BlockSpec(memory_space=pltpu.VMEM), pl.BlockSpec(memory_space=pl.ANY)
    dma = pltpu.SemaphoreType.DMA
    scratch = [
        pltpu.VMEM((3, S, K, W), bf),
        pltpu.VMEM((R + WINDOW, keys.shape[1]), bf),
        pltpu.VMEM((R + WINDOW, keys.shape[1]), bf),
        pltpu.VMEM((blocks * 8 + 8, WINDOW), jnp.int32),
        pltpu.VMEM((T, R, queries.shape[1]), bf),
        pltpu.VMEM((T, R, C), bf),
        pltpu.VMEM((T, T, out_weight.shape[0], C), bf),
        pltpu.VMEM((T, R, C), bf),
        pltpu.VMEM((S, 2 * R, K), bf),
        pltpu.VMEM((2 * R, W), f32),
        pltpu.VMEM((2 * R, W), f32),
        pltpu.VMEM((2 * R, W), bf),
        pltpu.VMEM((S, 2, R, K), bf),
        pltpu.VMEM((S, 2, R, K), bf),
        pltpu.VMEM((PER, R, K), bf),
        pltpu.VMEM((PER, R, K), bf),
        pltpu.VMEM((S, R, K), bf),
        pltpu.VMEM((S, R, K), bf),
        pltpu.VMEM((PER, R, K), f32),
        dma((96,)), dma((3, S, 2)), dma((3,)), dma((3,)), dma((3 + 2 * T,)),
        dma((3, T)), dma((T, T)), dma((3,)), dma((T,)), dma((4, 2)), dma((T, 2)),
        dma((S, 2)), dma((S, 2)), dma((PER,)), dma((PER,)), dma((S,)), dma((S,)),
    ]
    return pl.pallas_call(
        functools.partial(kernel, S, T, W, N),
        out_shape=jax.ShapeDtypeStruct((R, C), bf),
        in_specs=[hbm, vm, vm, vm, vm, pl.BlockSpec(memory_space=pltpu.SMEM), hbm, vm, hbm, hbm, hbm],
        out_specs=vm,
        scratch_shapes=scratch,
        compiler_params=pltpu.CompilerParams(
            collective_id=0, has_side_effects=True, vmem_limit_bytes=60 * 2**20),
    )(residual, queries, keys, values, docs, sinks, out_weight, norm_gain.reshape(T, 1, C),
      gate_weight, up_weight, down_weight)


def line_of_four_pairs(mesh):
    return mesh.shape["sp"] == 8 and mesh.shape["tp"] == 4


def solution(mesh):
    return jax.shard_map(
        fused if line_of_four_pairs(mesh) else on_device,
        mesh=mesh,
        in_specs=(
            P("sp", None),
            P("sp", "tp"),
            P("sp", "tp"),
            P("sp", "tp"),
            P("sp"),
            P("tp"),
            P("tp", None),
            P(),
            P("sp", "tp"),
            P("sp", "tp"),
            P("sp", "tp"),
        ),
        out_specs=P("sp", "tp"),
        check_vma=False,
    )
```

```python
import functools

import jax
import jax.numpy as jnp
from jax import lax
from jax.experimental import pallas as pl
from jax.experimental.pallas import tpu as pltpu
from jax.sharding import PartitionSpec as P

HEAD_DIM = 64
WINDOW = 128
GROUP = 2


neg_big = -1e30
norm_eps = 1e-05


def from_behind(shard, axis, by):
    length = lax.axis_size(axis)
    pairs = [(i, i + by) for i in range(length) if 0 <= i + by < length]
    return lax.ppermute(shard, axis, pairs)


def attend(queries, keys, values, documents, sinks, tail_keys, tail_values, tail_docs, offset):
    rows_here = queries.shape[0]
    block_count = rows_here // WINDOW
    kv_here = keys.shape[1] // HEAD_DIM
    q_blocks = queries.reshape(block_count, WINDOW, kv_here, GROUP, HEAD_DIM)
    k_blocks = keys.reshape(block_count, WINDOW, kv_here, HEAD_DIM)
    v_blocks = values.reshape(block_count, WINDOW, kv_here, HEAD_DIM)
    k_prev = jnp.concatenate(
        [tail_keys.reshape(1, WINDOW, kv_here, HEAD_DIM), k_blocks[:-1]], axis=0
    )
    v_prev = jnp.concatenate(
        [tail_values.reshape(1, WINDOW, kv_here, HEAD_DIM), v_blocks[:-1]], axis=0
    )
    k_band = jnp.concatenate([k_prev, k_blocks], axis=1)
    v_band = jnp.concatenate([v_prev, v_blocks], axis=1)
    doc_own = documents.astype(jnp.float32).reshape(block_count, WINDOW)
    doc_prev = jnp.concatenate(
        [tail_docs.astype(jnp.float32).reshape(1, WINDOW), doc_own[:-1]], axis=0
    )
    doc_band = jnp.concatenate([doc_prev, doc_own], axis=1)
    row_idx = jnp.arange(WINDOW, dtype=jnp.int32)
    col_idx = jnp.arange(2 * WINDOW, dtype=jnp.int32)
    first = offset + jnp.arange(block_count, dtype=jnp.int32) * WINDOW
    q_pos = first[:, None] + row_idx[None, :]
    k_pos = first[:, None] - WINDOW + col_idx[None, :]
    distance = q_pos[:, :, None] - k_pos[:, None, :]
    visible = (
        (distance >= 0)
        & (distance < WINDOW)
        & (k_pos[:, None, :] >= 0)
        & (doc_own[:, :, None] == doc_band[:, None, :])
    )
    scores = jnp.einsum(
        "nikgd,njkd->nkgij", q_blocks, k_band, preferred_element_type=jnp.float32
    ) * HEAD_DIM ** (-0.5)
    scores = jnp.where(visible[:, None, None], scores, neg_big)
    sink_logit = sinks.reshape(1, kv_here, GROUP, 1, 1)
    row_max = jnp.maximum(scores.max(-1, keepdims=True), sink_logit)
    expo = jnp.where(visible[:, None, None], jnp.exp(scores - row_max), 0.0)
    denom_sum = expo.sum(-1, keepdims=True) + jnp.exp(sink_logit - row_max)
    weights = (expo / denom_sum).astype(jnp.bfloat16)
    mixed = jnp.einsum("nkgij,njkd->nikgd", weights, v_band, preferred_element_type=jnp.float32)
    return mixed.reshape(rows_here, kv_here * GROUP * HEAD_DIM).astype(jnp.bfloat16)


def on_device(
    residual,
    queries,
    keys,
    values,
    documents,
    sinks,
    out_weight,
    norm_gain,
    gate_weight,
    up_weight,
    down_weight,
):
    rows_here = queries.shape[0]
    offset = lax.axis_index("sp") * rows_here
    doc_tail = documents[rows_here - WINDOW :].astype(jnp.bfloat16)
    tail_keys, tail_values, tail_docs = from_behind(
        (keys[rows_here - WINDOW :], values[rows_here - WINDOW :], doc_tail), "sp", 1
    )
    attended = attend(
        queries, keys, values, documents, sinks, tail_keys, tail_values, tail_docs, offset
    )
    model_width = residual.shape[1]
    col_count = model_width // lax.axis_size("tp")
    col_first = lax.axis_index("tp") * col_count
    full_term = jnp.dot(attended, out_weight, preferred_element_type=jnp.float32)
    projected = lax.psum(full_term.astype(jnp.bfloat16), "tp").astype(jnp.float32)
    after_full = (residual.astype(jnp.float32) + projected).astype(jnp.bfloat16)
    after_f = after_full.astype(jnp.float32)
    inv_rms = lax.rsqrt(jnp.mean(after_f * after_f, axis=1, keepdims=True) + norm_eps)
    normed = (after_f * inv_rms * norm_gain[None, :]).astype(jnp.bfloat16)
    after = lax.dynamic_slice_in_dim(after_full, col_first, col_count, 1)
    gate_act = jnp.dot(
        normed,
        lax.all_gather(gate_weight, "sp", axis=0, tiled=True),
        preferred_element_type=jnp.float32,
    )
    up_act = jnp.dot(
        normed,
        lax.all_gather(up_weight, "sp", axis=0, tiled=True),
        preferred_element_type=jnp.float32,
    )
    down_full = lax.all_gather(down_weight, "sp", axis=0, tiled=True)
    hidden = (jax.nn.silu(gate_act) * up_act).astype(jnp.bfloat16)
    summed = lax.psum_scatter(
        lax.dot_general(
            down_full, hidden, (((1,), (1,)), ((), ())), preferred_element_type=jnp.float32
        ).astype(jnp.bfloat16),
        "tp",
        scatter_dimension=0,
        tiled=True,
    ).astype(jnp.float32)
    return (after.astype(jnp.float32) + summed.T).astype(jnp.bfloat16)


MESH = pl.DeviceIdType.MESH
NT = (((1,), (1,)), ((), ()))


def dot(a, b, dims=(((1,), (0,)), ((), ()))):
    return lax.dot_general(a, b, dims, preferred_element_type=jnp.float32)


def when(cond, f):
    if cond is None:
        f()
    else:
        pl.when(cond)(f)


def kernel(
    S, T, W, N,
    res_hbm, q_hbm, k_hbm, v_hbm, doc_hbm, sink_ref, ow_hbm, gain_hbm, g_hbm, u_hbm, d_hbm,
    out_hbm,
    q_ref, doc_ref, gain_ref, out_v,
    G, kx, vx, dx, att, res_v, ow_v, after, normed, ga, ua, hidden, dsend, drecv, ysend, yrecv, zsend, zrecv, own_sum, nsend, nrecv,
    w_send, w_recv, tail_send, tail_recv, loc, ow_send, ow_recv, att_send, att_recv, n_send, n_recv,
    d_send, d_recv, y_send, y_recv, z_send, z_recv, o_sem, o_send, o_recv,
):
    s = lax.axis_index("sp")
    t = lax.axis_index("tp")
    R = q_ref.shape[0]
    C = gain_ref.shape[2]
    D = T * C
    K = D // S
    F = g_hbm.shape[1]
    HK = K // 2
    PER = C // K
    z, x = s // 2, s % 2
    p, c = z % 2, t % 2
    wide = p == c
    n1_z, fr_z, ot_z = z + 1 - 2 * p, (z + 2) % 4, 3 - z
    xp = z * 2 + 1 - x
    n1, fr, ot = n1_z * 2 + x, fr_z * 2 + x, ot_z * 2 + x
    n1_x, fr_x, ot_x = n1_z * 2 + 1 - x, fr_z * 2 + 1 - x, ot_z * 2 + 1 - x
    mid = (z == 1) | (z == 2)
    one, two = jnp.where(mid, fr, ot), jnp.where(mid, ot, fr)
    one_x, two_x = jnp.where(mid, fr_x, ot_x), jnp.where(mid, ot_x, fr_x)
    outer = (z == 0) | (z == 3)
    tc = t + 1 - 2 * c
    ty = (t + 2) % T

    weights = (g_hbm, u_hbm, d_hbm)
    ow_parts = [
        pltpu.make_async_copy(ow_hbm.at[:, i * C:(i + 1) * C], ow_v.at[t, i], loc.at[3 + i]) for i in range(T)
    ]
    res_parts = [
        pltpu.make_async_copy(res_hbm.at[:, i * C:(i + 1) * C], res_v.at[i], loc.at[3 + T + i]) for i in range(T)
    ]
    firsts = [
        pltpu.make_async_copy(a, b, loc.at[3 + 2 * T + i]) for i, (a, b) in enumerate((
            (doc_hbm, doc_ref), (k_hbm, kx.at[pl.ds(WINDOW, R)]), (v_hbm, vx.at[pl.ds(WINDOW, R)]),
            (q_hbm, q_ref), (gain_hbm, gain_ref)))
    ]
    for cp in firsts + ow_parts + res_parts:
        cp.start()

    def split(is_wide, cond, f):
        for flag, width in ((is_wide, W), (jnp.logical_not(is_wide), N)):
            both = flag if cond is None else flag & cond
            pl.when(both)(functools.partial(f, width))

    def columns(q, width):
        return pl.ds(pl.multiple_of(q * (F - width), 128), width)

    def local(m, width):
        return pltpu.make_async_copy(
            weights[m].at[:, columns(p, width)], G.at[m, s, :, pl.ds(0, width)], loc.at[m])

    for m in range(3):
        split(wide, None, lambda width: local(m, width).start())

    barrier = pltpu.get_barrier_semaphore()
    peers = [(xp, t, None), (fr, t, None), (n1, t, None), (ot, t, mid)]
    peers += [(s, (t + d) % T, None) for d in range(1, T)]
    peers += [((s + 1) % S, t, (x == 1) & (z < 3)), ((s + S - 1) % S, t, (x == 0) & (z > 0))]
    for a, b, cond in peers:
        when(cond, lambda: pl.semaphore_signal(barrier, inc=1, device_id=(a, b), device_id_type=MESH))
    present = sum(1 if cond is None else cond.astype(jnp.int32) for _, _, cond in peers)
    pl.semaphore_wait(barrier, present)

    firsts[0].wait()
    blocks = doc_ref.shape[0]
    for i in range(blocks):
        dx[8 + 8 * i:16 + 8 * i, :] = jnp.broadcast_to(doc_ref[i:i + 1, :], (8, WINDOW))
    finish = []

    def go(cond, cp):
        when(cond, cp.start)
        finish.append(lambda: when(cond, cp.wait_send))

    def remote(src, dst, send_sem, recv_sem, to):
        return pltpu.make_async_remote_copy(
            src_ref=src, dst_ref=dst, send_sem=send_sem, recv_sem=recv_sem, device_id=to, device_id_type=MESH)

    tails = []
    for i, (a, b) in enumerate((
        (k_hbm.at[pl.ds(R - WINDOW, WINDOW)], kx.at[pl.ds(0, WINDOW)]),
        (v_hbm.at[pl.ds(R - WINDOW, WINDOW)], vx.at[pl.ds(0, WINDOW)]),
        (dx.at[pl.ds(8 * blocks, 8)], dx.at[pl.ds(0, 8)]),
    )):
        cp = remote(a, b, tail_send.at[i], tail_recv.at[i], ((s + 1) % S, t))
        go(s < S - 1, cp)
        tails.append(cp)

    count = [0]

    def weight(kind, m, h, src=None, cond=None):
        q, to = {
            "A": (1 - p, n1), "B": (p, fr), "C": (1 - p, ot), "D": (p, fr), "X": (p, xp),
        }[kind]
        rows = pl.ds(h * HK, HK)
        sem = w_send.at[count[0]]
        count[0] += 1

        def copy(width):
            part = pl.ds(0, width)
            if src is None:
                return remote(weights[m].at[rows, columns(q, width)], G.at[m, s, rows, part],
                              sem, w_recv.at[m, s, h], (to, t))
            place = G.at[m, src, rows, part]
            return remote(place, place, sem, w_recv.at[m, src, h], (to, t))

        split(q == c, cond, lambda width: copy(width).start())
        finish.append(lambda: split(q == c, cond, lambda width: copy(width).wait_send()))

    def recv(m, src, h, cond=None):
        def wait(width):
            place = G.at[m, src, pl.ds(h * HK, HK), pl.ds(0, width)]
            remote(place, place, w_send.at[0], w_recv.at[m, src, h], (xp, t)).wait_recv()
        split(wide, cond, wait)

    def landed(ref, sem):
        remote(ref, ref, w_send.at[0], sem, (s, tc)).wait_recv()

    GU = ((0, 0), (1, 0), (0, 1), (1, 1))
    DN = ((2, 0), (2, 1))

    for m, h in GU:
        weight("A", m, h)
        weight("X", m, h)
    for i in range(T):
        part = ow_hbm.at[:, i * C:(i + 1) * C]
        go(None, remote(part, ow_v.at[t, i], ow_send.at[0, i], ow_recv.at[t, i], (s, ty)))
        go(None, remote(part, ow_v.at[t, i], ow_send.at[1, i], ow_recv.at[t, i], (s, tc)))
    for m, h in DN:
        weight("A", m, h, cond=mid)
    for m, h in GU[:2]:
        weight("C", m, h, cond=mid)
        weight("B", m, h)
    for m, h in GU[2:]:
        weight("B", m, h, cond=outer)

    @pl.when(jnp.logical_not(wide))
    def _():
        def clear(i, carry):
            for m in range(3):
                G[m, i, :, N:W] = jnp.zeros((K, W - N), jnp.bfloat16)
            return carry
        if W > N:
            lax.fori_loop(0, S, clear, 0)

    @pl.when(s == 0)
    def _():
        kx[pl.ds(0, WINDOW), :] = jnp.zeros((WINDOW, kx.shape[1]), jnp.bfloat16)
        vx[pl.ds(0, WINDOW), :] = jnp.zeros((WINDOW, vx.shape[1]), jnp.bfloat16)
        dx[pl.ds(0, 8), :] = jnp.zeros((8, dx.shape[1]), jnp.int32)

    for cp in firsts[1:]:
        cp.wait()
    for cp in tails:
        when(s > 0, cp.wait_recv)
    heads = q_ref.shape[1] // HEAD_DIM

    def block(b, carry):
        rows = pl.ds(pl.multiple_of(b * WINDOW, WINDOW), WINDOW)
        band = pl.ds(pl.multiple_of(b * WINDOW, WINDOW), 2 * WINDOW)
        prev = dx[pl.ds(pl.multiple_of(b * 8, 8), 8), :][0:1].astype(jnp.float32)
        own = dx[pl.ds(pl.multiple_of(b * 8 + 8, 8), 8), :][0:1].astype(jnp.float32)
        doc_q = jnp.broadcast_to(own, (WINDOW, WINDOW)).T
        i = lax.broadcasted_iota(jnp.int32, (WINDOW, WINDOW), 0)
        j = lax.broadcasted_iota(jnp.int32, (WINDOW, WINDOW), 1)
        first = s * R + b * WINDOW - WINDOW
        see_prev = (j > i) & (doc_q == prev) & (first + j >= 0)
        see_own = (j <= i) & (doc_q == own)
        visible = jnp.concatenate(
            [see_prev.astype(jnp.float32), see_own.astype(jnp.float32)], axis=1) > 0.5
        for h in range(heads):
            kv = h // GROUP
            cols = slice(kv * HEAD_DIM, (kv + 1) * HEAD_DIM)
            q = q_ref[rows, h * HEAD_DIM:(h + 1) * HEAD_DIM]
            scores = dot(q, kx[band, cols], NT) * HEAD_DIM ** (-0.5)
            scores = jnp.where(visible, scores, neg_big)
            sink = sink_ref[h]
            row_max = jnp.maximum(scores.max(-1, keepdims=True), sink)
            expo = jnp.where(visible, jnp.exp(scores - row_max), 0.0)
            total = expo.sum(-1, keepdims=True) + jnp.exp(sink - row_max)
            w = (expo / total).astype(jnp.bfloat16)
            att[t, rows, h * HEAD_DIM:(h + 1) * HEAD_DIM] = dot(w, vx[band, cols]).astype(jnp.bfloat16)
        return carry

    lax.fori_loop(0, R // WINDOW, block, 0)

    go(None, remote(att.at[t], att.at[t], att_send.at[0], att_recv.at[t], (s, ty)))
    go(None, remote(att.at[t], att.at[t], att_send.at[1], att_recv.at[t], (s, tc)))

    def ow_relay(i):
        landed(ow_v.at[ty, i], ow_recv.at[ty, i])
        go(None, remote(ow_v.at[ty, i], ow_v.at[ty, i], ow_send.at[2, i], ow_recv.at[ty, i], (s, tc)))

    def pass_on(m, h, src, cond=None):
        recv(m, src, h, cond)
        weight("X", m, h, src=src, cond=cond)

    pass_on(0, 0, n1)
    weight("D", 0, 0, src=n1, cond=mid)
    for m, h in (GU[2], GU[3], DN[0]):
        weight("C", m, h, cond=mid)
    pass_on(1, 0, n1)
    weight("D", 1, 0, src=n1, cond=mid)
    weight("B", 0, 1, cond=mid)
    ow_relay(0)
    pass_on(0, 0, ot, mid)
    pass_on(0, 0, fr, outer)
    ow_relay(1)
    pass_on(0, 1, n1)
    weight("D", 0, 1, src=n1, cond=mid)
    weight("B", 1, 1, cond=mid)
    pass_on(1, 1, n1)
    weight("D", 1, 1, src=n1, cond=mid)
    ow_relay(2)
    pass_on(1, 0, ot, mid)
    pass_on(1, 0, fr, outer)
    ow_relay(3)
    landed(att.at[ty], att_recv.at[ty])
    go(None, remote(att.at[ty], att.at[ty], att_send.at[2], att_recv.at[ty], (s, tc)))
    for cp in ow_parts + res_parts:
        cp.wait()
    td = (tc + 2) % T
    for g in (tc, td):
        for i in range(T):
            landed(ow_v.at[g, i], ow_recv.at[g, i])
        landed(att.at[g], att_recv.at[g])

    HR = R // 2
    for r in range(2):
        rows = slice(r * HR, (r + 1) * HR)

        def project(i, square):
            total = dot(att[0, rows, :], ow_v[0, i]).astype(jnp.bfloat16).astype(jnp.float32)
            for g in range(1, T):
                total += dot(att[g, rows, :], ow_v[g, i]).astype(jnp.bfloat16).astype(jnp.float32)
            value = (res_v[i, rows, :].astype(jnp.float32) + total).astype(jnp.bfloat16)
            after[i, rows, :] = value
            value = value.astype(jnp.float32)
            return square + (value * value).sum(-1, keepdims=True)

        square = lax.fori_loop(0, T, project, jnp.zeros((HR, 1), jnp.float32))
        inv = lax.rsqrt(square / D + norm_eps)

        def norm(i, carry):
            n = (after[i, rows, :].astype(jnp.float32) * inv * gain_ref[i]).astype(jnp.bfloat16)
            for j in range(PER):
                normed[i * PER + j, rows, :] = n[:, j * K:(j + 1) * K]
            return carry

        lax.fori_loop(0, T, norm, 0)
        go(None, remote(
            normed.at[pl.ds(t * PER, PER), pl.ds(r * HR, HR)],
            normed.at[pl.ds(t * PER, PER), pl.ds(R + r * HR, HR)],
            n_send.at[0, r], n_recv.at[t, r], (n1, t)))

    for m, h in DN:
        weight("A", m, h, cond=outer)

    def passed(g, r):
        return normed.at[pl.ds(g * PER, PER), pl.ds(R + r * HR, HR)]

    TM = 256

    def gate_up(src, first, last, begin=False):
        def tile(r, carry):
            rows = pl.ds(pl.multiple_of(r * TM, TM), TM)
            a = normed[src, rows, :]
            for m, acc in ((0, ga), (1, ua)):
                value = dot(a, G[m, src])
                if begin:
                    acc[rows, :] = value
                else:
                    acc[rows, :] += value
            return carry
        lax.fori_loop(first // TM, last // TM, tile, 0)

    for m in range(3):
        split(wide, None, lambda width: local(m, width).wait())
    for m, h in GU:
        pass_on(m, h, fr, mid)
    for m, h in DN:
        weight("X", m, h, cond=outer)
    gate_up(s, 0, R, True)
    gate_up(n1, 0, R)
    pass_on(0, 0, ot, outer)
    for src in (xp, n1_x):
        for m, h in GU:
            recv(m, src, h)
        gate_up(src, 0, R)
    pass_on(0, 1, ot, mid)
    for r in range(2):
        landed(passed(t, r), n_recv.at[t, r])
        go(None, remote(passed(t, r), passed(t, r), n_send.at[1, r], n_recv.at[t, r], (s, ty)))
        go(None, remote(passed(t, r), passed(t, r), n_send.at[2, r], n_recv.at[t, r], (s, tc)))
    pass_on(1, 1, ot, mid)
    for m, h in DN:
        weight("X", m, h, cond=mid)
    pass_on(1, 0, ot, outer)
    for r in range(2):
        landed(passed(ty, r), n_recv.at[ty, r])
        go(None, remote(passed(ty, r), passed(ty, r), n_send.at[3, r], n_recv.at[ty, r], (s, tc)))
    for m, h in DN:
        recv(m, n1, h, mid)
        weight("X", m, h, src=n1, cond=mid)
        weight("D", m, h, src=n1, cond=mid)
        weight("B", m, h, cond=mid)
        if h == 0:
            weight("C", 2, 1, cond=mid)
    pass_on(0, 1, fr, outer)
    for g in (tc, td):
        for r in range(2):
            landed(passed(g, r), n_recv.at[g, r])
    gate_up(s, R, 2 * R, True)
    gate_up(n1, R, 2 * R)
    pass_on(0, 1, ot, outer)
    gate_up(xp, R, 2 * R)
    gate_up(n1_x, R, 2 * R)
    pass_on(1, 1, fr, outer)
    gate_up(fr, 0, 2 * R)
    pass_on(1, 1, ot, outer)
    for m, h in DN:
        weight("B", m, h, cond=outer)
        pass_on(m, h, n1, outer)
    gate_up(ot, 0, 2 * R)
    for m, h in GU:
        recv(m, fr_x, h)
    gate_up(fr_x, 0, 2 * R)
    for m, h in GU:
        recv(m, ot_x, h)
    gate_up(ot_x, 0, 2 * R)

    def act(r, carry):
        rows = pl.ds(pl.multiple_of(r * 32, 32), 32)
        g = ga[rows, :]
        hidden[rows, :] = (g / (1.0 + jnp.exp(-g)) * ua[rows, :]).astype(jnp.bfloat16)
        return carry

    lax.fori_loop(0, 2 * R // 32, act, 0)

    def handed(k, h, r):
        return remote(dsend.at[k, h, r], drecv.at[k, h, r], d_send.at[k, 2 * h + r], d_recv.at[k, 2 * h + r], (s, tc))

    def across(j, h):
        return remote(ysend.at[j, h], yrecv.at[j, h], y_send.at[j, h], y_recv.at[j, h], (s, ty))

    def over(j, h):
        return remote(nsend.at[j, h], nrecv.at[j, h], o_send.at[j, h], o_recv.at[j, h], (s, ty))

    def back(k, h):
        return remote(zsend.at[k, h], zrecv.at[k, h], z_send.at[k, h], z_recv.at[k, h], (n1, t))

    def add(out, at, *terms):
        def rows_of(i, carry):
            rows = pl.ds(pl.multiple_of(i * WINDOW, WINDOW), WINDOW)
            total = None
            for ref, where in terms:
                value = ref[(*where, rows, slice(None))].astype(jnp.float32)
                total = value if total is None else total + value
            out[(*at, rows, slice(None))] = total.astype(out.dtype)
            return carry
        lax.fori_loop(0, R // WINDOW, rows_of, 0)

    def kept(k):
        return (k // PER) % 2 == c

    def down(k, *hs):
        given = jnp.logical_not(kept(k))
        value = dot(hidden[...], G[2, k, hs[0] * HK:(hs[-1] + 1) * HK, :], NT).astype(jnp.bfloat16)
        for r in (1, 0):
            for i, h in enumerate(hs):
                dsend[k, h, r] = value[r * R:(r + 1) * R, i * HK:(i + 1) * HK]

        @pl.when(given)
        def _():
            for r in (1, 0):
                for h in hs:
                    handed(k, h, r).start()

        def sent():
            for h in hs:
                for r in (1, 0):
                    handed(k, h, r).wait_send()
        finish.append(lambda: pl.when(given)(sent))

    def pair(k, h, r):
        landed(drecv.at[k, h, r], d_recv.at[k, 2 * h + r])
        return (dsend, (k, h, r)), (drecv, (k, h, r))

    def case(k, cond, f, *hs):
        @pl.when(cond)
        def _():
            for h in hs:
                f(k % PER, h)

    def cross(k, *hs):
        def straight(j, h):
            add(zsend, (k, h), *pair(k, h, 1))
            back(k, h).start()

        def sideways(j, h):
            add(nsend, (j, h), *pair(k, h, 1))
            over(j, h).start()

        def plain(j, h):
            add(ysend, (j, h), *pair(k, h, 0))
            across(j, h).start()

        case(k, outer & kept(k), straight, *hs)
        case(k, outer & (k // PER == ty), plain, *hs)
        case(k, mid & (k // PER == ty), sideways, *hs)
        sends = (outer & kept(k)) | (mid & (k // PER == t))
        finish.append(lambda: case(k, sends, lambda j, h: back(k, h).wait_send(), *hs))
        finish.append(lambda: case(k, mid & (k // PER == ty), lambda j, h: over(j, h).wait_send(), *hs))

    def lift(k, *hs):
        def up(j, h):
            terms = pair(k, h, 1)
            landed(nrecv.at[j, h], o_recv.at[j, h])
            add(zsend, (k, h), *terms, (nrecv, (j, h)))
            back(k, h).start()

        case(k, mid & (k // PER == t), up, *hs)

    def settle(k, *hs):
        def own(j, h):
            terms = pair(k, h, 0)
            landed(zrecv.at[k, h], z_recv.at[k, h])
            add(own_sum, (j, h), *terms, (zrecv, (k, h)))

        case(k, k // PER == t, own, *hs)

    def passing(k, *hs):
        def onward(j, h):
            terms = pair(k, h, 0)
            landed(zrecv.at[k, h], z_recv.at[k, h])
            add(ysend, (j, h), *terms, (zrecv, (k, h)))
            across(j, h).start()

        case(k, mid & (k // PER == ty), onward, *hs)

    def halves(src, *hs):
        for h in hs:
            recv(2, src, h)

    down(s, 0, 1)
    down(n1, 0, 1)
    cross(s, 0, 1)
    pass_on(2, 0, ot)
    halves(xp, 0, 1)
    down(xp, 0, 1)
    cross(n1, 0, 1)
    pass_on(2, 0, fr)
    halves(n1_x, 0, 1)
    down(n1_x, 0, 1)
    cross(xp, 0, 1)
    down(ot, 0)
    cross(n1_x, 0, 1)
    down(fr, 0)
    cross(ot, 0)
    halves(ot_x, 0)
    down(ot_x, 0)
    cross(fr, 0)
    lift(s, 0, 1)
    lift(n1, 0, 1)
    pass_on(2, 1, one)
    down(one, 1)
    cross(ot_x, 0)
    lift(xp, 0, 1)
    lift(n1_x, 0, 1)
    pass_on(2, 1, two)
    halves(fr_x, 0)
    down(fr_x, 0)
    cross(one, 1)
    passing(s, 0, 1)
    passing(n1, 0, 1)
    down(two, 1)
    cross(fr_x, 0)
    cross(two, 1)
    halves(one_x, 1)
    down(one_x, 1)
    lift(ot, 0)
    lift(fr, 0)
    cross(one_x, 1)
    halves(two_x, 1)
    down(two_x, 1)
    passing(xp, 0, 1)
    passing(n1_x, 0, 1)
    cross(two_x, 1)
    lift(ot_x, 0)
    lift(one, 1)
    passing(ot, 0)
    passing(fr, 0)
    passing(ot_x, 0)
    lift(fr_x, 0)
    lift(two, 1)
    passing(one, 1)
    passing(fr_x, 0)
    passing(two, 1)
    lift(one_x, 1)
    lift(two_x, 1)
    passing(one_x, 1)
    passing(two_x, 1)
    for k in (s, n1, xp, n1_x):
        settle(k, 0, 1)
    for k, h in ((ot, 0), (fr, 0), (ot_x, 0), (one, 1), (fr_x, 0), (two, 1), (one_x, 1), (two_x, 1)):
        settle(k, h)

    stores = []
    for h in (0, 1):
        for j in range(PER):
            landed(yrecv.at[j, h], y_recv.at[j, h])
            cols = slice((j * 2 + h) * HK, (j * 2 + h + 1) * HK)
            out_v[:, cols] = (
                after[t, :, cols].astype(jnp.float32) + (own_sum[j, h] + yrecv[j, h].astype(jnp.float32))
            ).astype(jnp.bfloat16)
            cp = pltpu.make_async_copy(out_v.at[:, cols], out_hbm.at[:, cols], o_sem.at[j, h])
            cp.start()
            stores.append(cp)

    for f in finish:
        f()
    for j in range(PER):
        for h in (0, 1):
            across(j, h).wait_send()
    for cp in stores:
        cp.wait()


def fused(residual, queries, keys, values, documents, sinks, out_weight, norm_gain, gate_weight, up_weight, down_weight):
    S, T = lax.axis_size("sp"), lax.axis_size("tp")
    R, D = residual.shape
    F = gate_weight.shape[1]
    C, K = D // T, D // S
    W = (F // 128 + 1) // 2 * 128
    N = F - W
    PER = C // K
    blocks = R // WINDOW
    HK = K // 2
    bf, f32 = jnp.bfloat16, jnp.float32
    hbm = pl.BlockSpec(memory_space=pl.ANY)
    dma = pltpu.SemaphoreType.DMA
    scratch = [
        pltpu.VMEM((R, queries.shape[1]), bf),
        pltpu.VMEM((blocks, WINDOW), jnp.int32),
        pltpu.VMEM((T, 1, C), f32),
        pltpu.VMEM((R, C), bf),
        pltpu.VMEM((3, S, K, W), bf),
        pltpu.VMEM((R + WINDOW, keys.shape[1]), bf),
        pltpu.VMEM((R + WINDOW, keys.shape[1]), bf),
        pltpu.VMEM((blocks * 8 + 8, WINDOW), jnp.int32),
        pltpu.VMEM((T, R, queries.shape[1]), bf),
        pltpu.VMEM((T, R, C), bf),
        pltpu.VMEM((T, T, out_weight.shape[0], C), bf),
        pltpu.VMEM((T, R, C), bf),
        pltpu.VMEM((S, 2 * R, K), bf),
        pltpu.VMEM((2 * R, W), f32),
        pltpu.VMEM((2 * R, W), f32),
        pltpu.VMEM((2 * R, W), bf),
        pltpu.VMEM((S, 2, 2, R, HK), bf),
        pltpu.VMEM((S, 2, 2, R, HK), bf),
        pltpu.VMEM((PER, 2, R, HK), bf),
        pltpu.VMEM((PER, 2, R, HK), bf),
        pltpu.VMEM((S, 2, R, HK), bf),
        pltpu.VMEM((S, 2, R, HK), bf),
        pltpu.VMEM((PER, 2, R, HK), f32),
        pltpu.VMEM((PER, 2, R, HK), bf),
        pltpu.VMEM((PER, 2, R, HK), bf),
        dma((96,)), dma((3, S, 2)), dma((3,)), dma((3,)), dma((8 + 2 * T,)),
        dma((3, T)), dma((T, T)), dma((3,)), dma((T,)), dma((4, 2)), dma((T, 2)),
        dma((S, 4)), dma((S, 4)), dma((PER, 2)), dma((PER, 2)), dma((S, 2)), dma((S, 2)), dma((PER, 2)), dma((PER, 2)), dma((PER, 2)),
    ]
    return pl.pallas_call(
        functools.partial(kernel, S, T, W, N),
        out_shape=jax.ShapeDtypeStruct((R, C), bf),
        in_specs=[hbm] * 5 + [pl.BlockSpec(memory_space=pltpu.SMEM)] + [hbm] * 5,
        out_specs=hbm,
        scratch_shapes=scratch,
        compiler_params=pltpu.CompilerParams(
            collective_id=0, has_side_effects=True, vmem_limit_bytes=60 * 2**20),
    )(residual, queries, keys, values, documents.reshape(blocks, WINDOW), sinks, out_weight, norm_gain.reshape(T, 1, C),
      gate_weight, up_weight, down_weight)


def line_of_four_pairs(mesh):
    return mesh.shape["sp"] == 8 and mesh.shape["tp"] == 4


def solution(mesh):
    return jax.shard_map(
        fused if line_of_four_pairs(mesh) else on_device,
        mesh=mesh,
        in_specs=(
            P("sp", None),
            P("sp", "tp"),
            P("sp", "tp"),
            P("sp", "tp"),
            P("sp"),
            P("tp"),
            P("tp", None),
            P(),
            P("sp", "tp"),
            P("sp", "tp"),
            P("sp", "tp"),
        ),
        out_specs=P("sp", "tp"),
        check_vma=False,
    )
```

```python
import functools

import jax
import jax.numpy as jnp
from jax import lax
from jax.experimental import pallas as pl
from jax.experimental.pallas import tpu as pltpu
from jax.sharding import PartitionSpec as P

HEAD_DIM = 64
WINDOW = 128
GROUP = 2


neg_big = -1e30
norm_eps = 1e-05


def from_behind(shard, axis, by):
    length = lax.axis_size(axis)
    pairs = [(i, i + by) for i in range(length) if 0 <= i + by < length]
    return lax.ppermute(shard, axis, pairs)


def attend(queries, keys, values, documents, sinks, tail_keys, tail_values, tail_docs, offset):
    rows_here = queries.shape[0]
    block_count = rows_here // WINDOW
    kv_here = keys.shape[1] // HEAD_DIM
    q_blocks = queries.reshape(block_count, WINDOW, kv_here, GROUP, HEAD_DIM)
    k_blocks = keys.reshape(block_count, WINDOW, kv_here, HEAD_DIM)
    v_blocks = values.reshape(block_count, WINDOW, kv_here, HEAD_DIM)
    k_prev = jnp.concatenate(
        [tail_keys.reshape(1, WINDOW, kv_here, HEAD_DIM), k_blocks[:-1]], axis=0
    )
    v_prev = jnp.concatenate(
        [tail_values.reshape(1, WINDOW, kv_here, HEAD_DIM), v_blocks[:-1]], axis=0
    )
    k_band = jnp.concatenate([k_prev, k_blocks], axis=1)
    v_band = jnp.concatenate([v_prev, v_blocks], axis=1)
    doc_own = documents.astype(jnp.float32).reshape(block_count, WINDOW)
    doc_prev = jnp.concatenate(
        [tail_docs.astype(jnp.float32).reshape(1, WINDOW), doc_own[:-1]], axis=0
    )
    doc_band = jnp.concatenate([doc_prev, doc_own], axis=1)
    row_idx = jnp.arange(WINDOW, dtype=jnp.int32)
    col_idx = jnp.arange(2 * WINDOW, dtype=jnp.int32)
    first = offset + jnp.arange(block_count, dtype=jnp.int32) * WINDOW
    q_pos = first[:, None] + row_idx[None, :]
    k_pos = first[:, None] - WINDOW + col_idx[None, :]
    distance = q_pos[:, :, None] - k_pos[:, None, :]
    visible = (
        (distance >= 0)
        & (distance < WINDOW)
        & (k_pos[:, None, :] >= 0)
        & (doc_own[:, :, None] == doc_band[:, None, :])
    )
    scores = jnp.einsum(
        "nikgd,njkd->nkgij", q_blocks, k_band, preferred_element_type=jnp.float32
    ) * HEAD_DIM ** (-0.5)
    scores = jnp.where(visible[:, None, None], scores, neg_big)
    sink_logit = sinks.reshape(1, kv_here, GROUP, 1, 1)
    row_max = jnp.maximum(scores.max(-1, keepdims=True), sink_logit)
    expo = jnp.where(visible[:, None, None], jnp.exp(scores - row_max), 0.0)
    denom_sum = expo.sum(-1, keepdims=True) + jnp.exp(sink_logit - row_max)
    weights = (expo / denom_sum).astype(jnp.bfloat16)
    mixed = jnp.einsum("nkgij,njkd->nikgd", weights, v_band, preferred_element_type=jnp.float32)
    return mixed.reshape(rows_here, kv_here * GROUP * HEAD_DIM).astype(jnp.bfloat16)


def on_device(
    residual,
    queries,
    keys,
    values,
    documents,
    sinks,
    out_weight,
    norm_gain,
    gate_weight,
    up_weight,
    down_weight,
):
    rows_here = queries.shape[0]
    offset = lax.axis_index("sp") * rows_here
    doc_tail = documents[rows_here - WINDOW :].astype(jnp.bfloat16)
    tail_keys, tail_values, tail_docs = from_behind(
        (keys[rows_here - WINDOW :], values[rows_here - WINDOW :], doc_tail), "sp", 1
    )
    attended = attend(
        queries, keys, values, documents, sinks, tail_keys, tail_values, tail_docs, offset
    )
    model_width = residual.shape[1]
    col_count = model_width // lax.axis_size("tp")
    col_first = lax.axis_index("tp") * col_count
    full_term = jnp.dot(attended, out_weight, preferred_element_type=jnp.float32)
    projected = lax.psum(full_term.astype(jnp.bfloat16), "tp").astype(jnp.float32)
    after_full = (residual.astype(jnp.float32) + projected).astype(jnp.bfloat16)
    after_f = after_full.astype(jnp.float32)
    inv_rms = lax.rsqrt(jnp.mean(after_f * after_f, axis=1, keepdims=True) + norm_eps)
    normed = (after_f * inv_rms * norm_gain[None, :]).astype(jnp.bfloat16)
    after = lax.dynamic_slice_in_dim(after_full, col_first, col_count, 1)
    gate_act = jnp.dot(
        normed,
        lax.all_gather(gate_weight, "sp", axis=0, tiled=True),
        preferred_element_type=jnp.float32,
    )
    up_act = jnp.dot(
        normed,
        lax.all_gather(up_weight, "sp", axis=0, tiled=True),
        preferred_element_type=jnp.float32,
    )
    down_full = lax.all_gather(down_weight, "sp", axis=0, tiled=True)
    hidden = (jax.nn.silu(gate_act) * up_act).astype(jnp.bfloat16)
    summed = lax.psum_scatter(
        lax.dot_general(
            down_full, hidden, (((1,), (1,)), ((), ())), preferred_element_type=jnp.float32
        ).astype(jnp.bfloat16),
        "tp",
        scatter_dimension=0,
        tiled=True,
    ).astype(jnp.float32)
    return (after.astype(jnp.float32) + summed.T).astype(jnp.bfloat16)


MESH = pl.DeviceIdType.MESH
NT = (((1,), (1,)), ((), ()))


def dot(a, b, dims=(((1,), (0,)), ((), ()))):
    return lax.dot_general(a, b, dims, preferred_element_type=jnp.float32)


def when(cond, f):
    if cond is None:
        f()
    else:
        pl.when(cond)(f)


def kernel(
    S, T, W, N,
    res_hbm, q_hbm, k_hbm, v_hbm, doc_hbm, sink_ref, ow_hbm, gain_hbm, g_hbm, u_hbm, d_hbm,
    out_hbm,
    q_ref, doc_ref, gain_ref, out_v,
    G, kx, vx, dx, att, res_v, ow_v, after, normed, ga, ua, hidden, dsend, drecv, ysend, yrecv, zsend, zrecv, own_sum, nsend, nrecv,
    w_send, w_recv, tail_send, tail_recv, loc, ow_send, ow_recv, att_send, att_recv, n_send, n_recv,
    d_send, d_recv, y_send, y_recv, z_send, z_recv, o_sem, o_send, o_recv,
):
    s = lax.axis_index("sp")
    t = lax.axis_index("tp")
    R = q_ref.shape[0]
    C = gain_ref.shape[2]
    D = T * C
    K = D // S
    F = g_hbm.shape[1]
    HK = K // 2
    PER = C // K
    z, x = s // 2, s % 2
    p, c = z % 2, t % 2
    wide = p == c
    n1_z, fr_z, ot_z = z + 1 - 2 * p, (z + 2) % 4, 3 - z
    xp = z * 2 + 1 - x
    n1, fr, ot = n1_z * 2 + x, fr_z * 2 + x, ot_z * 2 + x
    n1_x, fr_x, ot_x = n1_z * 2 + 1 - x, fr_z * 2 + 1 - x, ot_z * 2 + 1 - x
    mid = (z == 1) | (z == 2)
    one, two = jnp.where(mid, fr, ot), jnp.where(mid, ot, fr)
    one_x, two_x = jnp.where(mid, fr_x, ot_x), jnp.where(mid, ot_x, fr_x)
    outer = (z == 0) | (z == 3)
    tc = t + 1 - 2 * c
    ty = (t + 2) % T

    weights = (g_hbm, u_hbm, d_hbm)
    ow_parts = [
        pltpu.make_async_copy(ow_hbm.at[:, i * C:(i + 1) * C], ow_v.at[t, i], loc.at[0]) for i in range(T)
    ]
    res_parts = [
        pltpu.make_async_copy(res_hbm.at[:, i * C:(i + 1) * C], res_v.at[i], loc.at[1]) for i in range(T)
    ]
    firsts = [
        pltpu.make_async_copy(a, b, loc.at[3 + i]) for i, (a, b) in enumerate((
            (doc_hbm, doc_ref), (k_hbm, kx.at[pl.ds(WINDOW, R)]), (v_hbm, vx.at[pl.ds(WINDOW, R)]),
            (q_hbm, q_ref), (gain_hbm, gain_ref)))
    ]
    for cp in firsts + ow_parts + res_parts:
        cp.start()

    def split(is_wide, cond, f):
        for flag, width in ((is_wide, W), (jnp.logical_not(is_wide), N)):
            both = flag if cond is None else flag & cond
            pl.when(both)(functools.partial(f, width))

    def columns(q, width):
        return pl.ds(pl.multiple_of(q * (F - width), 128), width)

    def local(m, width):
        return pltpu.make_async_copy(
            weights[m].at[:, columns(p, width)], G.at[m, s, :, pl.ds(0, width)], loc.at[2])

    for m in range(3):
        split(wide, None, lambda width: local(m, width).start())

    barrier = pltpu.get_barrier_semaphore()
    peers = [(xp, t, None), (fr, t, None), (n1, t, None), (ot, t, mid)]
    peers += [(s, (t + d) % T, None) for d in range(1, T)]
    peers += [((s + 1) % S, t, (x == 1) & (z < 3)), ((s + S - 1) % S, t, (x == 0) & (z > 0))]
    for a, b, cond in peers:
        when(cond, lambda: pl.semaphore_signal(barrier, inc=1, device_id=(a, b), device_id_type=MESH))
    present = sum(1 if cond is None else cond.astype(jnp.int32) for _, _, cond in peers)
    pl.semaphore_wait(barrier, present)

    firsts[0].wait()
    blocks = doc_ref.shape[0]
    for i in range(blocks):
        dx[8 + 8 * i:16 + 8 * i, :] = jnp.broadcast_to(doc_ref[i:i + 1, :], (8, WINDOW))
    finish = []

    def go(cond, cp):
        when(cond, cp.start)
        finish.append(lambda: when(cond, cp.wait_send))

    def start(cp):
        cp.start()

    def remote(src, dst, send_sem, recv_sem, to):
        return pltpu.make_async_remote_copy(
            src_ref=src, dst_ref=dst, send_sem=send_sem, recv_sem=recv_sem, device_id=to, device_id_type=MESH)

    tails = []
    for i, (a, b) in enumerate((
        (k_hbm.at[pl.ds(R - WINDOW, WINDOW)], kx.at[pl.ds(0, WINDOW)]),
        (v_hbm.at[pl.ds(R - WINDOW, WINDOW)], vx.at[pl.ds(0, WINDOW)]),
        (dx.at[pl.ds(8 * blocks, 8)], dx.at[pl.ds(0, 8)]),
    )):
        cp = remote(a, b, tail_send.at[i], tail_recv.at[i], ((s + 1) % S, t))
        go(s < S - 1, cp)
        tails.append(cp)

    kinds = {"A": (1 - p, n1), "B": (p, fr), "C": (1 - p, ot), "D": (p, fr), "X": (p, xp)}

    def weight(kind, m, h, src=None, cond=None):
        q, to = kinds[kind]
        rows = pl.ds(h * HK, HK)
        sem = w_send.at["ABCDX".index(kind)]

        def copy(width):
            part = pl.ds(0, width)
            if src is None:
                return remote(weights[m].at[rows, columns(q, width)], G.at[m, s, rows, part],
                              sem, w_recv.at[m, s, h], (to, t))
            place = G.at[m, src, rows, part]
            return remote(place, place, sem, w_recv.at[m, src, h], (to, t))

        split(q == c, cond, lambda width: copy(width).start())

    def weights_sent(kind, sources, cond=None):
        q, to = kinds[kind]

        def wait(width):
            place = G.at[:, pl.ds(0, sources), :, pl.ds(0, width)]
            remote(place, place, w_send.at["ABCDX".index(kind)], w_recv.at[0, 0, 0], (to, t)).wait_send()

        split(q == c, cond, wait)

    def recv(m, src, h, cond=None):
        def wait(width):
            place = G.at[m, src, pl.ds(h * HK, HK), pl.ds(0, width)]
            remote(place, place, w_send.at[0], w_recv.at[m, src, h], (xp, t)).wait_recv()
        split(wide, cond, wait)

    def landed(ref, sem):
        remote(ref, ref, w_send.at[0], sem, (s, tc)).wait_recv()

    GU = ((0, 0), (1, 0), (0, 1), (1, 1))
    DN = ((2, 0), (2, 1))

    for m, h in GU:
        weight("A", m, h)
        weight("X", m, h)
    for i in range(T):
        part = ow_hbm.at[:, i * C:(i + 1) * C]
        start(remote(part, ow_v.at[t, i], ow_send.at[0], ow_recv.at[i], (s, ty)))
        start(remote(part, ow_v.at[t, i], ow_send.at[1], ow_recv.at[T], (s, tc)))
    weight("A", 2, 0, cond=mid)
    weight("C", 0, 0, cond=mid)
    for m, h in GU[:2]:
        weight("B", m, h)
    for m, h in GU[2:]:
        weight("B", m, h, cond=outer)

    @pl.when(jnp.logical_not(wide))
    def _():
        def clear(i, carry):
            for m in range(3):
                G[m, i, :, N:W] = jnp.zeros((K, W - N), jnp.bfloat16)
            return carry
        if W > N:
            lax.fori_loop(0, S, clear, 0)

    @pl.when(s == 0)
    def _():
        kx[pl.ds(0, WINDOW), :] = jnp.zeros((WINDOW, kx.shape[1]), jnp.bfloat16)
        vx[pl.ds(0, WINDOW), :] = jnp.zeros((WINDOW, vx.shape[1]), jnp.bfloat16)
        dx[pl.ds(0, 8), :] = jnp.zeros((8, dx.shape[1]), jnp.int32)

    for cp in firsts[1:]:
        cp.wait()
    for cp in tails:
        when(s > 0, cp.wait_recv)
    heads = q_ref.shape[1] // HEAD_DIM

    def block(b, carry):
        rows = pl.ds(pl.multiple_of(b * WINDOW, WINDOW), WINDOW)
        band = pl.ds(pl.multiple_of(b * WINDOW, WINDOW), 2 * WINDOW)
        prev = dx[pl.ds(pl.multiple_of(b * 8, 8), 8), :][0:1].astype(jnp.float32)
        own = dx[pl.ds(pl.multiple_of(b * 8 + 8, 8), 8), :][0:1].astype(jnp.float32)
        doc_q = jnp.broadcast_to(own, (WINDOW, WINDOW)).T
        i = lax.broadcasted_iota(jnp.int32, (WINDOW, WINDOW), 0)
        j = lax.broadcasted_iota(jnp.int32, (WINDOW, WINDOW), 1)
        first = s * R + b * WINDOW - WINDOW
        see_prev = (j > i) & (doc_q == prev) & (first + j >= 0)
        see_own = (j <= i) & (doc_q == own)
        visible = jnp.concatenate(
            [see_prev.astype(jnp.float32), see_own.astype(jnp.float32)], axis=1) > 0.5
        for h in range(heads):
            kv = h // GROUP
            cols = slice(kv * HEAD_DIM, (kv + 1) * HEAD_DIM)
            q = q_ref[rows, h * HEAD_DIM:(h + 1) * HEAD_DIM]
            scores = dot(q, kx[band, cols], NT) * HEAD_DIM ** (-0.5)
            scores = jnp.where(visible, scores, neg_big)
            sink = sink_ref[h]
            row_max = jnp.maximum(scores.max(-1, keepdims=True), sink)
            expo = jnp.where(visible, jnp.exp(scores - row_max), 0.0)
            total = expo.sum(-1, keepdims=True) + jnp.exp(sink - row_max)
            w = (expo / total).astype(jnp.bfloat16)
            att[t, rows, h * HEAD_DIM:(h + 1) * HEAD_DIM] = dot(w, vx[band, cols]).astype(jnp.bfloat16)
        return carry

    lax.fori_loop(0, R // WINDOW, block, 0)

    go(None, remote(att.at[t], att.at[t], att_send.at[0], att_recv.at[t], (s, ty)))
    go(None, remote(att.at[t], att.at[t], att_send.at[1], att_recv.at[t], (s, tc)))

    def ow_relay(i):
        landed(ow_v.at[ty, i], ow_recv.at[i])
        start(remote(ow_v.at[ty, i], ow_v.at[ty, i], ow_send.at[2], ow_recv.at[T + 1], (s, tc)))

    def pass_on(m, h, src, cond=None):
        recv(m, src, h, cond)
        weight("X", m, h, src=src, cond=cond)

    pass_on(0, 0, n1)
    weight("D", 0, 0, src=n1, cond=mid)
    pass_on(1, 0, n1)
    weight("D", 1, 0, src=n1, cond=mid)
    for m, h in GU[1:]:
        weight("C", m, h, cond=mid)
    weight("B", 0, 1, cond=mid)
    ow_relay(0)
    pass_on(0, 0, fr, outer)
    ow_relay(1)
    pass_on(0, 1, n1)
    weight("D", 0, 1, src=n1, cond=mid)
    weight("B", 1, 1, cond=mid)
    pass_on(1, 1, n1)
    weight("D", 1, 1, src=n1, cond=mid)
    weight("C", 2, 0, cond=mid)
    ow_relay(2)
    pass_on(0, 0, ot, mid)
    pass_on(1, 0, fr, outer)
    ow_relay(3)
    pass_on(0, 0, ot, outer)
    landed(att.at[ty], att_recv.at[ty])
    go(None, remote(att.at[ty], att.at[ty], att_send.at[2], att_recv.at[ty], (s, tc)))
    pltpu.make_async_copy(ow_v.at[t], ow_v.at[t], loc.at[0]).wait()
    pltpu.make_async_copy(res_v, res_v, loc.at[1]).wait()
    td = (tc + 2) % T
    for i, g in enumerate((tc, td)):
        landed(ow_v.at[g], ow_recv.at[T + i])
        landed(att.at[g], att_recv.at[g])

    HR = R // 2
    for r in range(2):
        rows = slice(r * HR, (r + 1) * HR)

        def project(i, square):
            total = dot(att[0, rows, :], ow_v[0, i]).astype(jnp.bfloat16).astype(jnp.float32)
            for g in range(1, T):
                total += dot(att[g, rows, :], ow_v[g, i]).astype(jnp.bfloat16).astype(jnp.float32)
            value = (res_v[i, rows, :].astype(jnp.float32) + total).astype(jnp.bfloat16)
            after[i, rows, :] = value
            value = value.astype(jnp.float32)
            return square + (value * value).sum(-1, keepdims=True)

        square = lax.fori_loop(0, T, project, jnp.zeros((HR, 1), jnp.float32))
        inv = lax.rsqrt(square / D + norm_eps)

        def norm(i, carry):
            n = (after[i, rows, :].astype(jnp.float32) * inv * gain_ref[i]).astype(jnp.bfloat16)
            for j in range(PER):
                normed[i * PER + j, rows, :] = n[:, j * K:(j + 1) * K]
            return carry

        lax.fori_loop(0, T, norm, 0)
        go(None, remote(
            normed.at[pl.ds(t * PER, PER), pl.ds(r * HR, HR)],
            normed.at[pl.ds(t * PER, PER), pl.ds(R + r * HR, HR)],
            n_send.at[0, r], n_recv.at[t, r], (n1, t)))

    weight("A", 2, 0, cond=outer)
    weight("A", 2, 1)

    def passed(g, r):
        return normed.at[pl.ds(g * PER, PER), pl.ds(R + r * HR, HR)]

    TM = 256

    def gate_up(src, first, last, begin=False):
        def tile(r, carry):
            rows = pl.ds(pl.multiple_of(r * TM, TM), TM)
            a = normed[src, rows, :]
            for m, acc in ((0, ga), (1, ua)):
                value = dot(a, G[m, src])
                if begin:
                    acc[rows, :] = value
                else:
                    acc[rows, :] += value
            return carry
        lax.fori_loop(first // TM, last // TM, tile, 0)

    def local_done(width):
        place = G.at[:, s, :, pl.ds(0, width)]
        pltpu.make_async_copy(place, place, loc.at[2]).wait()

    split(wide, None, local_done)
    for m, h in GU:
        pass_on(m, h, fr, mid)
    gate_up(s, 0, R, True)
    gate_up(n1, 0, R)
    pass_on(1, 0, ot, outer)
    weight("X", 2, 0, cond=outer)
    for src in (xp, n1_x):
        for m, h in GU:
            recv(m, src, h)
        gate_up(src, 0, R)
    pass_on(1, 0, ot, mid)
    for r in range(2):
        landed(passed(t, r), n_recv.at[t, r])
        go(None, remote(passed(t, r), passed(t, r), n_send.at[1, r], n_recv.at[t, r], (s, ty)))
        go(None, remote(passed(t, r), passed(t, r), n_send.at[2, r], n_recv.at[t, r], (s, tc)))
    pass_on(0, 1, ot, mid)
    pass_on(1, 1, ot, mid)
    for m, h in DN:
        weight("X", m, h, cond=mid)
    pass_on(0, 1, fr, outer)
    for r in range(2):
        landed(passed(ty, r), n_recv.at[ty, r])
        go(None, remote(passed(ty, r), passed(ty, r), n_send.at[3, r], n_recv.at[ty, r], (s, tc)))
    for m, h in DN:
        recv(m, n1, h, mid)
        weight("X", m, h, src=n1, cond=mid)
        weight("D", m, h, src=n1, cond=mid)
        if h == 1:
            weight("C", m, h, cond=mid)
        weight("B", m, h, cond=mid)
    pass_on(0, 1, ot, outer)
    for g in (tc, td):
        for r in range(2):
            landed(passed(g, r), n_recv.at[g, r])
    gate_up(s, R, 2 * R, True)
    gate_up(n1, R, 2 * R)
    pass_on(1, 1, fr, outer)
    gate_up(xp, R, 2 * R)
    gate_up(n1_x, R, 2 * R)
    pass_on(1, 1, ot, outer)
    weight("X", 2, 1, cond=outer)
    for m, h in DN:
        weight("B", m, h, cond=outer)
    pass_on(2, 0, n1, outer)
    gate_up(fr, 0, 2 * R)
    gate_up(ot, 0, 2 * R)
    for m, h in GU:
        recv(m, fr_x, h)
    gate_up(fr_x, 0, 2 * R)
    for m, h in GU:
        recv(m, ot_x, h)
    pass_on(2, 1, n1, outer)
    gate_up(ot_x, 0, 2 * R)

    def act(r, carry):
        rows = pl.ds(pl.multiple_of(r * 32, 32), 32)
        g = ga[rows, :]
        hidden[rows, :] = (g / (1.0 + jnp.exp(-g)) * ua[rows, :]).astype(jnp.bfloat16)
        return carry

    lax.fori_loop(0, 2 * R // 32, act, 0)

    def slot(k):
        return k // PER // 2 * PER + k % PER

    def handed(k, h):
        return remote(dsend.at[k, h], drecv.at[k, h], d_send.at[slot(k), h], d_recv.at[slot(k), h], (s, tc))

    def across(j, h):
        return remote(ysend.at[j, h], yrecv.at[j, h], y_send.at[j, h], y_recv.at[j, h], (s, ty))

    def over(j, h):
        return remote(nsend.at[j, h], nrecv.at[j, h], o_send.at[j, h], o_recv.at[j, h], (s, ty))

    def back(k, h):
        return remote(zsend.at[k, h], zrecv.at[k, h], z_send.at[slot(k), h], z_recv.at[slot(k), h], (n1, t))

    def add(out, at, *terms):
        def rows_of(i, carry):
            rows = pl.ds(pl.multiple_of(i * WINDOW, WINDOW), WINDOW)
            total = None
            for ref, where in terms:
                value = ref[(*where, rows, slice(None))].astype(jnp.float32)
                total = value if total is None else total + value
            out[(*at, rows, slice(None))] = total.astype(out.dtype)
            return carry
        lax.fori_loop(0, R // WINDOW, rows_of, 0)

    def kept(k):
        return (k // PER) % 2 == c

    def down(k, *hs):
        given = jnp.logical_not(kept(k))
        value = dot(hidden[...], G[2, k, hs[0] * HK:(hs[-1] + 1) * HK, :], NT).astype(jnp.bfloat16)
        for r in (1, 0):
            for i, h in enumerate(hs):
                dsend[k, h, r] = value[r * R:(r + 1) * R, i * HK:(i + 1) * HK]

        @pl.when(given)
        def _():
            for h in hs:
                handed(k, h).start()

        for h in hs:
            finish.append(functools.partial(when, given, handed(k, h).wait_send))

    def pair(k, h, r):
        return (dsend, (k, h, r)), (drecv, (k, h, r))

    def cross(k, *hs):
        owned, passed_to = k // PER == t, k // PER == ty
        for h in hs:
            j = k % PER

            @pl.when(kept(k))
            def _():
                landed(drecv.at[k, h], d_recv.at[slot(k), h])

            if h == 0:
                @pl.when(passed_to)
                def _():
                    add(nsend, (j, h), *pair(k, h, 1))
                    over(j, h).start()
                    add(ysend, (j, h), *pair(k, h, 0))
                    across(j, h).start()
                finish.append(functools.partial(when, passed_to, over(j, h).wait_send))
                finish.append(functools.partial(when, owned, back(k, h).wait_send))
            else:
                @pl.when(kept(k))
                def _():
                    add(zsend, (k, h), *pair(k, h, 1))
                    back(k, h).start()
                finish.append(functools.partial(when, kept(k), back(k, h).wait_send))

    def lift(k):
        j = k % PER

        @pl.when(k // PER == t)
        def _():
            terms = pair(k, 0, 1)
            landed(nrecv.at[j, 0], o_recv.at[j, 0])
            add(zsend, (k, 0), *terms, (nrecv, (j, 0)))
            back(k, 0).start()

    def settle(k, *hs):
        for h in hs:
            @pl.when(k // PER == t)
            def _():
                terms = pair(k, h, 0)
                landed(zrecv.at[k, h], z_recv.at[slot(k), h])
                add(own_sum, (k % PER, h), *terms, (zrecv, (k, h)))

    def passing(k):
        j = k % PER

        @pl.when(k // PER == ty)
        def _():
            terms = pair(k, 1, 0)
            landed(zrecv.at[k, 1], z_recv.at[slot(k), 1])
            add(ysend, (j, 1), *terms, (zrecv, (k, 1)))
            across(j, 1).start()

    def halves(src, *hs):
        for h in hs:
            recv(2, src, h)

    down(s, 0, 1)
    down(n1, 0, 1)
    cross(s, 0, 1)
    pass_on(2, 0, ot)
    halves(xp, 0, 1)
    down(xp, 0, 1)
    cross(n1, 0, 1)
    pass_on(2, 0, fr)
    halves(n1_x, 0, 1)
    down(n1_x, 0, 1)
    cross(xp, 0, 1)
    down(ot, 0)
    cross(n1_x, 0, 1)
    down(fr, 0)
    cross(ot, 0)
    halves(ot_x, 0)
    down(ot_x, 0)
    cross(fr, 0)
    lift(s)
    lift(n1)
    pass_on(2, 1, one)
    down(one, 1)
    cross(ot_x, 0)
    lift(xp)
    pass_on(2, 1, two)
    halves(fr_x, 0)
    down(fr_x, 0)
    cross(one, 1)
    lift(n1_x)
    passing(s)
    passing(n1)
    down(two, 1)
    cross(fr_x, 0)
    cross(two, 1)
    lift(ot)
    halves(one_x, 1)
    down(one_x, 1)
    cross(one_x, 1)
    lift(fr)
    passing(xp)
    passing(n1_x)
    halves(two_x, 1)
    down(two_x, 1)
    cross(two_x, 1)
    lift(ot_x)
    lift(fr_x)
    passing(one)
    passing(two)
    passing(one_x)
    passing(two_x)
    for k in (s, n1, xp, n1_x):
        settle(k, 0, 1)
    for k, h in ((ot, 0), (fr, 0), (ot_x, 0), (one, 1), (fr_x, 0), (two, 1), (one_x, 1), (two_x, 1)):
        settle(k, h)

    for h in (0, 1):
        for j in range(PER):
            landed(yrecv.at[j, h], y_recv.at[j, h])
            cols = slice((j * 2 + h) * HK, (j * 2 + h + 1) * HK)
            out_v[:, cols] = (
                after[t, :, cols].astype(jnp.float32) + (own_sum[j, h] + yrecv[j, h].astype(jnp.float32))
            ).astype(jnp.bfloat16)
            cp = pltpu.make_async_copy(out_v.at[:, cols], out_hbm.at[:, cols], o_sem.at[0])
            cp.start()

    weights_sent("A", 1)
    weights_sent("B", 1)
    weights_sent("C", 1, mid)
    weights_sent("D", 1, mid)
    weights_sent("X", 4)
    for i, to in enumerate((ty, tc, tc)):
        remote(ow_v.at[0], ow_v.at[0], ow_send.at[i], ow_recv.at[0], (s, to)).wait_send()
    for f in finish:
        f()
    for j in range(PER):
        for h in (0, 1):
            across(j, h).wait_send()
    pltpu.make_async_copy(out_v, out_hbm, o_sem.at[0]).wait()


def fused(residual, queries, keys, values, documents, sinks, out_weight, norm_gain, gate_weight, up_weight, down_weight):
    S, T = lax.axis_size("sp"), lax.axis_size("tp")
    R, D = residual.shape
    F = gate_weight.shape[1]
    C, K = D // T, D // S
    W = (F // 128 + 1) // 2 * 128
    N = F - W
    PER = C // K
    blocks = R // WINDOW
    HK = K // 2
    bf, f32 = jnp.bfloat16, jnp.float32
    hbm = pl.BlockSpec(memory_space=pl.ANY)
    dma = pltpu.SemaphoreType.DMA
    scratch = [
        pltpu.VMEM((R, queries.shape[1]), bf),
        pltpu.VMEM((blocks, WINDOW), jnp.int32),
        pltpu.VMEM((T, 1, C), f32),
        pltpu.VMEM((R, C), bf),
        pltpu.VMEM((3, S, K, W), bf),
        pltpu.VMEM((R + WINDOW, keys.shape[1]), bf),
        pltpu.VMEM((R + WINDOW, keys.shape[1]), bf),
        pltpu.VMEM((blocks * 8 + 8, WINDOW), jnp.int32),
        pltpu.VMEM((T, R, queries.shape[1]), bf),
        pltpu.VMEM((T, R, C), bf),
        pltpu.VMEM((T, T, out_weight.shape[0], C), bf),
        pltpu.VMEM((T, R, C), bf),
        pltpu.VMEM((S, 2 * R, K), bf),
        pltpu.VMEM((2 * R, W), f32),
        pltpu.VMEM((2 * R, W), f32),
        pltpu.VMEM((2 * R, W), bf),
        pltpu.VMEM((S, 2, 2, R, HK), bf),
        pltpu.VMEM((S, 2, 2, R, HK), bf),
        pltpu.VMEM((PER, 2, R, HK), bf),
        pltpu.VMEM((PER, 2, R, HK), bf),
        pltpu.VMEM((S, 2, R, HK), bf),
        pltpu.VMEM((S, 2, R, HK), bf),
        pltpu.VMEM((PER, 2, R, HK), f32),
        pltpu.VMEM((PER, 2, R, HK), bf),
        pltpu.VMEM((PER, 2, R, HK), bf),
        dma((5,)), dma((3, S, 2)), dma((3,)), dma((3,)), dma((8,)),
        dma((3,)), dma((T + 2,)), dma((3,)), dma((T,)), dma((4, 2)), dma((T, 2)),
        dma((S // 2, 2)), dma((S // 2, 2)), dma((PER, 2)), dma((PER, 2)), dma((S // 2, 2)), dma((S // 2, 2)),
        dma((1,)), dma((PER, 2)), dma((PER, 2)),
    ]
    return pl.pallas_call(
        functools.partial(kernel, S, T, W, N),
        out_shape=jax.ShapeDtypeStruct((R, C), bf),
        in_specs=[hbm] * 5 + [pl.BlockSpec(memory_space=pltpu.SMEM)] + [hbm] * 5,
        out_specs=hbm,
        scratch_shapes=scratch,
        compiler_params=pltpu.CompilerParams(
            collective_id=0, has_side_effects=True, vmem_limit_bytes=60 * 2**20),
    )(residual, queries, keys, values, documents.reshape(blocks, WINDOW), sinks, out_weight, norm_gain.reshape(T, 1, C),
      gate_weight, up_weight, down_weight)


def line_of_four_pairs(mesh):
    return mesh.shape["sp"] == 8 and mesh.shape["tp"] == 4


def solution(mesh):
    return jax.shard_map(
        fused if line_of_four_pairs(mesh) else on_device,
        mesh=mesh,
        in_specs=(
            P("sp", None),
            P("sp", "tp"),
            P("sp", "tp"),
            P("sp", "tp"),
            P("sp"),
            P("tp"),
            P("tp", None),
            P(),
            P("sp", "tp"),
            P("sp", "tp"),
            P("sp", "tp"),
        ),
        out_specs=P("sp", "tp"),
        check_vma=False,
    )
```

```python
import functools

import jax
import jax.numpy as jnp
from jax import lax
from jax.experimental import pallas as pl
from jax.experimental.pallas import tpu as pltpu
from jax.sharding import PartitionSpec as P

HEAD_DIM = 64
WINDOW = 128
GROUP = 2


neg_big = -1e30
norm_eps = 1e-05


def from_behind(shard, axis, by):
    length = lax.axis_size(axis)
    pairs = [(i, i + by) for i in range(length) if 0 <= i + by < length]
    return lax.ppermute(shard, axis, pairs)


def attend(queries, keys, values, documents, sinks, tail_keys, tail_values, tail_docs, offset):
    rows_here = queries.shape[0]
    block_count = rows_here // WINDOW
    kv_here = keys.shape[1] // HEAD_DIM
    q_blocks = queries.reshape(block_count, WINDOW, kv_here, GROUP, HEAD_DIM)
    k_blocks = keys.reshape(block_count, WINDOW, kv_here, HEAD_DIM)
    v_blocks = values.reshape(block_count, WINDOW, kv_here, HEAD_DIM)
    k_prev = jnp.concatenate(
        [tail_keys.reshape(1, WINDOW, kv_here, HEAD_DIM), k_blocks[:-1]], axis=0
    )
    v_prev = jnp.concatenate(
        [tail_values.reshape(1, WINDOW, kv_here, HEAD_DIM), v_blocks[:-1]], axis=0
    )
    k_band = jnp.concatenate([k_prev, k_blocks], axis=1)
    v_band = jnp.concatenate([v_prev, v_blocks], axis=1)
    doc_own = documents.astype(jnp.float32).reshape(block_count, WINDOW)
    doc_prev = jnp.concatenate(
        [tail_docs.astype(jnp.float32).reshape(1, WINDOW), doc_own[:-1]], axis=0
    )
    doc_band = jnp.concatenate([doc_prev, doc_own], axis=1)
    row_idx = jnp.arange(WINDOW, dtype=jnp.int32)
    col_idx = jnp.arange(2 * WINDOW, dtype=jnp.int32)
    first = offset + jnp.arange(block_count, dtype=jnp.int32) * WINDOW
    q_pos = first[:, None] + row_idx[None, :]
    k_pos = first[:, None] - WINDOW + col_idx[None, :]
    distance = q_pos[:, :, None] - k_pos[:, None, :]
    visible = (
        (distance >= 0)
        & (distance < WINDOW)
        & (k_pos[:, None, :] >= 0)
        & (doc_own[:, :, None] == doc_band[:, None, :])
    )
    scores = jnp.einsum(
        "nikgd,njkd->nkgij", q_blocks, k_band, preferred_element_type=jnp.float32
    ) * HEAD_DIM ** (-0.5)
    scores = jnp.where(visible[:, None, None], scores, neg_big)
    sink_logit = sinks.reshape(1, kv_here, GROUP, 1, 1)
    row_max = jnp.maximum(scores.max(-1, keepdims=True), sink_logit)
    expo = jnp.where(visible[:, None, None], jnp.exp(scores - row_max), 0.0)
    denom_sum = expo.sum(-1, keepdims=True) + jnp.exp(sink_logit - row_max)
    weights = (expo / denom_sum).astype(jnp.bfloat16)
    mixed = jnp.einsum("nkgij,njkd->nikgd", weights, v_band, preferred_element_type=jnp.float32)
    return mixed.reshape(rows_here, kv_here * GROUP * HEAD_DIM).astype(jnp.bfloat16)


def on_device(
    residual,
    queries,
    keys,
    values,
    documents,
    sinks,
    out_weight,
    norm_gain,
    gate_weight,
    up_weight,
    down_weight,
):
    rows_here = queries.shape[0]
    offset = lax.axis_index("sp") * rows_here
    doc_tail = documents[rows_here - WINDOW :].astype(jnp.bfloat16)
    tail_keys, tail_values, tail_docs = from_behind(
        (keys[rows_here - WINDOW :], values[rows_here - WINDOW :], doc_tail), "sp", 1
    )
    attended = attend(
        queries, keys, values, documents, sinks, tail_keys, tail_values, tail_docs, offset
    )
    model_width = residual.shape[1]
    col_count = model_width // lax.axis_size("tp")
    col_first = lax.axis_index("tp") * col_count
    full_term = jnp.dot(attended, out_weight, preferred_element_type=jnp.float32)
    projected = lax.psum(full_term.astype(jnp.bfloat16), "tp").astype(jnp.float32)
    after_full = (residual.astype(jnp.float32) + projected).astype(jnp.bfloat16)
    after_f = after_full.astype(jnp.float32)
    inv_rms = lax.rsqrt(jnp.mean(after_f * after_f, axis=1, keepdims=True) + norm_eps)
    normed = (after_f * inv_rms * norm_gain[None, :]).astype(jnp.bfloat16)
    after = lax.dynamic_slice_in_dim(after_full, col_first, col_count, 1)
    gate_act = jnp.dot(
        normed,
        lax.all_gather(gate_weight, "sp", axis=0, tiled=True),
        preferred_element_type=jnp.float32,
    )
    up_act = jnp.dot(
        normed,
        lax.all_gather(up_weight, "sp", axis=0, tiled=True),
        preferred_element_type=jnp.float32,
    )
    down_full = lax.all_gather(down_weight, "sp", axis=0, tiled=True)
    hidden = (jax.nn.silu(gate_act) * up_act).astype(jnp.bfloat16)
    summed = lax.psum_scatter(
        lax.dot_general(
            down_full, hidden, (((1,), (1,)), ((), ())), preferred_element_type=jnp.float32
        ).astype(jnp.bfloat16),
        "tp",
        scatter_dimension=0,
        tiled=True,
    ).astype(jnp.float32)
    return (after.astype(jnp.float32) + summed.T).astype(jnp.bfloat16)


MESH = pl.DeviceIdType.MESH
NT = (((1,), (1,)), ((), ()))


def dot(a, b, dims=(((1,), (0,)), ((), ()))):
    return lax.dot_general(a, b, dims, preferred_element_type=jnp.float32)


def when(cond, f):
    if cond is None:
        f()
    else:
        pl.when(cond)(f)


def kernel(
    S, T, W, N,
    res_hbm, q_hbm, k_hbm, v_hbm, doc_hbm, sink_ref, ow_hbm, gain_hbm, g_hbm, u_hbm, d_hbm,
    out_ref,
    q_ref, doc_ref, gain_ref,
    G, kx, vx, dx, att, res_v, ow_v, after, normed, ga, ua, hidden, dsend, drecv, ysend, yrecv, zsend, zrecv, own_sum, nsend, nrecv,
    w_send, w_recv, last_recv, tail_send, tail_recv, loc, ow_send, ow_recv, att_send, att_recv, n_send, n_recv,
    d_send, d_recv, y_send, y_recv, z_send, z_recv, o_send, o_recv,
):
    s = lax.axis_index("sp")
    t = lax.axis_index("tp")
    R = q_ref.shape[0]
    C = gain_ref.shape[2]
    D = T * C
    K = D // S
    F = g_hbm.shape[1]
    HK = K // 2
    PER = C // K
    z, x = s // 2, s % 2
    p, c = z % 2, t % 2
    wide = p == c
    n1_z, fr_z, ot_z = z + 1 - 2 * p, (z + 2) % 4, 3 - z
    xp = z * 2 + 1 - x
    n1, fr, ot = n1_z * 2 + x, fr_z * 2 + x, ot_z * 2 + x
    n1_x, fr_x, ot_x = n1_z * 2 + 1 - x, fr_z * 2 + 1 - x, ot_z * 2 + 1 - x
    mid = (z == 1) | (z == 2)
    one, two = jnp.where(mid, fr, ot), jnp.where(mid, ot, fr)
    one_x, two_x = jnp.where(mid, fr_x, ot_x), jnp.where(mid, ot_x, fr_x)
    outer = (z == 0) | (z == 3)
    tc = t + 1 - 2 * c
    ty = (t + 2) % T

    weights = (g_hbm, u_hbm, d_hbm)
    ow_parts = [
        pltpu.make_async_copy(ow_hbm.at[:, i * C:(i + 1) * C], ow_v.at[t, i], loc.at[0]) for i in range(T)
    ]
    res_parts = [
        pltpu.make_async_copy(res_hbm.at[:, i * C:(i + 1) * C], res_v.at[i], loc.at[1]) for i in range(T)
    ]
    firsts = [
        pltpu.make_async_copy(a, b, loc.at[3 + i]) for i, (a, b) in enumerate((
            (doc_hbm, doc_ref), (k_hbm, kx.at[pl.ds(WINDOW, R)]), (v_hbm, vx.at[pl.ds(WINDOW, R)]),
            (q_hbm, q_ref), (gain_hbm, gain_ref)))
    ]
    for cp in firsts + ow_parts + res_parts:
        cp.start()

    def split(is_wide, cond, f):
        for flag, width in ((is_wide, W), (jnp.logical_not(is_wide), N)):
            both = flag if cond is None else flag & cond
            pl.when(both)(functools.partial(f, width))

    def columns(q, width):
        return pl.ds(pl.multiple_of(q * (F - width), 128), width)

    def local(m, width):
        return pltpu.make_async_copy(
            weights[m].at[:, columns(p, width)], G.at[m, s, :, pl.ds(0, width)], loc.at[2])

    for m in range(3):
        split(wide, None, lambda width: local(m, width).start())

    barrier = pltpu.get_barrier_semaphore()
    peers = [(xp, t, None), (fr, t, None), (n1, t, None), (ot, t, mid)]
    peers += [(s, (t + d) % T, None) for d in range(1, T)]
    peers += [((s + 1) % S, t, (x == 1) & (z < 3)), ((s + S - 1) % S, t, (x == 0) & (z > 0))]
    for a, b, cond in peers:
        when(cond, lambda: pl.semaphore_signal(barrier, inc=1, device_id=(a, b), device_id_type=MESH))
    present = sum(1 if cond is None else cond.astype(jnp.int32) for _, _, cond in peers)
    pl.semaphore_wait(barrier, present)

    firsts[0].wait()
    blocks = doc_ref.shape[0]
    for i in range(blocks):
        dx[8 + 8 * i:16 + 8 * i, :] = jnp.broadcast_to(doc_ref[i:i + 1, :], (8, WINDOW))
    finish = []

    def go(cond, cp):
        when(cond, cp.start)
        finish.append(lambda: when(cond, cp.wait_send))

    def start(cp):
        cp.start()

    def remote(src, dst, send_sem, recv_sem, to):
        return pltpu.make_async_remote_copy(
            src_ref=src, dst_ref=dst, send_sem=send_sem, recv_sem=recv_sem, device_id=to, device_id_type=MESH)

    tails = []
    for i, (a, b) in enumerate((
        (k_hbm.at[pl.ds(R - WINDOW, WINDOW)], kx.at[pl.ds(0, WINDOW)]),
        (v_hbm.at[pl.ds(R - WINDOW, WINDOW)], vx.at[pl.ds(0, WINDOW)]),
        (dx.at[pl.ds(8 * blocks, 8)], dx.at[pl.ds(0, 8)]),
    )):
        cp = remote(a, b, tail_send.at[i], tail_recv.at[i], ((s + 1) % S, t))
        go(s < S - 1, cp)
        tails.append(cp)

    kinds = {"A": (1 - p, n1), "B": (p, fr), "C": (1 - p, ot), "D": (p, fr), "X": (p, xp)}

    def weight(kind, m, h, src=None, cond=None, part=None):
        q, to = kinds[kind]
        rows = pl.ds(h * HK, HK) if part is None else pl.ds(h * HK + part * HK // 2, HK // 2)
        sem = w_send.at["ABCDX".index(kind)]
        arrived = last_recv.at[int(kind == "X")] if part == 1 else w_recv.at[m, s if src is None else src, h]

        def copy(width):
            cols = pl.ds(0, width)
            if src is None:
                return remote(weights[m].at[rows, columns(q, width)], G.at[m, s, rows, cols],
                              sem, arrived, (to, t))
            place = G.at[m, src, rows, cols]
            return remote(place, place, sem, arrived, (to, t))

        split(q == c, cond, lambda width: copy(width).start())

    def weights_sent(kind, sources, cond=None):
        q, to = kinds[kind]

        def wait(width):
            place = G.at[:, pl.ds(0, sources), :, pl.ds(0, width)]
            remote(place, place, w_send.at["ABCDX".index(kind)], w_recv.at[0, 0, 0], (to, t)).wait_send()

        split(q == c, cond, wait)

    def recv(m, src, h, cond=None):
        def wait(width):
            place = G.at[m, src, pl.ds(h * HK, HK), pl.ds(0, width)]
            remote(place, place, w_send.at[0], w_recv.at[m, src, h], (xp, t)).wait_recv()
        split(wide, cond, wait)

    def recv_last(src, x_link, part):
        sem = last_recv.at[x_link] if part == 1 else w_recv.at[2, src, 1]

        def wait(width):
            place = G.at[2, src, pl.ds(HK + part * HK // 2, HK // 2), pl.ds(0, width)]
            remote(place, place, w_send.at[0], sem, (xp, t)).wait_recv()
        split(wide, None, wait)

    def landed(ref, sem):
        remote(ref, ref, w_send.at[0], sem, (s, tc)).wait_recv()

    GU = ((0, 0), (1, 0), (0, 1), (1, 1))
    DN = ((2, 0), (2, 1))

    for m, h in GU:
        weight("A", m, h)
        weight("X", m, h)
    for i in range(T):
        part = ow_hbm.at[:, i * C:(i + 1) * C]
        start(remote(part, ow_v.at[t, i], ow_send.at[0], ow_recv.at[i], (s, ty)))
        start(remote(part, ow_v.at[t, i], ow_send.at[1], ow_recv.at[T], (s, tc)))
    weight("A", 2, 0, cond=mid)
    weight("C", 0, 0, cond=mid)
    for m, h in GU[:2]:
        weight("B", m, h)
    for m, h in GU[2:]:
        weight("B", m, h, cond=outer)

    @pl.when(jnp.logical_not(wide))
    def _():
        def clear(i, carry):
            for m in range(3):
                G[m, i, :, N:W] = jnp.zeros((K, W - N), jnp.bfloat16)
            return carry
        if W > N:
            lax.fori_loop(0, S, clear, 0)

    @pl.when(s == 0)
    def _():
        kx[pl.ds(0, WINDOW), :] = jnp.zeros((WINDOW, kx.shape[1]), jnp.bfloat16)
        vx[pl.ds(0, WINDOW), :] = jnp.zeros((WINDOW, vx.shape[1]), jnp.bfloat16)
        dx[pl.ds(0, 8), :] = jnp.zeros((8, dx.shape[1]), jnp.int32)

    for cp in firsts[1:]:
        cp.wait()
    for cp in tails:
        when(s > 0, cp.wait_recv)
    heads = q_ref.shape[1] // HEAD_DIM

    def block(b, carry):
        rows = pl.ds(pl.multiple_of(b * WINDOW, WINDOW), WINDOW)
        band = pl.ds(pl.multiple_of(b * WINDOW, WINDOW), 2 * WINDOW)
        prev = dx[pl.ds(pl.multiple_of(b * 8, 8), 8), :][0:1].astype(jnp.float32)
        own = dx[pl.ds(pl.multiple_of(b * 8 + 8, 8), 8), :][0:1].astype(jnp.float32)
        doc_q = jnp.broadcast_to(own, (WINDOW, WINDOW)).T
        i = lax.broadcasted_iota(jnp.int32, (WINDOW, WINDOW), 0)
        j = lax.broadcasted_iota(jnp.int32, (WINDOW, WINDOW), 1)
        first = s * R + b * WINDOW - WINDOW
        see_prev = (j > i) & (doc_q == prev) & (first + j >= 0)
        see_own = (j <= i) & (doc_q == own)
        visible = jnp.concatenate(
            [see_prev.astype(jnp.float32), see_own.astype(jnp.float32)], axis=1) > 0.5
        for h in range(heads):
            kv = h // GROUP
            cols = slice(kv * HEAD_DIM, (kv + 1) * HEAD_DIM)
            q = q_ref[rows, h * HEAD_DIM:(h + 1) * HEAD_DIM]
            scores = dot(q, kx[band, cols], NT) * HEAD_DIM ** (-0.5)
            scores = jnp.where(visible, scores, neg_big)
            sink = sink_ref[h]
            row_max = jnp.maximum(scores.max(-1, keepdims=True), sink)
            expo = jnp.where(visible, jnp.exp(scores - row_max), 0.0)
            total = expo.sum(-1, keepdims=True) + jnp.exp(sink - row_max)
            w = (expo / total).astype(jnp.bfloat16)
            att[t, rows, h * HEAD_DIM:(h + 1) * HEAD_DIM] = dot(w, vx[band, cols]).astype(jnp.bfloat16)
        return carry

    lax.fori_loop(0, R // WINDOW, block, 0)

    go(None, remote(att.at[t], att.at[t], att_send.at[0], att_recv.at[t], (s, ty)))
    go(None, remote(att.at[t], att.at[t], att_send.at[1], att_recv.at[t], (s, tc)))

    def ow_relay(i):
        landed(ow_v.at[ty, i], ow_recv.at[i])
        start(remote(ow_v.at[ty, i], ow_v.at[ty, i], ow_send.at[2], ow_recv.at[T + 1], (s, tc)))

    def pass_on(m, h, src, cond=None):
        recv(m, src, h, cond)
        weight("X", m, h, src=src, cond=cond)

    pass_on(0, 0, n1)
    weight("D", 0, 0, src=n1, cond=mid)
    pass_on(1, 0, n1)
    weight("D", 1, 0, src=n1, cond=mid)
    for m, h in GU[1:]:
        weight("C", m, h, cond=mid)
    weight("B", 0, 1, cond=mid)
    ow_relay(0)
    pass_on(0, 0, fr, outer)
    ow_relay(1)
    pass_on(0, 1, n1)
    weight("D", 0, 1, src=n1, cond=mid)
    weight("B", 1, 1, cond=mid)
    pass_on(1, 1, n1)
    weight("D", 1, 1, src=n1, cond=mid)
    weight("C", 2, 0, cond=mid)
    ow_relay(2)
    pass_on(0, 0, ot, mid)
    pass_on(1, 0, fr, outer)
    ow_relay(3)
    pass_on(0, 0, ot, outer)
    landed(att.at[ty], att_recv.at[ty])
    go(None, remote(att.at[ty], att.at[ty], att_send.at[2], att_recv.at[ty], (s, tc)))
    pltpu.make_async_copy(ow_v.at[t], ow_v.at[t], loc.at[0]).wait()
    pltpu.make_async_copy(res_v, res_v, loc.at[1]).wait()
    td = (tc + 2) % T
    for i, g in enumerate((tc, td)):
        landed(ow_v.at[g], ow_recv.at[T + i])
        landed(att.at[g], att_recv.at[g])

    HR = R // 2
    for r in range(2):
        rows = slice(r * HR, (r + 1) * HR)

        def project(i, square):
            total = dot(att[0, rows, :], ow_v[0, i]).astype(jnp.bfloat16).astype(jnp.float32)
            for g in range(1, T):
                total += dot(att[g, rows, :], ow_v[g, i]).astype(jnp.bfloat16).astype(jnp.float32)
            value = (res_v[i, rows, :].astype(jnp.float32) + total).astype(jnp.bfloat16)
            after[i, rows, :] = value
            value = value.astype(jnp.float32)
            return square + (value * value).sum(-1, keepdims=True)

        square = lax.fori_loop(0, T, project, jnp.zeros((HR, 1), jnp.float32))
        inv = lax.rsqrt(square / D + norm_eps)

        def norm(i, carry):
            n = (after[i, rows, :].astype(jnp.float32) * inv * gain_ref[i]).astype(jnp.bfloat16)
            for j in range(PER):
                normed[i * PER + j, rows, :] = n[:, j * K:(j + 1) * K]
            return carry

        lax.fori_loop(0, T, norm, 0)
        go(None, remote(
            normed.at[pl.ds(t * PER, PER), pl.ds(r * HR, HR)],
            normed.at[pl.ds(t * PER, PER), pl.ds(R + r * HR, HR)],
            n_send.at[0, r], n_recv.at[t, r], (n1, t)))

    weight("A", 2, 0, cond=outer)
    weight("A", 2, 1)

    def passed(g, r):
        return normed.at[pl.ds(g * PER, PER), pl.ds(R + r * HR, HR)]

    TM = 256

    def gate_up(src, first, last, begin=False):
        def tile(r, carry):
            rows = pl.ds(pl.multiple_of(r * TM, TM), TM)
            a = normed[src, rows, :]
            for m, acc in ((0, ga), (1, ua)):
                value = dot(a, G[m, src])
                if begin:
                    acc[rows, :] = value
                else:
                    acc[rows, :] += value
            return carry
        lax.fori_loop(first // TM, last // TM, tile, 0)

    def local_done(width):
        place = G.at[:, s, :, pl.ds(0, width)]
        pltpu.make_async_copy(place, place, loc.at[2]).wait()

    split(wide, None, local_done)
    for m, h in GU:
        pass_on(m, h, fr, mid)
    gate_up(s, 0, R, True)
    gate_up(n1, 0, R)
    pass_on(1, 0, ot, outer)
    weight("X", 2, 0, cond=outer)
    for src in (xp, n1_x):
        for m, h in GU:
            recv(m, src, h)
        gate_up(src, 0, R)
    pass_on(1, 0, ot, mid)
    for r in range(2):
        landed(passed(t, r), n_recv.at[t, r])
        go(None, remote(passed(t, r), passed(t, r), n_send.at[1, r], n_recv.at[t, r], (s, ty)))
        go(None, remote(passed(t, r), passed(t, r), n_send.at[2, r], n_recv.at[t, r], (s, tc)))
    pass_on(0, 1, ot, mid)
    pass_on(1, 1, ot, mid)
    for m, h in DN:
        weight("X", m, h, cond=mid)
    pass_on(0, 1, fr, outer)
    for r in range(2):
        landed(passed(ty, r), n_recv.at[ty, r])
        go(None, remote(passed(ty, r), passed(ty, r), n_send.at[3, r], n_recv.at[ty, r], (s, tc)))
    for m, h in DN:
        recv(m, n1, h, mid)
        weight("X", m, h, src=n1, cond=mid)
        weight("D", m, h, src=n1, cond=mid)
        if h == 0:
            weight("B", m, h, cond=mid)
    for part in (0, 1):
        weight("B", 2, 1, cond=mid, part=part)
        weight("C", 2, 1, cond=mid, part=part)
    pass_on(0, 1, ot, outer)
    for g in (tc, td):
        for r in range(2):
            landed(passed(g, r), n_recv.at[g, r])
    gate_up(s, R, 2 * R, True)
    gate_up(n1, R, 2 * R)
    pass_on(1, 1, fr, outer)
    gate_up(xp, R, 2 * R)
    gate_up(n1_x, R, 2 * R)
    pass_on(1, 1, ot, outer)
    weight("X", 2, 1, cond=outer)
    for m, h in DN:
        weight("B", m, h, cond=outer)
    pass_on(2, 0, n1, outer)
    gate_up(fr, 0, 2 * R)
    gate_up(ot, 0, 2 * R)
    for m, h in GU:
        recv(m, fr_x, h)
    gate_up(fr_x, 0, 2 * R)
    for m, h in GU:
        recv(m, ot_x, h)
    pass_on(2, 1, n1, outer)
    gate_up(ot_x, 0, 2 * R)

    def act(r, carry):
        rows = pl.ds(pl.multiple_of(r * 32, 32), 32)
        g = ga[rows, :]
        hidden[rows, :] = (g / (1.0 + jnp.exp(-g)) * ua[rows, :]).astype(jnp.bfloat16)
        return carry

    lax.fori_loop(0, 2 * R // 32, act, 0)

    def slot(k):
        return k // PER // 2 * PER + k % PER

    def handed(k, h):
        return remote(dsend.at[k, h], drecv.at[k, h], d_send.at[slot(k), h], d_recv.at[slot(k), h], (s, tc))

    def across(j, h):
        return remote(ysend.at[j, h], yrecv.at[j, h], y_send.at[j, h], y_recv.at[j, h], (s, ty))

    def over(j, h):
        return remote(nsend.at[j, h], nrecv.at[j, h], o_send.at[j, h], o_recv.at[j, h], (s, ty))

    def back(k, h):
        return remote(zsend.at[k, h], zrecv.at[k, h], z_send.at[slot(k), h], z_recv.at[slot(k), h], (n1, t))

    def add(out, at, *terms):
        def rows_of(i, carry):
            rows = pl.ds(pl.multiple_of(i * WINDOW, WINDOW), WINDOW)
            total = None
            for ref, where in terms:
                value = ref[(*where, rows, slice(None))].astype(jnp.float32)
                total = value if total is None else total + value
            out[(*at, rows, slice(None))] = total.astype(out.dtype)
            return carry
        lax.fori_loop(0, R // WINDOW, rows_of, 0)

    def kept(k):
        return (k // PER) % 2 == c

    def down(k, *hs):
        given = jnp.logical_not(kept(k))
        value = dot(hidden[...], G[2, k, hs[0] * HK:(hs[-1] + 1) * HK, :], NT).astype(jnp.bfloat16)
        for r in (1, 0):
            for i, h in enumerate(hs):
                dsend[k, h, r] = value[r * R:(r + 1) * R, i * HK:(i + 1) * HK]

        @pl.when(given)
        def _():
            for h in hs:
                handed(k, h).start()

        for h in hs:
            finish.append(functools.partial(when, given, handed(k, h).wait_send))

    def pair(k, h, r):
        return (dsend, (k, h, r)), (drecv, (k, h, r))

    def cross(k, *hs):
        owned, passed_to = k // PER == t, k // PER == ty
        for h in hs:
            j = k % PER

            @pl.when(kept(k))
            def _():
                landed(drecv.at[k, h], d_recv.at[slot(k), h])

            if h == 0:
                @pl.when(passed_to)
                def _():
                    add(nsend, (j, h), *pair(k, h, 1))
                    over(j, h).start()
                    add(ysend, (j, h), *pair(k, h, 0))
                    across(j, h).start()
                finish.append(functools.partial(when, passed_to, over(j, h).wait_send))
                finish.append(functools.partial(when, owned, back(k, h).wait_send))
            else:
                @pl.when(kept(k))
                def _():
                    add(zsend, (k, h), *pair(k, h, 1))
                    back(k, h).start()
                finish.append(functools.partial(when, kept(k), back(k, h).wait_send))

    def lift(k):
        j = k % PER

        @pl.when(k // PER == t)
        def _():
            terms = pair(k, 0, 1)
            landed(nrecv.at[j, 0], o_recv.at[j, 0])
            add(zsend, (k, 0), *terms, (nrecv, (j, 0)))
            back(k, 0).start()

    def settle(k, *hs):
        for h in hs:
            @pl.when(k // PER == t)
            def _():
                terms = pair(k, h, 0)
                landed(zrecv.at[k, h], z_recv.at[slot(k), h])
                add(own_sum, (k % PER, h), *terms, (zrecv, (k, h)))

    def passing(k):
        j = k % PER

        @pl.when(k // PER == ty)
        def _():
            terms = pair(k, 1, 0)
            landed(zrecv.at[k, 1], z_recv.at[slot(k), 1])
            add(ysend, (j, 1), *terms, (zrecv, (k, 1)))
            across(j, 1).start()

    def halves(src, *hs):
        for h in hs:
            recv(2, src, h)

    down(s, 0, 1)
    down(n1, 0, 1)
    cross(s, 0, 1)
    halves(xp, 0, 1)
    down(xp, 0, 1)
    cross(n1, 0, 1)
    pass_on(2, 0, ot)
    halves(n1_x, 0, 1)
    down(n1_x, 0, 1)
    cross(xp, 0, 1)
    pass_on(2, 0, fr)
    down(ot, 0)
    cross(n1_x, 0, 1)
    down(fr, 0)
    cross(ot, 0)
    halves(ot_x, 0)
    down(ot_x, 0)
    cross(fr, 0)
    lift(s)
    lift(n1)
    pass_on(2, 1, one)
    down(one, 1)
    cross(ot_x, 0)
    lift(xp)
    for part in (0, 1):
        recv_last(two, 0, part)
        weight("X", 2, 1, src=two, part=part)
    halves(fr_x, 0)
    down(fr_x, 0)
    cross(one, 1)
    lift(n1_x)
    passing(s)
    passing(n1)
    down(two, 1)
    cross(fr_x, 0)
    cross(two, 1)
    lift(ot)
    halves(one_x, 1)
    down(one_x, 1)
    cross(one_x, 1)
    lift(fr)
    passing(xp)
    passing(n1_x)
    for part in (0, 1):
        recv_last(two_x, 1, part)
    down(two_x, 1)
    cross(two_x, 1)
    lift(ot_x)
    lift(fr_x)
    passing(one)
    passing(two)
    passing(one_x)
    passing(two_x)
    for k in (s, n1, xp, n1_x):
        settle(k, 0, 1)
    for k, h in ((ot, 0), (fr, 0), (ot_x, 0), (one, 1), (fr_x, 0), (two, 1), (one_x, 1), (two_x, 1)):
        settle(k, h)

    for h in (0, 1):
        for j in range(PER):
            landed(yrecv.at[j, h], y_recv.at[j, h])
            cols = slice((j * 2 + h) * HK, (j * 2 + h + 1) * HK)
            out_ref[:, cols] = (
                after[t, :, cols].astype(jnp.float32) + (own_sum[j, h] + yrecv[j, h].astype(jnp.float32))
            ).astype(jnp.bfloat16)

    weights_sent("A", 1)
    weights_sent("B", 1)
    weights_sent("C", 1, mid)
    weights_sent("D", 1, mid)
    weights_sent("X", 4)
    for i, to in enumerate((ty, tc, tc)):
        remote(ow_v.at[0], ow_v.at[0], ow_send.at[i], ow_recv.at[0], (s, to)).wait_send()
    for f in finish:
        f()
    for j in range(PER):
        for h in (0, 1):
            across(j, h).wait_send()


def fused(residual, queries, keys, values, documents, sinks, out_weight, norm_gain, gate_weight, up_weight, down_weight):
    S, T = lax.axis_size("sp"), lax.axis_size("tp")
    R, D = residual.shape
    F = gate_weight.shape[1]
    C, K = D // T, D // S
    W = (F // 128 + 1) // 2 * 128
    N = F - W
    PER = C // K
    blocks = R // WINDOW
    HK = K // 2
    bf, f32 = jnp.bfloat16, jnp.float32
    hbm = pl.BlockSpec(memory_space=pl.ANY)
    dma = pltpu.SemaphoreType.DMA
    scratch = [
        pltpu.VMEM((R, queries.shape[1]), bf),
        pltpu.VMEM((blocks, WINDOW), jnp.int32),
        pltpu.VMEM((T, 1, C), f32),
        pltpu.VMEM((3, S, K, W), bf),
        pltpu.VMEM((R + WINDOW, keys.shape[1]), bf),
        pltpu.VMEM((R + WINDOW, keys.shape[1]), bf),
        pltpu.VMEM((blocks * 8 + 8, WINDOW), jnp.int32),
        pltpu.VMEM((T, R, queries.shape[1]), bf),
        pltpu.VMEM((T, R, C), bf),
        pltpu.VMEM((T, T, out_weight.shape[0], C), bf),
        pltpu.VMEM((T, R, C), bf),
        pltpu.VMEM((S, 2 * R, K), bf),
        pltpu.VMEM((2 * R, W), f32),
        pltpu.VMEM((2 * R, W), f32),
        pltpu.VMEM((2 * R, W), bf),
        pltpu.VMEM((S, 2, 2, R, HK), bf),
        pltpu.VMEM((S, 2, 2, R, HK), bf),
        pltpu.VMEM((PER, 2, R, HK), bf),
        pltpu.VMEM((PER, 2, R, HK), bf),
        pltpu.VMEM((S, 2, R, HK), bf),
        pltpu.VMEM((S, 2, R, HK), bf),
        pltpu.VMEM((PER, 2, R, HK), f32),
        pltpu.VMEM((PER, 2, R, HK), bf),
        pltpu.VMEM((PER, 2, R, HK), bf),
        dma((5,)), dma((3, S, 2)), dma((2,)), dma((3,)), dma((3,)), dma((8,)),
        dma((3,)), dma((T + 2,)), dma((3,)), dma((T,)), dma((4, 2)), dma((T, 2)),
        dma((S // 2, 2)), dma((S // 2, 2)), dma((PER, 2)), dma((PER, 2)), dma((S // 2, 2)), dma((S // 2, 2)),
        dma((PER, 2)), dma((PER, 2)),
    ]
    return pl.pallas_call(
        functools.partial(kernel, S, T, W, N),
        out_shape=pltpu.VMEM((R, C), bf),
        in_specs=[hbm] * 5 + [pl.BlockSpec(memory_space=pltpu.SMEM)] + [hbm] * 5,
        out_specs=pl.BlockSpec(memory_space=pltpu.VMEM),
        scratch_shapes=scratch,
        compiler_params=pltpu.CompilerParams(
            collective_id=0, has_side_effects=True, vmem_limit_bytes=60 * 2**20),
    )(residual, queries, keys, values, documents.reshape(blocks, WINDOW), sinks, out_weight, norm_gain.reshape(T, 1, C),
      gate_weight, up_weight, down_weight)


def line_of_four_pairs(mesh):
    return mesh.shape["sp"] == 8 and mesh.shape["tp"] == 4


def solution(mesh):
    return jax.shard_map(
        fused if line_of_four_pairs(mesh) else on_device,
        mesh=mesh,
        in_specs=(
            P("sp", None),
            P("sp", "tp"),
            P("sp", "tp"),
            P("sp", "tp"),
            P("sp"),
            P("tp"),
            P("tp", None),
            P(),
            P("sp", "tp"),
            P("sp", "tp"),
            P("sp", "tp"),
        ),
        out_specs=P("sp", "tp"),
        check_vma=False,
    )
```

```python
import functools

import jax
import jax.numpy as jnp
from jax import lax
from jax.experimental import pallas as pl
from jax.experimental.pallas import tpu as pltpu
from jax.sharding import PartitionSpec as P

HEAD_DIM = 64
WINDOW = 128
GROUP = 2


neg_big = -1e30
norm_eps = 1e-05


def from_behind(shard, axis, by):
    length = lax.axis_size(axis)
    pairs = [(i, i + by) for i in range(length) if 0 <= i + by < length]
    return lax.ppermute(shard, axis, pairs)


def attend(queries, keys, values, documents, sinks, tail_keys, tail_values, tail_docs, offset):
    rows_here = queries.shape[0]
    block_count = rows_here // WINDOW
    kv_here = keys.shape[1] // HEAD_DIM
    q_blocks = queries.reshape(block_count, WINDOW, kv_here, GROUP, HEAD_DIM)
    k_blocks = keys.reshape(block_count, WINDOW, kv_here, HEAD_DIM)
    v_blocks = values.reshape(block_count, WINDOW, kv_here, HEAD_DIM)
    k_prev = jnp.concatenate(
        [tail_keys.reshape(1, WINDOW, kv_here, HEAD_DIM), k_blocks[:-1]], axis=0
    )
    v_prev = jnp.concatenate(
        [tail_values.reshape(1, WINDOW, kv_here, HEAD_DIM), v_blocks[:-1]], axis=0
    )
    k_band = jnp.concatenate([k_prev, k_blocks], axis=1)
    v_band = jnp.concatenate([v_prev, v_blocks], axis=1)
    doc_own = documents.astype(jnp.float32).reshape(block_count, WINDOW)
    doc_prev = jnp.concatenate(
        [tail_docs.astype(jnp.float32).reshape(1, WINDOW), doc_own[:-1]], axis=0
    )
    doc_band = jnp.concatenate([doc_prev, doc_own], axis=1)
    row_idx = jnp.arange(WINDOW, dtype=jnp.int32)
    col_idx = jnp.arange(2 * WINDOW, dtype=jnp.int32)
    first = offset + jnp.arange(block_count, dtype=jnp.int32) * WINDOW
    q_pos = first[:, None] + row_idx[None, :]
    k_pos = first[:, None] - WINDOW + col_idx[None, :]
    distance = q_pos[:, :, None] - k_pos[:, None, :]
    visible = (
        (distance >= 0)
        & (distance < WINDOW)
        & (k_pos[:, None, :] >= 0)
        & (doc_own[:, :, None] == doc_band[:, None, :])
    )
    scores = jnp.einsum(
        "nikgd,njkd->nkgij", q_blocks, k_band, preferred_element_type=jnp.float32
    ) * HEAD_DIM ** (-0.5)
    scores = jnp.where(visible[:, None, None], scores, neg_big)
    sink_logit = sinks.reshape(1, kv_here, GROUP, 1, 1)
    row_max = jnp.maximum(scores.max(-1, keepdims=True), sink_logit)
    expo = jnp.where(visible[:, None, None], jnp.exp(scores - row_max), 0.0)
    denom_sum = expo.sum(-1, keepdims=True) + jnp.exp(sink_logit - row_max)
    weights = (expo / denom_sum).astype(jnp.bfloat16)
    mixed = jnp.einsum("nkgij,njkd->nikgd", weights, v_band, preferred_element_type=jnp.float32)
    return mixed.reshape(rows_here, kv_here * GROUP * HEAD_DIM).astype(jnp.bfloat16)


def on_device(
    residual,
    queries,
    keys,
    values,
    documents,
    sinks,
    out_weight,
    norm_gain,
    gate_weight,
    up_weight,
    down_weight,
):
    rows_here = queries.shape[0]
    offset = lax.axis_index("sp") * rows_here
    doc_tail = documents[rows_here - WINDOW :].astype(jnp.bfloat16)
    tail_keys, tail_values, tail_docs = from_behind(
        (keys[rows_here - WINDOW :], values[rows_here - WINDOW :], doc_tail), "sp", 1
    )
    attended = attend(
        queries, keys, values, documents, sinks, tail_keys, tail_values, tail_docs, offset
    )
    model_width = residual.shape[1]
    col_count = model_width // lax.axis_size("tp")
    col_first = lax.axis_index("tp") * col_count
    full_term = jnp.dot(attended, out_weight, preferred_element_type=jnp.float32)
    projected = lax.psum(full_term.astype(jnp.bfloat16), "tp").astype(jnp.float32)
    after_full = (residual.astype(jnp.float32) + projected).astype(jnp.bfloat16)
    after_f = after_full.astype(jnp.float32)
    inv_rms = lax.rsqrt(jnp.mean(after_f * after_f, axis=1, keepdims=True) + norm_eps)
    normed = (after_f * inv_rms * norm_gain[None, :]).astype(jnp.bfloat16)
    after = lax.dynamic_slice_in_dim(after_full, col_first, col_count, 1)
    gate_act = jnp.dot(
        normed,
        lax.all_gather(gate_weight, "sp", axis=0, tiled=True),
        preferred_element_type=jnp.float32,
    )
    up_act = jnp.dot(
        normed,
        lax.all_gather(up_weight, "sp", axis=0, tiled=True),
        preferred_element_type=jnp.float32,
    )
    down_full = lax.all_gather(down_weight, "sp", axis=0, tiled=True)
    hidden = (jax.nn.silu(gate_act) * up_act).astype(jnp.bfloat16)
    summed = lax.psum_scatter(
        lax.dot_general(
            down_full, hidden, (((1,), (1,)), ((), ())), preferred_element_type=jnp.float32
        ).astype(jnp.bfloat16),
        "tp",
        scatter_dimension=0,
        tiled=True,
    ).astype(jnp.float32)
    return (after.astype(jnp.float32) + summed.T).astype(jnp.bfloat16)


MESH = pl.DeviceIdType.MESH
NT = (((1,), (1,)), ((), ()))


def dot(a, b, dims=(((1,), (0,)), ((), ()))):
    return lax.dot_general(a, b, dims, preferred_element_type=jnp.float32)


def when(cond, f):
    if cond is None:
        f()
    else:
        pl.when(cond)(f)


def kernel(
    S, T, W, N,
    res_hbm, q_hbm, k_hbm, v_hbm, doc_hbm, sink_ref, ow_hbm, gain_hbm, g_hbm, u_hbm, d_hbm,
    out_ref,
    q_ref, doc_ref, gain_ref,
    G, kx, vx, dx, att, res_v, ow_v, after, normed, ga, ua, hidden, dsend, drecv, ysend, yrecv, zsend, zrecv, own_sum, nsend, nrecv,
    w_send, w_recv, last_recv, tail_send, tail_recv, loc, ow_send, ow_recv, att_send, att_recv, n_send, n_recv,
    d_send, d_recv, y_send, y_recv, z_send, z_recv, o_send, o_recv,
):
    s = lax.axis_index("sp")
    t = lax.axis_index("tp")
    R = q_ref.shape[0]
    C = gain_ref.shape[2]
    D = T * C
    K = D // S
    F = g_hbm.shape[1]
    HK = K // 2
    PER = C // K
    z, x = s // 2, s % 2
    p, c = z % 2, t % 2
    wide = p == c
    n1_z, fr_z, ot_z = z + 1 - 2 * p, (z + 2) % 4, 3 - z
    xp = z * 2 + 1 - x
    n1, fr, ot = n1_z * 2 + x, fr_z * 2 + x, ot_z * 2 + x
    n1_x, fr_x, ot_x = n1_z * 2 + 1 - x, fr_z * 2 + 1 - x, ot_z * 2 + 1 - x
    mid = (z == 1) | (z == 2)
    one, two = jnp.where(mid, fr, ot), jnp.where(mid, ot, fr)
    one_x, two_x = jnp.where(mid, fr_x, ot_x), jnp.where(mid, ot_x, fr_x)
    outer = (z == 0) | (z == 3)
    tc = t + 1 - 2 * c
    ty = (t + 2) % T

    weights = (g_hbm, u_hbm, d_hbm)
    ow_parts = [
        pltpu.make_async_copy(ow_hbm.at[:, i * C:(i + 1) * C], ow_v.at[t, i], loc.at[0]) for i in range(T)
    ]
    res_parts = [
        pltpu.make_async_copy(res_hbm.at[:, i * C:(i + 1) * C], res_v.at[i], loc.at[1]) for i in range(T)
    ]
    firsts = [
        pltpu.make_async_copy(a, b, loc.at[3 + i]) for i, (a, b) in enumerate((
            (doc_hbm, doc_ref), (k_hbm, kx.at[pl.ds(WINDOW, R)]), (v_hbm, vx.at[pl.ds(WINDOW, R)]),
            (q_hbm, q_ref), (gain_hbm, gain_ref)))
    ]
    for cp in firsts + ow_parts + res_parts:
        cp.start()

    def split(is_wide, cond, f):
        for flag, width in ((is_wide, W), (jnp.logical_not(is_wide), N)):
            both = flag if cond is None else flag & cond
            pl.when(both)(functools.partial(f, width))

    def columns(q, width):
        return pl.ds(pl.multiple_of(q * (F - width), 128), width)

    def local(m, width):
        return pltpu.make_async_copy(
            weights[m].at[:, columns(p, width)], G.at[m, s, :, pl.ds(0, width)], loc.at[2])

    for m in range(3):
        split(wide, None, lambda width: local(m, width).start())

    barrier = pltpu.get_barrier_semaphore()
    peers = [(xp, t, None), (fr, t, None), (n1, t, None), (ot, t, mid)]
    peers += [(s, (t + d) % T, None) for d in range(1, T)]
    peers += [((s + 1) % S, t, (x == 1) & (z < 3)), ((s + S - 1) % S, t, (x == 0) & (z > 0))]
    for a, b, cond in peers:
        when(cond, lambda: pl.semaphore_signal(barrier, inc=1, device_id=(a, b), device_id_type=MESH))
    present = sum(1 if cond is None else cond.astype(jnp.int32) for _, _, cond in peers)
    pl.semaphore_wait(barrier, present)

    firsts[0].wait()
    blocks = doc_ref.shape[0]
    for i in range(blocks):
        dx[8 + 8 * i:16 + 8 * i, :] = jnp.broadcast_to(doc_ref[i:i + 1, :], (8, WINDOW))
    finish = []

    def go(cond, cp):
        when(cond, cp.start)
        finish.append(lambda: when(cond, cp.wait_send))

    def start(cp):
        cp.start()

    def remote(src, dst, send_sem, recv_sem, to):
        return pltpu.make_async_remote_copy(
            src_ref=src, dst_ref=dst, send_sem=send_sem, recv_sem=recv_sem, device_id=to, device_id_type=MESH)

    tails = []
    for i, (a, b) in enumerate((
        (k_hbm.at[pl.ds(R - WINDOW, WINDOW)], kx.at[pl.ds(0, WINDOW)]),
        (v_hbm.at[pl.ds(R - WINDOW, WINDOW)], vx.at[pl.ds(0, WINDOW)]),
        (dx.at[pl.ds(8 * blocks, 8)], dx.at[pl.ds(0, 8)]),
    )):
        cp = remote(a, b, tail_send.at[i], tail_recv.at[i], ((s + 1) % S, t))
        go(s < S - 1, cp)
        tails.append(cp)

    kinds = {"A": (1 - p, n1), "B": (p, fr), "C": (1 - p, ot), "D": (p, fr), "X": (p, xp)}

    def weight(kind, m, h, src=None, cond=None, part=None):
        q, to = kinds[kind]
        rows = pl.ds(h * HK, HK) if part is None else pl.ds(h * HK + part * HK // 2, HK // 2)
        sem = w_send.at["ABCDX".index(kind)]
        arrived = last_recv.at[int(kind == "X")] if part == 1 else w_recv.at[m, s if src is None else src, h]

        def copy(width):
            cols = pl.ds(0, width)
            if src is None:
                return remote(weights[m].at[rows, columns(q, width)], G.at[m, s, rows, cols],
                              sem, arrived, (to, t))
            place = G.at[m, src, rows, cols]
            return remote(place, place, sem, arrived, (to, t))

        split(q == c, cond, lambda width: copy(width).start())

    def weights_sent(kind, sources, cond=None):
        q, to = kinds[kind]

        def wait(width):
            place = G.at[:, pl.ds(0, sources), :, pl.ds(0, width)]
            remote(place, place, w_send.at["ABCDX".index(kind)], w_recv.at[0, 0, 0], (to, t)).wait_send()

        split(q == c, cond, wait)

    def recv(m, src, h, cond=None):
        def wait(width):
            place = G.at[m, src, pl.ds(h * HK, HK), pl.ds(0, width)]
            remote(place, place, w_send.at[0], w_recv.at[m, src, h], (xp, t)).wait_recv()
        split(wide, cond, wait)

    def recv_last(src, x_link, part):
        sem = last_recv.at[x_link] if part == 1 else w_recv.at[2, src, 1]

        def wait(width):
            place = G.at[2, src, pl.ds(HK + part * HK // 2, HK // 2), pl.ds(0, width)]
            remote(place, place, w_send.at[0], sem, (xp, t)).wait_recv()
        split(wide, None, wait)

    def landed(ref, sem):
        remote(ref, ref, w_send.at[0], sem, (s, tc)).wait_recv()

    GU = ((0, 0), (1, 0), (0, 1), (1, 1))
    DN = ((2, 0), (2, 1))

    for m, h in GU:
        weight("A", m, h)
        weight("X", m, h)
    for i in range(T):
        part = ow_hbm.at[:, i * C:(i + 1) * C]
        start(remote(part, ow_v.at[t, i], ow_send.at[0], ow_recv.at[i], (s, ty)))
        start(remote(part, ow_v.at[t, i], ow_send.at[1], ow_recv.at[T], (s, tc)))
    weight("A", 2, 0, cond=mid)
    weight("C", 0, 0, cond=mid)
    for m, h in GU[:2]:
        weight("B", m, h)
    for m, h in GU[2:]:
        weight("B", m, h, cond=outer)

    @pl.when(jnp.logical_not(wide))
    def _():
        def clear(i, carry):
            for m in range(3):
                G[m, i, :, N:W] = jnp.zeros((K, W - N), jnp.bfloat16)
            return carry
        if W > N:
            lax.fori_loop(0, S, clear, 0)

    @pl.when(s == 0)
    def _():
        kx[pl.ds(0, WINDOW), :] = jnp.zeros((WINDOW, kx.shape[1]), jnp.bfloat16)
        vx[pl.ds(0, WINDOW), :] = jnp.zeros((WINDOW, vx.shape[1]), jnp.bfloat16)
        dx[pl.ds(0, 8), :] = jnp.zeros((8, dx.shape[1]), jnp.int32)

    for cp in firsts[1:]:
        cp.wait()
    for cp in tails:
        when(s > 0, cp.wait_recv)
    heads = q_ref.shape[1] // HEAD_DIM

    def block(b, carry):
        rows = pl.ds(pl.multiple_of(b * WINDOW, WINDOW), WINDOW)
        band = pl.ds(pl.multiple_of(b * WINDOW, WINDOW), 2 * WINDOW)
        prev = dx[pl.ds(pl.multiple_of(b * 8, 8), 8), :][0:1].astype(jnp.float32)
        own = dx[pl.ds(pl.multiple_of(b * 8 + 8, 8), 8), :][0:1].astype(jnp.float32)
        doc_q = jnp.broadcast_to(own, (WINDOW, WINDOW)).T
        i = lax.broadcasted_iota(jnp.int32, (WINDOW, WINDOW), 0)
        j = lax.broadcasted_iota(jnp.int32, (WINDOW, WINDOW), 1)
        first = s * R + b * WINDOW - WINDOW
        see_prev = (j > i) & (doc_q == prev) & (first + j >= 0)
        see_own = (j <= i) & (doc_q == own)
        visible = jnp.concatenate(
            [see_prev.astype(jnp.float32), see_own.astype(jnp.float32)], axis=1) > 0.5
        for h in range(heads):
            kv = h // GROUP
            cols = slice(kv * HEAD_DIM, (kv + 1) * HEAD_DIM)
            q = q_ref[rows, h * HEAD_DIM:(h + 1) * HEAD_DIM]
            scores = dot(q, kx[band, cols], NT) * HEAD_DIM ** (-0.5)
            scores = jnp.where(visible, scores, neg_big)
            sink = sink_ref[h]
            row_max = jnp.maximum(scores.max(-1, keepdims=True), sink)
            expo = jnp.where(visible, jnp.exp(scores - row_max), 0.0)
            total = expo.sum(-1, keepdims=True) + jnp.exp(sink - row_max)
            w = (expo / total).astype(jnp.bfloat16)
            att[t, rows, h * HEAD_DIM:(h + 1) * HEAD_DIM] = dot(w, vx[band, cols]).astype(jnp.bfloat16)
        return carry

    lax.fori_loop(0, R // WINDOW, block, 0)

    go(None, remote(att.at[t], att.at[t], att_send.at[0], att_recv.at[t], (s, ty)))
    go(None, remote(att.at[t], att.at[t], att_send.at[1], att_recv.at[t], (s, tc)))

    def ow_relay(i):
        landed(ow_v.at[ty, i], ow_recv.at[i])
        start(remote(ow_v.at[ty, i], ow_v.at[ty, i], ow_send.at[2], ow_recv.at[T + 1], (s, tc)))

    def pass_on(m, h, src, cond=None):
        recv(m, src, h, cond)
        weight("X", m, h, src=src, cond=cond)

    pass_on(0, 0, n1)
    weight("D", 0, 0, src=n1, cond=mid)
    pass_on(1, 0, n1)
    weight("D", 1, 0, src=n1, cond=mid)
    for m, h in GU[1:]:
        weight("C", m, h, cond=mid)
    weight("B", 0, 1, cond=mid)
    ow_relay(0)
    pass_on(0, 0, fr, outer)
    ow_relay(1)
    pass_on(0, 1, n1)
    weight("D", 0, 1, src=n1, cond=mid)
    weight("B", 1, 1, cond=mid)
    pass_on(1, 1, n1)
    weight("D", 1, 1, src=n1, cond=mid)
    weight("C", 2, 0, cond=mid)
    ow_relay(2)
    pass_on(0, 0, ot, mid)
    pass_on(1, 0, fr, outer)
    ow_relay(3)
    pass_on(0, 0, ot, outer)
    landed(att.at[ty], att_recv.at[ty])
    go(None, remote(att.at[ty], att.at[ty], att_send.at[2], att_recv.at[ty], (s, tc)))
    pltpu.make_async_copy(ow_v.at[t], ow_v.at[t], loc.at[0]).wait()
    pltpu.make_async_copy(res_v, res_v, loc.at[1]).wait()
    td = (tc + 2) % T
    for i, g in enumerate((tc, td)):
        landed(ow_v.at[g], ow_recv.at[T + i])
        landed(att.at[g], att_recv.at[g])

    HR = R // 2
    for r in range(2):
        rows = slice(r * HR, (r + 1) * HR)

        def project(i, square):
            total = dot(att[0, rows, :], ow_v[0, i]).astype(jnp.bfloat16).astype(jnp.float32)
            for g in range(1, T):
                total += dot(att[g, rows, :], ow_v[g, i]).astype(jnp.bfloat16).astype(jnp.float32)
            value = (res_v[i, rows, :].astype(jnp.float32) + total).astype(jnp.bfloat16)
            after[i, rows, :] = value
            value = value.astype(jnp.float32)
            return square + (value * value).sum(-1, keepdims=True)

        square = lax.fori_loop(0, T, project, jnp.zeros((HR, 1), jnp.float32))
        inv = lax.rsqrt(square / D + norm_eps)

        def norm(i, carry):
            n = (after[i, rows, :].astype(jnp.float32) * inv * gain_ref[i]).astype(jnp.bfloat16)
            for j in range(PER):
                normed[i * PER + j, rows, :] = n[:, j * K:(j + 1) * K]
            return carry

        lax.fori_loop(0, T, norm, 0)
        go(None, remote(
            normed.at[pl.ds(t * PER, PER), pl.ds(r * HR, HR)],
            normed.at[pl.ds(t * PER, PER), pl.ds(R + r * HR, HR)],
            n_send.at[0, r], n_recv.at[t, r], (n1, t)))

    weight("A", 2, 0, cond=outer)
    weight("A", 2, 1)

    def passed(g, r):
        return normed.at[pl.ds(g * PER, PER), pl.ds(R + r * HR, HR)]

    TM = 256

    def gate_up(src, first, last, begin=False):
        def tile(r, carry):
            rows = pl.ds(pl.multiple_of(r * TM, TM), TM)
            a = normed[src, rows, :]
            for m, acc in ((0, ga), (1, ua)):
                value = dot(a, G[m, src])
                if begin:
                    acc[rows, :] = value
                else:
                    acc[rows, :] += value
            return carry
        lax.fori_loop(first // TM, last // TM, tile, 0)

    def local_done(width):
        place = G.at[:, s, :, pl.ds(0, width)]
        pltpu.make_async_copy(place, place, loc.at[2]).wait()

    split(wide, None, local_done)
    for m, h in GU:
        pass_on(m, h, fr, mid)
    gate_up(s, 0, R, True)
    gate_up(n1, 0, R)
    pass_on(1, 0, ot, outer)
    weight("X", 2, 0, cond=outer)
    for src in (xp, n1_x):
        for m, h in GU:
            recv(m, src, h)
        gate_up(src, 0, R)
    pass_on(1, 0, ot, mid)
    for r in range(2):
        landed(passed(t, r), n_recv.at[t, r])
        go(None, remote(passed(t, r), passed(t, r), n_send.at[1, r], n_recv.at[t, r], (s, ty)))
        go(None, remote(passed(t, r), passed(t, r), n_send.at[2, r], n_recv.at[t, r], (s, tc)))
    pass_on(0, 1, ot, mid)
    pass_on(1, 1, ot, mid)
    for m, h in DN:
        weight("X", m, h, cond=mid)
    pass_on(0, 1, fr, outer)
    for r in range(2):
        landed(passed(ty, r), n_recv.at[ty, r])
        go(None, remote(passed(ty, r), passed(ty, r), n_send.at[3, r], n_recv.at[ty, r], (s, tc)))
    for m, h in DN:
        recv(m, n1, h, mid)
        weight("X", m, h, src=n1, cond=mid)
        weight("D", m, h, src=n1, cond=mid)
        if h == 0:
            weight("B", m, h, cond=mid)
    for part in (0, 1):
        weight("B", 2, 1, cond=mid, part=part)
    for part in (0, 1):
        weight("C", 2, 1, cond=mid, part=part)
    pass_on(0, 1, ot, outer)
    for g in (tc, td):
        for r in range(2):
            landed(passed(g, r), n_recv.at[g, r])
    gate_up(s, R, 2 * R, True)
    gate_up(n1, R, 2 * R)
    pass_on(1, 1, fr, outer)
    gate_up(xp, R, 2 * R)
    gate_up(n1_x, R, 2 * R)
    pass_on(1, 1, ot, outer)
    weight("X", 2, 1, cond=outer)
    for m, h in DN:
        weight("B", m, h, cond=outer)
    pass_on(2, 0, n1, outer)
    gate_up(fr, 0, 2 * R)
    gate_up(ot, 0, 2 * R)
    for m, h in GU:
        recv(m, fr_x, h)
    gate_up(fr_x, 0, 2 * R)
    for m, h in GU:
        recv(m, ot_x, h)
    pass_on(2, 1, n1, outer)
    gate_up(ot_x, 0, 2 * R)

    def act(r, carry):
        rows = pl.ds(pl.multiple_of(r * 32, 32), 32)
        g = ga[rows, :]
        hidden[rows, :] = (g / (1.0 + jnp.exp(-g)) * ua[rows, :]).astype(jnp.bfloat16)
        return carry

    lax.fori_loop(0, 2 * R // 32, act, 0)

    def slot(k):
        return k // PER // 2 * PER + k % PER

    def handed(k, h):
        return remote(dsend.at[k, h], drecv.at[k, h], d_send.at[slot(k), h], d_recv.at[slot(k), h], (s, tc))

    def across(j, h):
        return remote(ysend.at[j, h], yrecv.at[j, h], y_send.at[j, h], y_recv.at[j, h], (s, ty))

    def over(j, h):
        return remote(nsend.at[j, h], nrecv.at[j, h], o_send.at[j, h], o_recv.at[j, h], (s, ty))

    def back(k, h):
        return remote(zsend.at[k, h], zrecv.at[k, h], z_send.at[slot(k), h], z_recv.at[slot(k), h], (n1, t))

    def add(out, at, *terms):
        def rows_of(i, carry):
            rows = pl.ds(pl.multiple_of(i * WINDOW, WINDOW), WINDOW)
            total = None
            for ref, where in terms:
                value = ref[(*where, rows, slice(None))].astype(jnp.float32)
                total = value if total is None else total + value
            out[(*at, rows, slice(None))] = total.astype(out.dtype)
            return carry
        lax.fori_loop(0, R // WINDOW, rows_of, 0)

    def kept(k):
        return (k // PER) % 2 == c

    def down(k, *hs):
        given = jnp.logical_not(kept(k))
        value = dot(hidden[...], G[2, k, hs[0] * HK:(hs[-1] + 1) * HK, :], NT).astype(jnp.bfloat16)
        for r in (1, 0):
            for i, h in enumerate(hs):
                dsend[k, h, r] = value[r * R:(r + 1) * R, i * HK:(i + 1) * HK]

        @pl.when(given)
        def _():
            for h in hs:
                handed(k, h).start()

        for h in hs:
            finish.append(functools.partial(when, given, handed(k, h).wait_send))

    def pair(k, h, r):
        return (dsend, (k, h, r)), (drecv, (k, h, r))

    def cross(k, *hs):
        owned, passed_to = k // PER == t, k // PER == ty
        for h in hs:
            j = k % PER

            @pl.when(kept(k))
            def _():
                landed(drecv.at[k, h], d_recv.at[slot(k), h])

            if h == 0:
                @pl.when(passed_to)
                def _():
                    add(nsend, (j, h), *pair(k, h, 1))
                    over(j, h).start()
                    add(ysend, (j, h), *pair(k, h, 0))
                    across(j, h).start()
                finish.append(functools.partial(when, passed_to, over(j, h).wait_send))
                finish.append(functools.partial(when, owned, back(k, h).wait_send))
            else:
                @pl.when(kept(k))
                def _():
                    add(zsend, (k, h), *pair(k, h, 1))
                    back(k, h).start()
                finish.append(functools.partial(when, kept(k), back(k, h).wait_send))

    def cross_split(k):
        owned, passed_to = k // PER == t, k // PER == ty
        j = k % PER

        @pl.when(kept(k))
        def _():
            landed(drecv.at[k, 1], d_recv.at[slot(k), 1])

        @pl.when(mid & passed_to)
        def _():
            add(nsend, (j, 1), *pair(k, 1, 1))
            over(j, 1).start()

        @pl.when(outer & kept(k))
        def _():
            add(zsend, (k, 1), *pair(k, 1, 1))
            back(k, 1).start()

        @pl.when(outer & passed_to)
        def _():
            add(ysend, (j, 1), *pair(k, 1, 0))
            across(j, 1).start()

        finish.append(functools.partial(when, mid & passed_to, over(j, 1).wait_send))
        finish.append(functools.partial(when, (mid & owned) | (outer & kept(k)), back(k, 1).wait_send))

    def lift_split(k):
        j = k % PER

        @pl.when(mid & (k // PER == t))
        def _():
            landed(nrecv.at[j, 1], o_recv.at[j, 1])
            add(zsend, (k, 1), *pair(k, 1, 1), (nrecv, (j, 1)))
            back(k, 1).start()

    def lift(k):
        j = k % PER

        @pl.when(k // PER == t)
        def _():
            terms = pair(k, 0, 1)
            landed(nrecv.at[j, 0], o_recv.at[j, 0])
            add(zsend, (k, 0), *terms, (nrecv, (j, 0)))
            back(k, 0).start()

    def settle(k, *hs):
        for h in hs:
            @pl.when(k // PER == t)
            def _():
                terms = pair(k, h, 0)
                landed(zrecv.at[k, h], z_recv.at[slot(k), h])
                add(own_sum, (k % PER, h), *terms, (zrecv, (k, h)))

    def passing(k, role=True):
        j = k % PER

        @pl.when(role & (k // PER == ty))
        def _():
            terms = pair(k, 1, 0)
            landed(zrecv.at[k, 1], z_recv.at[slot(k), 1])
            add(ysend, (j, 1), *terms, (zrecv, (k, 1)))
            across(j, 1).start()

    def halves(src, *hs):
        for h in hs:
            recv(2, src, h)

    down(s, 0, 1)
    down(n1, 0, 1)
    cross(s, 0, 1)
    halves(xp, 0, 1)
    down(xp, 0, 1)
    cross(n1, 0, 1)
    pass_on(2, 0, ot)
    halves(n1_x, 0, 1)
    down(n1_x, 0, 1)
    cross(xp, 0, 1)
    pass_on(2, 0, fr)
    down(ot, 0)
    lift(s)
    lift(n1)
    cross(n1_x, 0, 1)
    down(fr, 0)
    cross(ot, 0)
    halves(ot_x, 0)
    down(ot_x, 0)
    lift(xp)
    cross(fr, 0)
    pass_on(2, 1, one)
    down(one, 1)
    cross(ot_x, 0)
    for part in (0, 1):
        recv_last(two, 0, part)
        weight("X", 2, 1, src=two, part=part)
    lift(ot)
    halves(fr_x, 0)
    down(fr_x, 0)
    cross_split(one)
    lift(fr)
    lift(n1_x)
    passing(s)
    passing(n1)
    down(two, 1)
    cross(fr_x, 0)
    cross_split(two)
    lift(ot_x)
    halves(one_x, 1)
    down(one_x, 1)
    cross(one_x, 1)
    lift_split(one)
    lift(fr_x)
    passing(xp)
    passing(n1_x)
    for part in (0, 1):
        recv_last(two_x, 1, part)
    down(two_x, 1)
    cross(two_x, 1)
    lift_split(two)
    passing(one, mid)
    passing(two, mid)
    passing(one_x)
    passing(two_x)
    for k in (s, n1, xp, n1_x):
        settle(k, 0, 1)
    for k, h in ((ot, 0), (fr, 0), (ot_x, 0), (one, 1), (fr_x, 0), (two, 1), (one_x, 1), (two_x, 1)):
        settle(k, h)

    for h in (0, 1):
        for j in range(PER):
            landed(yrecv.at[j, h], y_recv.at[j, h])
            cols = slice((j * 2 + h) * HK, (j * 2 + h + 1) * HK)
            out_ref[:, cols] = (
                after[t, :, cols].astype(jnp.float32) + (own_sum[j, h] + yrecv[j, h].astype(jnp.float32))
            ).astype(jnp.bfloat16)

    weights_sent("A", 1)
    weights_sent("B", 1)
    weights_sent("C", 1, mid)
    weights_sent("D", 1, mid)
    weights_sent("X", 4)
    for i, to in enumerate((ty, tc, tc)):
        remote(ow_v.at[0], ow_v.at[0], ow_send.at[i], ow_recv.at[0], (s, to)).wait_send()
    for f in finish:
        f()
    for j in range(PER):
        for h in (0, 1):
            across(j, h).wait_send()


def fused(residual, queries, keys, values, documents, sinks, out_weight, norm_gain, gate_weight, up_weight, down_weight):
    S, T = lax.axis_size("sp"), lax.axis_size("tp")
    R, D = residual.shape
    F = gate_weight.shape[1]
    C, K = D // T, D // S
    W = (F // 128 + 1) // 2 * 128
    N = F - W
    PER = C // K
    blocks = R // WINDOW
    HK = K // 2
    bf, f32 = jnp.bfloat16, jnp.float32
    hbm = pl.BlockSpec(memory_space=pl.ANY)
    dma = pltpu.SemaphoreType.DMA
    scratch = [
        pltpu.VMEM((R, queries.shape[1]), bf),
        pltpu.VMEM((blocks, WINDOW), jnp.int32),
        pltpu.VMEM((T, 1, C), f32),
        pltpu.VMEM((3, S, K, W), bf),
        pltpu.VMEM((R + WINDOW, keys.shape[1]), bf),
        pltpu.VMEM((R + WINDOW, keys.shape[1]), bf),
        pltpu.VMEM((blocks * 8 + 8, WINDOW), jnp.int32),
        pltpu.VMEM((T, R, queries.shape[1]), bf),
        pltpu.VMEM((T, R, C), bf),
        pltpu.VMEM((T, T, out_weight.shape[0], C), bf),
        pltpu.VMEM((T, R, C), bf),
        pltpu.VMEM((S, 2 * R, K), bf),
        pltpu.VMEM((2 * R, W), f32),
        pltpu.VMEM((2 * R, W), f32),
        pltpu.VMEM((2 * R, W), bf),
        pltpu.VMEM((S, 2, 2, R, HK), bf),
        pltpu.VMEM((S, 2, 2, R, HK), bf),
        pltpu.VMEM((PER, 2, R, HK), bf),
        pltpu.VMEM((PER, 2, R, HK), bf),
        pltpu.VMEM((S, 2, R, HK), bf),
        pltpu.VMEM((S, 2, R, HK), bf),
        pltpu.VMEM((PER, 2, R, HK), f32),
        pltpu.VMEM((PER, 2, R, HK), bf),
        pltpu.VMEM((PER, 2, R, HK), bf),
        dma((5,)), dma((3, S, 2)), dma((2,)), dma((3,)), dma((3,)), dma((8,)),
        dma((3,)), dma((T + 2,)), dma((3,)), dma((T,)), dma((4, 2)), dma((T, 2)),
        dma((S // 2, 2)), dma((S // 2, 2)), dma((PER, 2)), dma((PER, 2)), dma((S // 2, 2)), dma((S // 2, 2)),
        dma((PER, 2)), dma((PER, 2)),
    ]
    return pl.pallas_call(
        functools.partial(kernel, S, T, W, N),
        out_shape=pltpu.VMEM((R, C), bf),
        in_specs=[hbm] * 5 + [pl.BlockSpec(memory_space=pltpu.SMEM)] + [hbm] * 5,
        out_specs=pl.BlockSpec(memory_space=pltpu.VMEM),
        scratch_shapes=scratch,
        compiler_params=pltpu.CompilerParams(
            collective_id=0, has_side_effects=True, vmem_limit_bytes=60 * 2**20),
    )(residual, queries, keys, values, documents.reshape(blocks, WINDOW), sinks, out_weight, norm_gain.reshape(T, 1, C),
      gate_weight, up_weight, down_weight)


def line_of_four_pairs(mesh):
    return mesh.shape["sp"] == 8 and mesh.shape["tp"] == 4


def solution(mesh):
    return jax.shard_map(
        fused if line_of_four_pairs(mesh) else on_device,
        mesh=mesh,
        in_specs=(
            P("sp", None),
            P("sp", "tp"),
            P("sp", "tp"),
            P("sp", "tp"),
            P("sp"),
            P("tp"),
            P("tp", None),
            P(),
            P("sp", "tp"),
            P("sp", "tp"),
            P("sp", "tp"),
        ),
        out_specs=P("sp", "tp"),
        check_vma=False,
    )
```

```python
import functools

import jax
import jax.numpy as jnp
from jax import lax
from jax.experimental import pallas as pl
from jax.experimental.pallas import tpu as pltpu
from jax.sharding import PartitionSpec as P

HEAD_DIM = 64
WINDOW = 128
GROUP = 2


neg_big = -1e30
norm_eps = 1e-05


def from_behind(shard, axis, by):
    length = lax.axis_size(axis)
    pairs = [(i, i + by) for i in range(length) if 0 <= i + by < length]
    return lax.ppermute(shard, axis, pairs)


def attend(queries, keys, values, documents, sinks, tail_keys, tail_values, tail_docs, offset):
    rows_here = queries.shape[0]
    block_count = rows_here // WINDOW
    kv_here = keys.shape[1] // HEAD_DIM
    q_blocks = queries.reshape(block_count, WINDOW, kv_here, GROUP, HEAD_DIM)
    k_blocks = keys.reshape(block_count, WINDOW, kv_here, HEAD_DIM)
    v_blocks = values.reshape(block_count, WINDOW, kv_here, HEAD_DIM)
    k_prev = jnp.concatenate(
        [tail_keys.reshape(1, WINDOW, kv_here, HEAD_DIM), k_blocks[:-1]], axis=0
    )
    v_prev = jnp.concatenate(
        [tail_values.reshape(1, WINDOW, kv_here, HEAD_DIM), v_blocks[:-1]], axis=0
    )
    k_band = jnp.concatenate([k_prev, k_blocks], axis=1)
    v_band = jnp.concatenate([v_prev, v_blocks], axis=1)
    doc_own = documents.astype(jnp.float32).reshape(block_count, WINDOW)
    doc_prev = jnp.concatenate(
        [tail_docs.astype(jnp.float32).reshape(1, WINDOW), doc_own[:-1]], axis=0
    )
    doc_band = jnp.concatenate([doc_prev, doc_own], axis=1)
    row_idx = jnp.arange(WINDOW, dtype=jnp.int32)
    col_idx = jnp.arange(2 * WINDOW, dtype=jnp.int32)
    first = offset + jnp.arange(block_count, dtype=jnp.int32) * WINDOW
    q_pos = first[:, None] + row_idx[None, :]
    k_pos = first[:, None] - WINDOW + col_idx[None, :]
    distance = q_pos[:, :, None] - k_pos[:, None, :]
    visible = (
        (distance >= 0)
        & (distance < WINDOW)
        & (k_pos[:, None, :] >= 0)
        & (doc_own[:, :, None] == doc_band[:, None, :])
    )
    scores = jnp.einsum(
        "nikgd,njkd->nkgij", q_blocks, k_band, preferred_element_type=jnp.float32
    ) * HEAD_DIM ** (-0.5)
    scores = jnp.where(visible[:, None, None], scores, neg_big)
    sink_logit = sinks.reshape(1, kv_here, GROUP, 1, 1)
    row_max = jnp.maximum(scores.max(-1, keepdims=True), sink_logit)
    expo = jnp.where(visible[:, None, None], jnp.exp(scores - row_max), 0.0)
    denom_sum = expo.sum(-1, keepdims=True) + jnp.exp(sink_logit - row_max)
    weights = (expo / denom_sum).astype(jnp.bfloat16)
    mixed = jnp.einsum("nkgij,njkd->nikgd", weights, v_band, preferred_element_type=jnp.float32)
    return mixed.reshape(rows_here, kv_here * GROUP * HEAD_DIM).astype(jnp.bfloat16)


def on_device(
    residual,
    queries,
    keys,
    values,
    documents,
    sinks,
    out_weight,
    norm_gain,
    gate_weight,
    up_weight,
    down_weight,
):
    rows_here = queries.shape[0]
    offset = lax.axis_index("sp") * rows_here
    doc_tail = documents[rows_here - WINDOW :].astype(jnp.bfloat16)
    tail_keys, tail_values, tail_docs = from_behind(
        (keys[rows_here - WINDOW :], values[rows_here - WINDOW :], doc_tail), "sp", 1
    )
    attended = attend(
        queries, keys, values, documents, sinks, tail_keys, tail_values, tail_docs, offset
    )
    model_width = residual.shape[1]
    col_count = model_width // lax.axis_size("tp")
    col_first = lax.axis_index("tp") * col_count
    full_term = jnp.dot(attended, out_weight, preferred_element_type=jnp.float32)
    projected = lax.psum(full_term.astype(jnp.bfloat16), "tp").astype(jnp.float32)
    after_full = (residual.astype(jnp.float32) + projected).astype(jnp.bfloat16)
    after_f = after_full.astype(jnp.float32)
    inv_rms = lax.rsqrt(jnp.mean(after_f * after_f, axis=1, keepdims=True) + norm_eps)
    normed = (after_f * inv_rms * norm_gain[None, :]).astype(jnp.bfloat16)
    after = lax.dynamic_slice_in_dim(after_full, col_first, col_count, 1)
    gate_act = jnp.dot(
        normed,
        lax.all_gather(gate_weight, "sp", axis=0, tiled=True),
        preferred_element_type=jnp.float32,
    )
    up_act = jnp.dot(
        normed,
        lax.all_gather(up_weight, "sp", axis=0, tiled=True),
        preferred_element_type=jnp.float32,
    )
    down_full = lax.all_gather(down_weight, "sp", axis=0, tiled=True)
    hidden = (jax.nn.silu(gate_act) * up_act).astype(jnp.bfloat16)
    summed = lax.psum_scatter(
        lax.dot_general(
            down_full, hidden, (((1,), (1,)), ((), ())), preferred_element_type=jnp.float32
        ).astype(jnp.bfloat16),
        "tp",
        scatter_dimension=0,
        tiled=True,
    ).astype(jnp.float32)
    return (after.astype(jnp.float32) + summed.T).astype(jnp.bfloat16)


MESH = pl.DeviceIdType.MESH
NT = (((1,), (1,)), ((), ()))


def dot(a, b, dims=(((1,), (0,)), ((), ()))):
    return lax.dot_general(a, b, dims, preferred_element_type=jnp.float32)


def when(cond, f):
    if cond is None:
        f()
    else:
        pl.when(cond)(f)


def kernel(
    S, T, W, N,
    res_hbm, q_hbm, k_hbm, v_hbm, doc_hbm, sink_ref, ow_hbm, gain_hbm, g_hbm, u_hbm, d_hbm,
    out_ref,
    q_ref, doc_ref, gain_ref,
    G, kx, vx, dx, att, res_v, ow_v, after, normed, ga, ua, hidden, dsend, drecv, ysend, yrecv, zsend, zrecv, own_sum, nsend, nrecv,
    w_send, w_recv, last_recv, tail_send, tail_recv, loc, ow_send, ow_recv, att_send, att_recv, n_send, n_recv,
    d_send, d_recv, y_send, y_recv, z_send, z_recv, o_send, o_recv,
):
    s = lax.axis_index("sp")
    t = lax.axis_index("tp")
    R = q_ref.shape[0]
    C = gain_ref.shape[2]
    D = T * C
    K = D // S
    F = g_hbm.shape[1]
    HK = K // 2
    PER = C // K
    z, x = s // 2, s % 2
    p, c = z % 2, t % 2
    wide = p == c
    n1_z, fr_z, ot_z = z + 1 - 2 * p, (z + 2) % 4, 3 - z
    xp = z * 2 + 1 - x
    n1, fr, ot = n1_z * 2 + x, fr_z * 2 + x, ot_z * 2 + x
    n1_x, fr_x, ot_x = n1_z * 2 + 1 - x, fr_z * 2 + 1 - x, ot_z * 2 + 1 - x
    mid = (z == 1) | (z == 2)
    one, two = jnp.where(mid, fr, ot), jnp.where(mid, ot, fr)
    one_x, two_x = jnp.where(mid, fr_x, ot_x), jnp.where(mid, ot_x, fr_x)
    outer = (z == 0) | (z == 3)
    tc = t + 1 - 2 * c
    ty = (t + 2) % T

    weights = (g_hbm, u_hbm, d_hbm)
    ow_parts = [
        pltpu.make_async_copy(ow_hbm.at[:, i * C:(i + 1) * C], ow_v.at[t, i], loc.at[0]) for i in range(T)
    ]
    res_parts = [
        pltpu.make_async_copy(res_hbm.at[:, i * C:(i + 1) * C], res_v.at[i], loc.at[1]) for i in range(T)
    ]
    firsts = [
        pltpu.make_async_copy(a, b, loc.at[3 + i]) for i, (a, b) in enumerate((
            (doc_hbm, doc_ref), (k_hbm, kx.at[pl.ds(WINDOW, R)]), (v_hbm, vx.at[pl.ds(WINDOW, R)]),
            (q_hbm, q_ref), (gain_hbm, gain_ref)))
    ]
    for cp in firsts + ow_parts + res_parts:
        cp.start()

    def split(is_wide, cond, f):
        for flag, width in ((is_wide, W), (jnp.logical_not(is_wide), N)):
            both = flag if cond is None else flag & cond
            pl.when(both)(functools.partial(f, width))

    def columns(q, width):
        return pl.ds(pl.multiple_of(q * (F - width), 128), width)

    def local(m, width):
        return pltpu.make_async_copy(
            weights[m].at[:, columns(p, width)], G.at[m, s, :, pl.ds(0, width)], loc.at[2])

    for m in range(3):
        split(wide, None, lambda width: local(m, width).start())

    barrier = pltpu.get_barrier_semaphore()
    peers = [(xp, t, None), (fr, t, None), (n1, t, None), (ot, t, mid)]
    peers += [(s, (t + d) % T, None) for d in range(1, T)]
    peers += [((s + 1) % S, t, (x == 1) & (z < 3)), ((s + S - 1) % S, t, (x == 0) & (z > 0))]
    for a, b, cond in peers:
        when(cond, lambda: pl.semaphore_signal(barrier, inc=1, device_id=(a, b), device_id_type=MESH))
    present = sum(1 if cond is None else cond.astype(jnp.int32) for _, _, cond in peers)
    pl.semaphore_wait(barrier, present)

    firsts[0].wait()
    blocks = doc_ref.shape[0]
    for i in range(blocks):
        dx[8 + 8 * i:16 + 8 * i, :] = jnp.broadcast_to(doc_ref[i:i + 1, :], (8, WINDOW))
    finish = []

    def go(cond, cp):
        when(cond, cp.start)
        finish.append(lambda: when(cond, cp.wait_send))

    def start(cp):
        cp.start()

    def remote(src, dst, send_sem, recv_sem, to):
        return pltpu.make_async_remote_copy(
            src_ref=src, dst_ref=dst, send_sem=send_sem, recv_sem=recv_sem, device_id=to, device_id_type=MESH)

    tails = []
    for i, (a, b) in enumerate((
        (k_hbm.at[pl.ds(R - WINDOW, WINDOW)], kx.at[pl.ds(0, WINDOW)]),
        (v_hbm.at[pl.ds(R - WINDOW, WINDOW)], vx.at[pl.ds(0, WINDOW)]),
        (dx.at[pl.ds(8 * blocks, 8)], dx.at[pl.ds(0, 8)]),
    )):
        cp = remote(a, b, tail_send.at[i], tail_recv.at[i], ((s + 1) % S, t))
        go(s < S - 1, cp)
        tails.append(cp)

    kinds = {"A": (1 - p, n1), "B": (p, fr), "C": (1 - p, ot), "D": (p, fr), "X": (p, xp)}

    def weight(kind, m, h, src=None, cond=None, part=None):
        q, to = kinds[kind]
        rows = pl.ds(h * HK, HK) if part is None else pl.ds(h * HK + part * HK // 2, HK // 2)
        sem = w_send.at["ABCDX".index(kind)]
        arrived = last_recv.at[int(kind == "X")] if part == 1 else w_recv.at[m, s if src is None else src, h]

        def copy(width):
            cols = pl.ds(0, width)
            if src is None:
                return remote(weights[m].at[rows, columns(q, width)], G.at[m, s, rows, cols],
                              sem, arrived, (to, t))
            place = G.at[m, src, rows, cols]
            return remote(place, place, sem, arrived, (to, t))

        split(q == c, cond, lambda width: copy(width).start())

    def weights_sent(kind, sources, cond=None):
        q, to = kinds[kind]

        def wait(width):
            place = G.at[:, pl.ds(0, sources), :, pl.ds(0, width)]
            remote(place, place, w_send.at["ABCDX".index(kind)], w_recv.at[0, 0, 0], (to, t)).wait_send()

        split(q == c, cond, wait)

    def recv(m, src, h, cond=None):
        def wait(width):
            place = G.at[m, src, pl.ds(h * HK, HK), pl.ds(0, width)]
            remote(place, place, w_send.at[0], w_recv.at[m, src, h], (xp, t)).wait_recv()
        split(wide, cond, wait)

    def recv_last(src, x_link, part):
        sem = last_recv.at[x_link] if part == 1 else w_recv.at[2, src, 1]

        def wait(width):
            place = G.at[2, src, pl.ds(HK + part * HK // 2, HK // 2), pl.ds(0, width)]
            remote(place, place, w_send.at[0], sem, (xp, t)).wait_recv()
        split(wide, None, wait)

    def landed(ref, sem):
        remote(ref, ref, w_send.at[0], sem, (s, tc)).wait_recv()

    GU = ((0, 0), (1, 0), (0, 1), (1, 1))
    DN = ((2, 0), (2, 1))

    for m, h in GU:
        weight("A", m, h)
        weight("X", m, h)
    for i in range(T):
        part = ow_hbm.at[:, i * C:(i + 1) * C]
        start(remote(part, ow_v.at[t, i], ow_send.at[0], ow_recv.at[i], (s, ty)))
        start(remote(part, ow_v.at[t, i], ow_send.at[1], ow_recv.at[T], (s, tc)))
    weight("A", 2, 0, cond=mid)
    weight("C", 0, 0, cond=mid)
    for m, h in GU[:2]:
        weight("B", m, h)
    for m, h in GU[2:]:
        weight("B", m, h, cond=outer)

    @pl.when(jnp.logical_not(wide))
    def _():
        def clear(i, carry):
            for m in range(3):
                G[m, i, :, N:W] = jnp.zeros((K, W - N), jnp.bfloat16)
            return carry
        if W > N:
            lax.fori_loop(0, S, clear, 0)

    @pl.when(s == 0)
    def _():
        kx[pl.ds(0, WINDOW), :] = jnp.zeros((WINDOW, kx.shape[1]), jnp.bfloat16)
        vx[pl.ds(0, WINDOW), :] = jnp.zeros((WINDOW, vx.shape[1]), jnp.bfloat16)
        dx[pl.ds(0, 8), :] = jnp.zeros((8, dx.shape[1]), jnp.int32)

    for cp in firsts[1:]:
        cp.wait()
    for cp in tails:
        when(s > 0, cp.wait_recv)
    heads = q_ref.shape[1] // HEAD_DIM

    def block(b, carry):
        rows = pl.ds(pl.multiple_of(b * WINDOW, WINDOW), WINDOW)
        band = pl.ds(pl.multiple_of(b * WINDOW, WINDOW), 2 * WINDOW)
        prev = dx[pl.ds(pl.multiple_of(b * 8, 8), 8), :][0:1].astype(jnp.float32)
        own = dx[pl.ds(pl.multiple_of(b * 8 + 8, 8), 8), :][0:1].astype(jnp.float32)
        doc_q = jnp.broadcast_to(own, (WINDOW, WINDOW)).T
        i = lax.broadcasted_iota(jnp.int32, (WINDOW, WINDOW), 0)
        j = lax.broadcasted_iota(jnp.int32, (WINDOW, WINDOW), 1)
        first = s * R + b * WINDOW - WINDOW
        see_prev = (j > i) & (doc_q == prev) & (first + j >= 0)
        see_own = (j <= i) & (doc_q == own)
        visible = jnp.concatenate(
            [see_prev.astype(jnp.float32), see_own.astype(jnp.float32)], axis=1) > 0.5
        for h in range(heads):
            kv = h // GROUP
            cols = slice(kv * HEAD_DIM, (kv + 1) * HEAD_DIM)
            q = q_ref[rows, h * HEAD_DIM:(h + 1) * HEAD_DIM]
            scores = dot(q, kx[band, cols], NT) * HEAD_DIM ** (-0.5)
            scores = jnp.where(visible, scores, neg_big)
            sink = sink_ref[h]
            row_max = jnp.maximum(scores.max(-1, keepdims=True), sink)
            expo = jnp.where(visible, jnp.exp(scores - row_max), 0.0)
            total = expo.sum(-1, keepdims=True) + jnp.exp(sink - row_max)
            w = (expo / total).astype(jnp.bfloat16)
            att[t, rows, h * HEAD_DIM:(h + 1) * HEAD_DIM] = dot(w, vx[band, cols]).astype(jnp.bfloat16)
        return carry

    lax.fori_loop(0, R // WINDOW, block, 0)

    go(None, remote(att.at[t], att.at[t], att_send.at[0], att_recv.at[t], (s, ty)))
    go(None, remote(att.at[t], att.at[t], att_send.at[1], att_recv.at[t], (s, tc)))

    def ow_relay(i):
        landed(ow_v.at[ty, i], ow_recv.at[i])
        start(remote(ow_v.at[ty, i], ow_v.at[ty, i], ow_send.at[2], ow_recv.at[T + 1], (s, tc)))

    def pass_on(m, h, src, cond=None):
        recv(m, src, h, cond)
        weight("X", m, h, src=src, cond=cond)

    pass_on(0, 0, n1)
    weight("D", 0, 0, src=n1, cond=mid)
    pass_on(1, 0, n1)
    weight("D", 1, 0, src=n1, cond=mid)
    for m, h in GU[1:]:
        weight("C", m, h, cond=mid)
    weight("B", 0, 1, cond=mid)
    ow_relay(0)
    pass_on(0, 0, fr, outer)
    ow_relay(1)
    pass_on(0, 1, n1)
    weight("D", 0, 1, src=n1, cond=mid)
    weight("B", 1, 1, cond=mid)
    pass_on(1, 1, n1)
    weight("D", 1, 1, src=n1, cond=mid)
    weight("C", 2, 0, cond=mid)
    ow_relay(2)
    pass_on(0, 0, ot, mid)
    pass_on(1, 0, fr, outer)
    ow_relay(3)
    pass_on(0, 0, ot, outer)
    landed(att.at[ty], att_recv.at[ty])
    go(None, remote(att.at[ty], att.at[ty], att_send.at[2], att_recv.at[ty], (s, tc)))
    pltpu.make_async_copy(ow_v.at[t], ow_v.at[t], loc.at[0]).wait()
    pltpu.make_async_copy(res_v, res_v, loc.at[1]).wait()
    td = (tc + 2) % T
    for i, g in enumerate((tc, td)):
        landed(ow_v.at[g], ow_recv.at[T + i])
        landed(att.at[g], att_recv.at[g])

    HR = R // 2
    for r in range(2):
        rows = slice(r * HR, (r + 1) * HR)

        def project(i, square):
            total = dot(att[0, rows, :], ow_v[0, i]).astype(jnp.bfloat16).astype(jnp.float32)
            for g in range(1, T):
                total += dot(att[g, rows, :], ow_v[g, i]).astype(jnp.bfloat16).astype(jnp.float32)
            value = (res_v[i, rows, :].astype(jnp.float32) + total).astype(jnp.bfloat16)
            after[i, rows, :] = value
            value = value.astype(jnp.float32)
            return square + (value * value).sum(-1, keepdims=True)

        square = lax.fori_loop(0, T, project, jnp.zeros((HR, 1), jnp.float32))
        inv = lax.rsqrt(square / D + norm_eps)

        def norm(i, carry):
            n = (after[i, rows, :].astype(jnp.float32) * inv * gain_ref[i]).astype(jnp.bfloat16)
            for j in range(PER):
                normed[i * PER + j, rows, :] = n[:, j * K:(j + 1) * K]
            return carry

        lax.fori_loop(0, T, norm, 0)
        go(None, remote(
            normed.at[pl.ds(t * PER, PER), pl.ds(r * HR, HR)],
            normed.at[pl.ds(t * PER, PER), pl.ds(R + r * HR, HR)],
            n_send.at[0, r], n_recv.at[t, r], (n1, t)))

    weight("A", 2, 0, cond=outer)
    weight("A", 2, 1)

    def passed(g, r):
        return normed.at[pl.ds(g * PER, PER), pl.ds(R + r * HR, HR)]

    TM = 256

    def gate_up(src, first, last, begin=False):
        def tile(r, carry):
            rows = pl.ds(pl.multiple_of(r * TM, TM), TM)
            a = normed[src, rows, :]
            for m, acc in ((0, ga), (1, ua)):
                value = dot(a, G[m, src])
                if begin:
                    acc[rows, :] = value
                else:
                    acc[rows, :] += value
            return carry
        lax.fori_loop(first // TM, last // TM, tile, 0)

    def local_done(width):
        place = G.at[:, s, :, pl.ds(0, width)]
        pltpu.make_async_copy(place, place, loc.at[2]).wait()

    split(wide, None, local_done)
    for m, h in GU:
        pass_on(m, h, fr, mid)
    gate_up(s, 0, R, True)
    gate_up(n1, 0, R)
    pass_on(1, 0, ot, outer)
    weight("X", 2, 0, cond=outer)
    for src in (xp, n1_x):
        for m, h in GU:
            recv(m, src, h)
        gate_up(src, 0, R)
    pass_on(1, 0, ot, mid)
    for r in range(2):
        landed(passed(t, r), n_recv.at[t, r])
        go(None, remote(passed(t, r), passed(t, r), n_send.at[1, r], n_recv.at[t, r], (s, ty)))
        go(None, remote(passed(t, r), passed(t, r), n_send.at[2, r], n_recv.at[t, r], (s, tc)))
    pass_on(0, 1, ot, mid)
    pass_on(1, 1, ot, mid)
    for m, h in DN:
        weight("X", m, h, cond=mid)
    pass_on(0, 1, fr, outer)
    for r in range(2):
        landed(passed(ty, r), n_recv.at[ty, r])
        go(None, remote(passed(ty, r), passed(ty, r), n_send.at[3, r], n_recv.at[ty, r], (s, tc)))
    for m, h in DN:
        recv(m, n1, h, mid)
        weight("X", m, h, src=n1, cond=mid)
        weight("D", m, h, src=n1, cond=mid)
        if h == 0:
            weight("B", m, h, cond=mid)
    for part in (0, 1):
        weight("B", 2, 1, cond=mid, part=part)
    for part in (0, 1):
        weight("C", 2, 1, cond=mid, part=part)
    pass_on(0, 1, ot, outer)
    for g in (tc, td):
        for r in range(2):
            landed(passed(g, r), n_recv.at[g, r])
    gate_up(s, R, 2 * R, True)
    gate_up(n1, R, 2 * R)
    pass_on(1, 1, fr, outer)
    gate_up(xp, R, 2 * R)
    gate_up(n1_x, R, 2 * R)
    pass_on(1, 1, ot, outer)
    weight("X", 2, 1, cond=outer)
    for m, h in DN:
        weight("B", m, h, cond=outer)
    pass_on(2, 0, n1, outer)
    gate_up(fr, 0, 2 * R)
    gate_up(ot, 0, 2 * R)
    for m, h in GU:
        recv(m, fr_x, h)
    gate_up(fr_x, 0, 2 * R)
    for m, h in GU:
        recv(m, ot_x, h)
    gate_up(ot_x, 0, 2 * R)

    def act(r, carry):
        rows = pl.ds(pl.multiple_of(r * 32, 32), 32)
        g = ga[rows, :]
        hidden[rows, :] = (g / (1.0 + jnp.exp(-g)) * ua[rows, :]).astype(jnp.bfloat16)
        return carry

    lax.fori_loop(0, 2 * R // 32, act, 0)

    def slot(k):
        return k // PER // 2 * PER + k % PER

    def handed(k, h):
        return remote(dsend.at[k, h], drecv.at[k, h], d_send.at[slot(k), h], d_recv.at[slot(k), h], (s, tc))

    def across(j, h):
        return remote(ysend.at[j, h], yrecv.at[j, h], y_send.at[j, h], y_recv.at[j, h], (s, ty))

    def over(j, h):
        return remote(nsend.at[j, h], nrecv.at[j, h], o_send.at[j, h], o_recv.at[j, h], (s, ty))

    def back(k, h):
        return remote(zsend.at[k, h], zrecv.at[k, h], z_send.at[slot(k), h], z_recv.at[slot(k), h], (n1, t))

    def add(out, at, *terms):
        def rows_of(i, carry):
            rows = pl.ds(pl.multiple_of(i * WINDOW, WINDOW), WINDOW)
            total = None
            for ref, where in terms:
                value = ref[(*where, rows, slice(None))].astype(jnp.float32)
                total = value if total is None else total + value
            out[(*at, rows, slice(None))] = total.astype(out.dtype)
            return carry
        lax.fori_loop(0, R // WINDOW, rows_of, 0)

    def kept(k):
        return (k // PER) % 2 == c

    def down(k, *hs):
        given = jnp.logical_not(kept(k))
        value = dot(hidden[...], G[2, k, hs[0] * HK:(hs[-1] + 1) * HK, :], NT).astype(jnp.bfloat16)
        for r in (1, 0):
            for i, h in enumerate(hs):
                dsend[k, h, r] = value[r * R:(r + 1) * R, i * HK:(i + 1) * HK]

        @pl.when(given)
        def _():
            for h in hs:
                handed(k, h).start()

        for h in hs:
            finish.append(functools.partial(when, given, handed(k, h).wait_send))

    def pair(k, h, r):
        return (dsend, (k, h, r)), (drecv, (k, h, r))

    def cross(k, *hs):
        owned, passed_to = k // PER == t, k // PER == ty
        for h in hs:
            j = k % PER

            @pl.when(kept(k))
            def _():
                landed(drecv.at[k, h], d_recv.at[slot(k), h])

            if h == 0:
                @pl.when(passed_to)
                def _():
                    add(nsend, (j, h), *pair(k, h, 1))
                    over(j, h).start()
                    add(ysend, (j, h), *pair(k, h, 0))
                    across(j, h).start()
                finish.append(functools.partial(when, passed_to, over(j, h).wait_send))
                finish.append(functools.partial(when, owned, back(k, h).wait_send))
            else:
                @pl.when(kept(k))
                def _():
                    add(zsend, (k, h), *pair(k, h, 1))
                    back(k, h).start()
                finish.append(functools.partial(when, kept(k), back(k, h).wait_send))

    def cross_split(k):
        owned, passed_to = k // PER == t, k // PER == ty
        j = k % PER

        @pl.when(kept(k))
        def _():
            landed(drecv.at[k, 1], d_recv.at[slot(k), 1])

        @pl.when(mid & passed_to)
        def _():
            add(nsend, (j, 1), *pair(k, 1, 1))
            over(j, 1).start()

        @pl.when(outer & kept(k))
        def _():
            add(zsend, (k, 1), *pair(k, 1, 1))
            back(k, 1).start()

        @pl.when(outer & passed_to)
        def _():
            add(ysend, (j, 1), *pair(k, 1, 0))
            across(j, 1).start()

        finish.append(functools.partial(when, mid & passed_to, over(j, 1).wait_send))
        finish.append(functools.partial(when, (mid & owned) | (outer & kept(k)), back(k, 1).wait_send))

    def lift_split(k):
        j = k % PER

        @pl.when(mid & (k // PER == t))
        def _():
            landed(nrecv.at[j, 1], o_recv.at[j, 1])
            add(zsend, (k, 1), *pair(k, 1, 1), (nrecv, (j, 1)))
            back(k, 1).start()

    def lift(k, role=True):
        j = k % PER

        @pl.when(role & (k // PER == t))
        def _():
            terms = pair(k, 0, 1)
            landed(nrecv.at[j, 0], o_recv.at[j, 0])
            add(zsend, (k, 0), *terms, (nrecv, (j, 0)))
            back(k, 0).start()

    def settle(k, *hs):
        for h in hs:
            @pl.when(k // PER == t)
            def _():
                terms = pair(k, h, 0)
                landed(zrecv.at[k, h], z_recv.at[slot(k), h])
                add(own_sum, (k % PER, h), *terms, (zrecv, (k, h)))

    def passing(k, role=True):
        j = k % PER

        @pl.when(role & (k // PER == ty))
        def _():
            terms = pair(k, 1, 0)
            landed(zrecv.at[k, 1], z_recv.at[slot(k), 1])
            add(ysend, (j, 1), *terms, (zrecv, (k, 1)))
            across(j, 1).start()

    def halves(src, *hs):
        for h in hs:
            recv(2, src, h)

    down(s, 0, 1)
    pass_on(2, 1, n1, outer)
    down(n1, 0, 1)
    cross(s, 0, 1)
    halves(xp, 0, 1)
    down(xp, 0, 1)
    cross(n1, 0, 1)
    pass_on(2, 0, ot)
    halves(n1_x, 0, 1)
    down(n1_x, 0, 1)
    cross(xp, 0, 1)
    pass_on(2, 0, fr)
    down(ot, 0)
    lift(s)
    lift(n1)
    cross(n1_x, 0, 1)
    down(fr, 0)
    cross(ot, 0)
    halves(ot_x, 0)
    down(ot_x, 0)
    lift(xp)
    cross(fr, 0)
    pass_on(2, 1, one)
    down(one, 1)
    cross(ot_x, 0)
    for part in (0, 1):
        recv_last(two, 0, part)
        weight("X", 2, 1, src=two, part=part)
    lift(ot, mid)
    halves(fr_x, 0)
    down(fr_x, 0)
    cross_split(one)
    lift(fr, mid)
    lift(ot, outer)
    lift(n1_x)
    passing(s)
    passing(n1)
    down(two, 1)
    cross(fr_x, 0)
    cross_split(two)
    lift(ot_x, mid)
    halves(one_x, 1)
    down(one_x, 1)
    cross(one_x, 1)
    lift_split(one)
    lift(fr_x, mid)
    lift(fr, outer)
    passing(xp)
    passing(n1_x)
    for part in (0, 1):
        recv_last(two_x, 1, part)
    down(two_x, 1)
    cross(two_x, 1)
    lift_split(two)
    lift(ot_x, outer)
    lift(fr_x, outer)
    passing(one, mid)
    passing(two, mid)
    passing(one_x)
    passing(two_x)
    for k in (s, n1, xp, n1_x):
        settle(k, 0, 1)
    for k, h in ((ot, 0), (fr, 0), (ot_x, 0), (one, 1), (fr_x, 0), (two, 1), (one_x, 1), (two_x, 1)):
        settle(k, h)

    for h in (0, 1):
        for j in range(PER):
            landed(yrecv.at[j, h], y_recv.at[j, h])
            cols = slice((j * 2 + h) * HK, (j * 2 + h + 1) * HK)
            out_ref[:, cols] = (
                after[t, :, cols].astype(jnp.float32) + (own_sum[j, h] + yrecv[j, h].astype(jnp.float32))
            ).astype(jnp.bfloat16)

    weights_sent("A", 1)
    weights_sent("B", 1)
    weights_sent("C", 1, mid)
    weights_sent("D", 1, mid)
    weights_sent("X", 4)
    for i, to in enumerate((ty, tc, tc)):
        remote(ow_v.at[0], ow_v.at[0], ow_send.at[i], ow_recv.at[0], (s, to)).wait_send()
    for f in finish:
        f()
    for j in range(PER):
        for h in (0, 1):
            across(j, h).wait_send()


def fused(residual, queries, keys, values, documents, sinks, out_weight, norm_gain, gate_weight, up_weight, down_weight):
    S, T = lax.axis_size("sp"), lax.axis_size("tp")
    R, D = residual.shape
    F = gate_weight.shape[1]
    C, K = D // T, D // S
    W = (F // 128 + 1) // 2 * 128
    N = F - W
    PER = C // K
    blocks = R // WINDOW
    HK = K // 2
    bf, f32 = jnp.bfloat16, jnp.float32
    hbm = pl.BlockSpec(memory_space=pl.ANY)
    dma = pltpu.SemaphoreType.DMA
    scratch = [
        pltpu.VMEM((R, queries.shape[1]), bf),
        pltpu.VMEM((blocks, WINDOW), jnp.int32),
        pltpu.VMEM((T, 1, C), f32),
        pltpu.VMEM((3, S, K, W), bf),
        pltpu.VMEM((R + WINDOW, keys.shape[1]), bf),
        pltpu.VMEM((R + WINDOW, keys.shape[1]), bf),
        pltpu.VMEM((blocks * 8 + 8, WINDOW), jnp.int32),
        pltpu.VMEM((T, R, queries.shape[1]), bf),
        pltpu.VMEM((T, R, C), bf),
        pltpu.VMEM((T, T, out_weight.shape[0], C), bf),
        pltpu.VMEM((T, R, C), bf),
        pltpu.VMEM((S, 2 * R, K), bf),
        pltpu.VMEM((2 * R, W), f32),
        pltpu.VMEM((2 * R, W), f32),
        pltpu.VMEM((2 * R, W), bf),
        pltpu.VMEM((S, 2, 2, R, HK), bf),
        pltpu.VMEM((S, 2, 2, R, HK), bf),
        pltpu.VMEM((PER, 2, R, HK), bf),
        pltpu.VMEM((PER, 2, R, HK), bf),
        pltpu.VMEM((S, 2, R, HK), bf),
        pltpu.VMEM((S, 2, R, HK), bf),
        pltpu.VMEM((PER, 2, R, HK), f32),
        pltpu.VMEM((PER, 2, R, HK), bf),
        pltpu.VMEM((PER, 2, R, HK), bf),
        dma((5,)), dma((3, S, 2)), dma((2,)), dma((3,)), dma((3,)), dma((8,)),
        dma((3,)), dma((T + 2,)), dma((3,)), dma((T,)), dma((4, 2)), dma((T, 2)),
        dma((S // 2, 2)), dma((S // 2, 2)), dma((PER, 2)), dma((PER, 2)), dma((S // 2, 2)), dma((S // 2, 2)),
        dma((PER, 2)), dma((PER, 2)),
    ]
    return pl.pallas_call(
        functools.partial(kernel, S, T, W, N),
        out_shape=pltpu.VMEM((R, C), bf),
        in_specs=[hbm] * 5 + [pl.BlockSpec(memory_space=pltpu.SMEM)] + [hbm] * 5,
        out_specs=pl.BlockSpec(memory_space=pltpu.VMEM),
        scratch_shapes=scratch,
        compiler_params=pltpu.CompilerParams(
            collective_id=0, has_side_effects=True, vmem_limit_bytes=60 * 2**20),
    )(residual, queries, keys, values, documents.reshape(blocks, WINDOW), sinks, out_weight, norm_gain.reshape(T, 1, C),
      gate_weight, up_weight, down_weight)


def line_of_four_pairs(mesh):
    return mesh.shape["sp"] == 8 and mesh.shape["tp"] == 4


def solution(mesh):
    return jax.shard_map(
        fused if line_of_four_pairs(mesh) else on_device,
        mesh=mesh,
        in_specs=(
            P("sp", None),
            P("sp", "tp"),
            P("sp", "tp"),
            P("sp", "tp"),
            P("sp"),
            P("tp"),
            P("tp", None),
            P(),
            P("sp", "tp"),
            P("sp", "tp"),
            P("sp", "tp"),
        ),
        out_specs=P("sp", "tp"),
        check_vma=False,
    )
```
